128 devices in a mesh: fs: 16 (over z, x), tp: 8 (over y, core).
Axes of the slice: x: 4, y: 4, z: 4, core: 2. Of those that a mesh axis runs over, the one named last changes fastest.
Arguments:
- prompts: bfloat16 [8, 1024, 2048], P('tp'), may hold values from -6 to 6
- gain_first: float32 [2048], P('fs'), may hold values from 0.1 to 1.9
- gate_first: float32 [2048, 5632], P('fs', 'tp'), may hold values from -0.125 to 0.125
- up_first: float32 [2048, 5632], P('fs', 'tp'), may hold values from -0.125 to 0.125
- down_first: float32 [5632, 2048], P('fs', 'tp'), may hold values from -0.078125 to 0.078125
- gain_second: float32 [2048], P('fs'), may hold values from 0.1 to 1.9
- gate_second: float32 [2048, 5632], P('fs', 'tp'), may hold values from -0.125 to 0.125
- up_second: float32 [2048, 5632], P('fs', 'tp'), may hold values from -0.125 to 0.125
- down_second: float32 [5632, 2048], P('fs', 'tp'), may hold values from -0.078125 to 0.078125
Outputs:
- served_gate_first: bfloat16 [2048, 5632], P(None, 'fs')
- served_up_first: bfloat16 [2048, 5632], P(None, 'fs')
- served_down_first: bfloat16 [5632, 2048], P('fs')
- served_gate_second: bfloat16 [2048, 5632], P(None, 'fs')
- served_up_second: bfloat16 [2048, 5632], P(None, 'fs')
- served_down_second: bfloat16 [5632, 2048], P('fs')
- prompt_states: bfloat16 [8, 1024, 2048], P('tp', 'fs')
The draws below stay inside these ranges and needn't reach their ends.
All inputs are finite; a program needn't handle non-finite values.
Results may differ from the reference program's by a relative error of at most 0.012.
Values may be sent and summed in bfloat16 or wider, within the bound.
A program may use at most 128 MiB of HBM per device.

```python
import jax
import jax.numpy as jnp
from jax import lax

D = 2048
FF = 5632
PLEN = 1024
PROMPTS = 8
N_FS = 16


def levels(rng, dims, cuts, smallest, top_value):
    gain, own = 1.0, jax.random.fold_in(rng, 6)
    for dim, parts in cuts:
        draws = jnp.exp(jax.random.uniform(jax.random.fold_in(own, dim), (parts,), jnp.float32, smallest / len(cuts), top_value / len(cuts)))
        gain = gain * jnp.repeat(draws, dims[dim] // parts).reshape([-1 if axis == dim else 1 for axis in range(len(dims))])
    return gain


def bell_draw(own_key, dims, spread, bound, split=(), held_as=jnp.bfloat16):
    factor_of = levels(own_key, dims, split, -0.22, 0.18) if split else 1.0
    result = jax.random.normal(own_key, dims, jnp.float32) * spread * factor_of
    return jnp.minimum(jnp.maximum(result, -bound), bound).astype(held_as)


def setup_inputs(seed: int = 0) -> dict:
    splits = jax.random.split(jax.random.key(seed), 10)
    prompts = bell_draw(splits[0], (PROMPTS, PLEN, D), 1.0, 6.0, ((0, 8),))
    gain_first = jnp.clip(1.0 + 0.18 * jax.random.normal(splits[1], (D,), jnp.float32), 0.1, 1.9)
    gate_first = bell_draw(splits[2], (D, FF), D ** -0.5, 0.125, ((0, 16), (1, 8)), jnp.float32)
    up_first = bell_draw(splits[3], (D, FF), D ** -0.5, 0.125, ((0, 16), (1, 8)), jnp.float32)
    down_first = bell_draw(splits[4], (FF, D), FF ** -0.5, 0.078125, ((0, 16), (1, 8)), jnp.float32)
    gain_second = jnp.clip(1.0 + 0.18 * jax.random.normal(splits[5], (D,), jnp.float32), 0.1, 1.9)
    gate_second = bell_draw(splits[6], (D, FF), D ** -0.5, 0.125, ((0, 16), (1, 8)), jnp.float32)
    up_second = bell_draw(splits[7], (D, FF), D ** -0.5, 0.125, ((0, 16), (1, 8)), jnp.float32)
    down_second = bell_draw(splits[8], (FF, D), FF ** -0.5, 0.078125, ((0, 16), (1, 8)), jnp.float32)
    return dict(prompts=prompts, gain_first=gain_first, gate_first=gate_first, up_first=up_first, down_first=down_first, gain_second=gain_second, gate_second=gate_second, up_second=up_second, down_second=down_second)


def normalize(row_block):
    widened = row_block.astype(jnp.float32)
    scaled = widened * lax.rsqrt(lax.optimization_barrier(jnp.mean(widened * widened, axis=-1, keepdims=True)) + 1e-06)
    return scaled.astype(jnp.bfloat16)

def block_sum(active, down_rows):
    unit_count = active.shape[1] // N_FS

    def advance(running, block_index):
        left_cols = lax.dynamic_slice_in_dim(active, block_index * unit_count, unit_count, 1)
        right_rows = lax.dynamic_slice_in_dim(down_rows, block_index * unit_count, unit_count, 0)
        partial_sum = jnp.dot(left_cols, right_rows, preferred_element_type=jnp.float32).astype(jnp.bfloat16)
        partial_sum = lax.optimization_barrier(partial_sum)
        return (running + partial_sum.astype(jnp.float32), None)
    start_sum = jnp.zeros((active.shape[0], down_rows.shape[1]), jnp.float32)
    running, _ = lax.scan(advance, start_sum, jnp.arange(N_FS, dtype=jnp.int32))
    return running

def half_step(tokens_in, gate_cols, up_cols, down_rows):
    normed = normalize(tokens_in)
    gate_val = jnp.dot(normed, gate_cols, preferred_element_type=jnp.float32)
    up_val = jnp.dot(normed, up_cols, preferred_element_type=jnp.float32)
    active = (jax.nn.silu(gate_val) * up_val).astype(jnp.bfloat16)
    branch = block_sum(active, down_rows)
    return (tokens_in.astype(jnp.float32) + 0.5 * branch).astype(jnp.bfloat16)

def reference(prompts, gain_first, gate_first, up_first, down_first, gain_second, gate_second, up_second, down_second):
    served_gate_first = (gain_first[:, None] * gate_first).astype(jnp.bfloat16)
    served_up_first = (gain_first[:, None] * up_first).astype(jnp.bfloat16)
    served_gate_second = (gain_second[:, None] * gate_second).astype(jnp.bfloat16)
    served_up_second = (gain_second[:, None] * up_second).astype(jnp.bfloat16)
    served_down_first = down_first.astype(jnp.bfloat16)
    served_down_second = down_second.astype(jnp.bfloat16)
    tokens_in = prompts.reshape(-1, prompts.shape[-1])
    middle = half_step(tokens_in, served_gate_first, served_up_first, served_down_first)
    finished = half_step(middle, served_gate_second, served_up_second, served_down_second)
    return (served_gate_first, served_up_first, served_down_first, served_gate_second, served_up_second, served_down_second, finished.reshape(prompts.shape))
```

```python
import functools

import jax
import jax.numpy as jnp
from jax import lax
from jax.experimental import pallas as pl
from jax.experimental.pallas import tpu as pltpu
from jax.sharding import PartitionSpec as P

D = 2048
FF = 5632
HB = 352
HP = 384
TOK = 1024
MESH = pl.DeviceIdType.MESH
BF = jnp.bfloat16
F32 = jnp.float32


def rem4(v):
    return lax.rem(v, 4)


def kernel(
    x_hbm, wt, dn,
    gu1_o, gu2_o, d1_o, d2_o, ps_o,
    nx, ng, xown, mid, gu, dd, act, part,
    r2, ra, rb, tt, acc, sb, q2, qa, qb, qt, ost,
    w_recv, w_a, w_f, w_s, d_recv, d_send, d_loc, rs_send, rs_recv, ag_send, ag_recv, x_sem, o_sem,
):
    f = lax.axis_index("fs")
    t = lax.axis_index("tp")
    z = lax.div(f, 4)
    x = lax.rem(f, 4)
    y = lax.div(t, 2)
    core = lax.rem(t, 2)
    sib = (f, 2 * y + 1 - core)
    pending = []

    def send(src, dst, ssem, rsem, dev, cond=None):
        cp = pltpu.make_async_remote_copy(
            src_ref=src, dst_ref=dst, send_sem=ssem, recv_sem=rsem, device_id=dev, device_id_type=MESH
        )
        if cond is None:
            cp.start()
        else:
            pl.when(cond)(cp.start)
        pending.append((cp, cond))

    def drain():
        for cp, cond in pending:
            if cond is None:
                cp.wait_send()
            else:
                pl.when(cond)(cp.wait_send)
        pending.clear()

    def arrived(dst, sem):
        pltpu.make_async_copy(dst, dst, sem).wait()

    xcp = []
    for r in range(4):
        cp = pltpu.make_async_copy(x_hbm.at[r], nx.at[r], x_sem.at[r])
        cp.start()
        xcp.append(cp)
    own_in = pltpu.make_async_copy(x_hbm.at[z, x], xown, x_sem.at[4])
    own_in.start()

    def wrows(h, ft):
        return gu.at[h, pl.ds(pl.multiple_of(ft * 128, 128), 128), :]

    def stage_a(h):
        for g in range(2):
            df = 2 * t + g
            dt = 2 * y + lax.rem(f, 2)
            same = jnp.logical_and(df == f, dt == t)
            other = jnp.logical_not(same)
            send(wt.at[h, g], wrows(h, f), w_a.at[h, g], w_recv.at[h, f], (df, dt), other)

            @pl.when(same)
            def _():
                pltpu.make_async_copy(wt.at[h, g], wrows(h, f), w_recv.at[h, f]).start()

    ny = rem4(y + 1 + 2 * core)
    dist = rem4(jnp.where(core == 0, y - z, z - y) + 4)
    ORDER = [(0, 0), (0, 1), (1, 0), (1, 1), (3, 0), (3, 1), (2, 0), (2, 1)]

    def chain(h, i):
        dz, k = ORDER[i]
        ft = 4 * rem4(z + dz) + 2 * k + core
        tile = wrows(h, ft)
        arrived(tile, w_recv.at[h, ft])
        send(tile, tile, w_f.at[h, i], w_recv.at[h, ft], (f, 2 * ny + core), dist < 3)
        send(tile, tile, w_s.at[h, i], w_recv.at[h, ft], sib)

    def chain_other(h):
        for i in range(8):
            ft = 2 * i + 1 - core
            arrived(wrows(h, ft), w_recv.at[h, ft])

    yp, ym, y2 = rem4(y + 1), rem4(y + 3), rem4(y + 2)

    def dblk(h, tb, q):
        return dd.at[h, pl.ds(176 * q, 176), pl.ds(pl.multiple_of(tb * 256, 256), 256)]

    def down_start(h):
        pltpu.make_async_copy(
            dn.at[h], dd.at[h, pl.ds(0, HB), pl.ds(pl.multiple_of(t * 256, 256), 256)], d_loc.at[h]
        ).start()
        k = 0
        for q in range(2):
            src = dn.at[h, pl.ds(176 * q, 176), :]
            for dev in ((f, 2 * yp + core), (f, 2 * ym + core), sib):
                send(src, dblk(h, t, q), d_send.at[h, k], d_recv.at[h, t, q], dev)
                k += 1

    def down_mid(h):
        tm, tp = 2 * ym + core, 2 * yp + core
        arrived(dblk(h, tm, 0), d_recv.at[h, tm, 0])
        send(dblk(h, tm, 0), dblk(h, tm, 0), d_send.at[h, 6], d_recv.at[h, tm, 0], (f, 2 * yp + core))
        arrived(dblk(h, tp, 1), d_recv.at[h, tp, 1])
        send(dblk(h, tp, 1), dblk(h, tp, 1), d_send.at[h, 7], d_recv.at[h, tp, 1], (f, 2 * ym + core))
        send(dblk(h, tm, 0), dblk(h, tm, 0), d_send.at[h, 8], d_recv.at[h, tm, 0], sib)
        send(dblk(h, tp, 1), dblk(h, tp, 1), d_send.at[h, 9], d_recv.at[h, tp, 1], sib)
        k = 10
        for tb, q in ((tm, 1), (tp, 0)):
            arrived(dblk(h, tb, q), d_recv.at[h, tb, q])
            send(dblk(h, tb, q), dblk(h, tb, q), d_send.at[h, k], d_recv.at[h, tb, q], sib)
            k += 1

    def down_end(h):
        t2 = 2 * y2 + core
        for q in range(2):
            arrived(dblk(h, t2, q), d_recv.at[h, t2, q])
            send(dblk(h, t2, q), dblk(h, t2, q), d_send.at[h, 12 + q], d_recv.at[h, t2, q], sib)
        for yy in range(4):
            for q in range(2):
                tb = 2 * yy + 1 - core
                arrived(dblk(h, tb, q), d_recv.at[h, tb, q])
        pltpu.make_async_copy(
            dn.at[h], dd.at[h, pl.ds(0, HB), pl.ds(pl.multiple_of(t * 256, 256), 256)], d_loc.at[h]
        ).wait()

    def norm_rows(v):
        w = v.astype(F32)
        return (w * lax.rsqrt(jnp.mean(w * w, axis=-1, keepdims=True) + 1e-06)).astype(BF)

    def gate_up(src, h):
        @pl.loop(0, 4)
        def _(r):
            a = src[r].reshape(256, D)
            v = jnp.dot(a, gu[h], preferred_element_type=F32)
            gt = v[:, :HP]
            up = v[:, HP:]
            act[r] = (gt * jax.nn.sigmoid(gt) * up).astype(BF).reshape(4, 64, HP)

    def colsl(ab):
        return pl.ds(1024 * ab, 1024)

    def pv(h, ab, idx, q):
        if ab == 0:
            return part.at[h, pl.ds(2 * q, 2), idx, :, colsl(0)]
        return part.at[h, idx, pl.ds(2 * q, 2), :, colsl(1)]

    def dev1(ab, step):
        if ab == 0:
            return (4 * z + rem4(x + step + 4), t)
        return (4 * rem4(z + step + 4) + x, t)

    def me1(ab, step):
        return rem4((x if ab == 0 else z) + step + 4)

    def down_chunk(h, ab, idx):
        w = dd[h, :, 1024 * ab:1024 * ab + 1024]
        if ab == 0:
            a = act[:, pl.ds(idx, 1)].reshape(256, HP)
        else:
            a = act[idx].reshape(256, HP)
        v = jnp.dot(a, w, preferred_element_type=F32).astype(BF)
        if ab == 0:
            part[h, :, pl.ds(idx, 1), :, 0:1024] = v.reshape(4, 1, 64, 1024)
        else:
            part[h, idx, :, :, 1024:2048] = v.reshape(4, 64, 1024)

    def s1(h, ab, k, src, dst, step):
        send(src, dst, rs_send.at[h, 0, ab, k], rs_recv.at[h, 0, ab, k], dev1(ab, step))

    def s2(h, ab, k, src, dst, step):
        send(src, dst, rs_send.at[h, 1, ab, k], rs_recv.at[h, 1, ab, k], dev1(1 - ab, step))

    def rs_first(h, between=None):
        for ab in range(2):
            i2 = me1(ab, 2)
            down_chunk(h, ab, i2)
            s1(h, ab, 0, pv(h, ab, i2, 0), r2.at[h, ab, 0], 1)
            s1(h, ab, 1, pv(h, ab, i2, 1), r2.at[h, ab, 1], -1)
        for ab in range(2):
            ip = me1(ab, 1)
            down_chunk(h, ab, ip)
            s1(h, ab, 3, pv(h, ab, ip, 1), ra.at[h, ab, pl.ds(2, 2)], 1)
        for ab in range(2):
            im = me1(ab, -1)
            down_chunk(h, ab, im)
            s1(h, ab, 4, pv(h, ab, im, 0), rb.at[h, ab, pl.ds(0, 2)], -1)
        for ab in range(2):
            down_chunk(h, ab, me1(ab, 0))

    def rs_second(h):
        for ab in range(2):
            arrived(r2.at[h, ab, 0], rs_recv.at[h, 0, ab, 0])
            tt[h, ab, 0] = (r2[h, ab, 0].astype(F32) + pv(h, ab, me1(ab, 1), 0)[...].astype(F32)).astype(BF)
            s1(h, ab, 2, tt.at[h, ab, 0], ra.at[h, ab, pl.ds(0, 2)], 1)
            arrived(r2.at[h, ab, 1], rs_recv.at[h, 0, ab, 1])
            tt[h, ab, 1] = (r2[h, ab, 1].astype(F32) + pv(h, ab, me1(ab, -1), 1)[...].astype(F32)).astype(BF)
            s1(h, ab, 5, tt.at[h, ab, 1], rb.at[h, ab, pl.ds(2, 2)], -1)

    def rs_third(h):
        for ab in range(2):
            for q in range(2):
                sl = pl.ds(2 * q, 2)
                arrived(ra.at[h, ab, sl], rs_recv.at[h, 0, ab, 2 + q])
                arrived(rb.at[h, ab, sl], rs_recv.at[h, 0, ab, 4 + q])
                s = (
                    pv(h, ab, me1(ab, 0), q)[...].astype(F32)
                    + ra[h, ab, 2 * q:2 * q + 2].astype(F32)
                    + rb[h, ab, 2 * q:2 * q + 2].astype(F32)
                )
                acc[ab, 2 * q:2 * q + 2] = s
                sb[h, ab, 2 * q:2 * q + 2] = s.astype(BF)
            i2, ip, im = me1(1 - ab, 2), me1(1 - ab, 1), me1(1 - ab, -1)
            s2(h, ab, 0, sb.at[h, ab, i2, pl.ds(0, 32)], q2.at[h, ab, 0], 1)
            s2(h, ab, 1, sb.at[h, ab, i2, pl.ds(32, 32)], q2.at[h, ab, 1], -1)
            s2(h, ab, 3, sb.at[h, ab, ip, pl.ds(32, 32)], qa.at[h, ab, pl.ds(32, 32)], 1)
            s2(h, ab, 4, sb.at[h, ab, im, pl.ds(0, 32)], qb.at[h, ab, pl.ds(0, 32)], -1)

    def rs_fourth(h):
        for ab in range(2):
            ip, im = me1(1 - ab, 1), me1(1 - ab, -1)
            arrived(q2.at[h, ab, 0], rs_recv.at[h, 1, ab, 0])
            qt[h, ab, 0] = (q2[h, ab, 0].astype(F32) + acc[ab, ip, 0:32]).astype(BF)
            s2(h, ab, 2, qt.at[h, ab, 0], qa.at[h, ab, pl.ds(0, 32)], 1)
            arrived(q2.at[h, ab, 1], rs_recv.at[h, 1, ab, 1])
            qt[h, ab, 1] = (q2[h, ab, 1].astype(F32) + acc[ab, im, 32:64]).astype(BF)
            s2(h, ab, 5, qt.at[h, ab, 1], qb.at[h, ab, pl.ds(32, 32)], -1)
        out = []
        for ab in range(2):
            for q in range(2):
                arrived(qa.at[h, ab, pl.ds(32 * q, 32)], rs_recv.at[h, 1, ab, 2 + q])
                arrived(qb.at[h, ab, pl.ds(32 * q, 32)], rs_recv.at[h, 1, ab, 4 + q])
            out.append(acc[ab, me1(1 - ab, 0)] + qa[h, ab].astype(F32) + qb[h, ab].astype(F32))
        return jnp.concatenate(out, axis=-1)

    def gv(ab, i, j, rows=None):
        rows = slice(None) if rows is None else rows
        if ab == 0:
            return ng.at[i, j, rows, colsl(0)]
        return ng.at[j, i, rows, colsl(1)]

    def ag(h=0):
        def snd(ab, k, ref, second, step):
            send(ref, ref, ag_send.at[ab, k], ag_recv.at[ab, k], dev1(ab if second else 1 - ab, step))

        idx = []
        for ab in range(2):
            i0 = me1(1 - ab, 0)
            j0 = me1(ab, 0)
            idx.append((i0, j0, rem4(i0 + 1), rem4(i0 + 3), rem4(i0 + 2), rem4(j0 + 1), rem4(j0 + 3), rem4(j0 + 2)))
        lo, hi = pl.ds(0, 32), pl.ds(32, 32)
        for ab in range(2):
            i0, j0 = idx[ab][:2]
            snd(ab, 0, gv(ab, i0, j0), False, 1)
            snd(ab, 1, gv(ab, i0, j0), False, -1)
            snd(ab, 4, gv(ab, i0, j0), True, 1)
            snd(ab, 8, gv(ab, i0, j0), True, -1)
        for ab in range(2):
            i0, j0, ip, im, i2, jp, jm, j2 = idx[ab]
            arrived(gv(ab, im, j0), ag_recv.at[ab, 0])
            snd(ab, 2, gv(ab, im, j0, lo), False, 1)
            snd(ab, 7, gv(ab, im, j0), True, 1)
            snd(ab, 11, gv(ab, im, j0), True, -1)
            arrived(gv(ab, ip, j0), ag_recv.at[ab, 1])
            snd(ab, 3, gv(ab, ip, j0, hi), False, -1)
            snd(ab, 5, gv(ab, ip, j0), True, 1)
            snd(ab, 9, gv(ab, ip, j0), True, -1)
        for ab in range(2):
            i0, j0, ip, im, i2, jp, jm, j2 = idx[ab]
            arrived(gv(ab, i0, jm), ag_recv.at[ab, 4])
            snd(ab, 12, gv(ab, i0, jm), True, 1)
            arrived(gv(ab, i0, jp), ag_recv.at[ab, 8])
        for ab in range(2):
            i0, j0, ip, im, i2, jp, jm, j2 = idx[ab]
            arrived(gv(ab, i2, j0, lo), ag_recv.at[ab, 2])
            arrived(gv(ab, i2, j0, hi), ag_recv.at[ab, 3])
            snd(ab, 6, gv(ab, i2, j0), True, 1)
            snd(ab, 10, gv(ab, i2, j0), True, -1)
        for ab in range(2):
            i0, j0, ip, im, i2, jp, jm, j2 = idx[ab]
            arrived(gv(ab, ip, jm), ag_recv.at[ab, 5])
            snd(ab, 13, gv(ab, ip, jm), True, 1)
            arrived(gv(ab, im, jp), ag_recv.at[ab, 11])
            snd(ab, 14, gv(ab, im, jp), True, -1)
        for ab in range(2):
            i0, j0, ip, im, i2, jp, jm, j2 = idx[ab]
            arrived(gv(ab, im, jm), ag_recv.at[ab, 7])
            arrived(gv(ab, ip, jp), ag_recv.at[ab, 9])
            arrived(gv(ab, i2, jm), ag_recv.at[ab, 6])
            arrived(gv(ab, i2, jp), ag_recv.at[ab, 10])
            snd(ab, 15, gv(ab, i2, jp), True, -1)
        for ab in range(2):
            i0, j0, ip, im, i2, jp, jm, j2 = idx[ab]
            arrived(gv(ab, i0, j2), ag_recv.at[ab, 12])
            arrived(gv(ab, ip, j2), ag_recv.at[ab, 13])
            arrived(gv(ab, im, j2), ag_recv.at[ab, 14])
            arrived(gv(ab, i2, j2), ag_recv.at[ab, 15])

    def put(src, dst, k):
        pltpu.make_async_copy(src, dst, o_sem.at[k]).start()

    def put_wait(src, dst, k):
        pltpu.make_async_copy(src, dst, o_sem.at[k]).wait()

    stage_a(0)
    down_start(0)
    for h in range(2):
        dd[h, HB:HP, :] = jnp.zeros((HP - HB, D), BF)
    for r in range(4):
        xcp[r].wait()
        for k in range(4):
            nx[r, k] = norm_rows(nx[r, k])
    for i in range(4):
        chain(0, i)
    down_mid(0)
    stage_a(1)
    for i in range(4, 8):
        chain(0, i)
    down_end(0)
    chain_other(0)
    put(gu.at[0], gu1_o, 0)
    put(dd.at[0, pl.ds(0, HB)], d1_o, 1)

    gate_up(nx, 0)
    rs_first(0)
    for i in range(2):
        chain(1, i)
    rs_second(0)
    for i in range(2, 8):
        chain(1, i)
    down_start(1)
    rs_third(0)
    chain_other(1)
    down_mid(1)
    branch = rs_fourth(0)
    own_in.wait()
    m = (xown[...].astype(F32) + 0.5 * branch).astype(BF)
    mid[...] = m
    ng[z, x] = norm_rows(m)
    ag()
    down_end(1)
    put(gu.at[1], gu2_o, 2)
    put(dd.at[1, pl.ds(0, HB)], d2_o, 3)

    gate_up(ng, 1)
    rs_first(1)
    rs_second(1)
    rs_third(1)
    branch = rs_fourth(1)
    ost[...] = (mid[...].astype(F32) + 0.5 * branch).astype(BF)
    put(ost, ps_o, 4)

    drain()
    put_wait(gu.at[0], gu1_o, 0)
    put_wait(dd.at[0, pl.ds(0, HB)], d1_o, 1)
    put_wait(gu.at[1], gu2_o, 2)
    put_wait(dd.at[1, pl.ds(0, HB)], d2_o, 3)
    put_wait(ost, ps_o, 4)


def run(xin, wt, dn):
    vm = pltpu.VMEM
    dma = pltpu.SemaphoreType.DMA
    out_shape = (
        jax.ShapeDtypeStruct((D, 2 * HP), BF),
        jax.ShapeDtypeStruct((D, 2 * HP), BF),
        jax.ShapeDtypeStruct((HB, D), BF),
        jax.ShapeDtypeStruct((HB, D), BF),
        jax.ShapeDtypeStruct((64, D), BF),
    )
    scratch = [
        vm((4, 4, 64, D), BF), vm((4, 4, 64, D), BF), vm((64, D), BF), vm((64, D), BF),
        vm((2, D, 2 * HP), BF), vm((2, HP, D), BF), vm((4, 4, 64, HP), BF), vm((2, 4, 4, 64, D), BF),
        vm((2, 2, 2, 2, 64, 1024), BF), vm((2, 2, 4, 64, 1024), BF), vm((2, 2, 4, 64, 1024), BF),
        vm((2, 2, 2, 2, 64, 1024), BF), vm((2, 4, 64, 1024), F32), vm((2, 2, 4, 64, 1024), BF),
        vm((2, 2, 2, 32, 1024), BF), vm((2, 2, 64, 1024), BF), vm((2, 2, 64, 1024), BF),
        vm((2, 2, 2, 32, 1024), BF), vm((64, D), BF),
        dma((2, 16)), dma((2, 2)), dma((2, 8)), dma((2, 8)), dma((2, 8, 2)), dma((2, 14)), dma((2,)),
        dma((2, 2, 2, 6)), dma((2, 2, 2, 6)), dma((2, 16)), dma((2, 16)), dma((5,)), dma((5,)),
    ]
    return pl.pallas_call(
        kernel,
        out_shape=out_shape,
        in_specs=[
            pl.BlockSpec(memory_space=pl.ANY),
            pl.BlockSpec(memory_space=pltpu.VMEM),
            pl.BlockSpec(memory_space=pltpu.VMEM),
        ],
        out_specs=tuple(pl.BlockSpec(memory_space=pl.ANY) for _ in range(5)),
        scratch_shapes=scratch,
        compiler_params=pltpu.CompilerParams(has_side_effects=True, vmem_limit_bytes=62 * 1024 * 1024),
    )(xin, wt, dn)


def tiles(gain, gate, up):
    def one(w):
        v = (gain[:, None] * w).astype(BF).reshape(128, 2, HB).transpose(1, 0, 2)
        return jnp.pad(v, ((0, 0), (0, 0), (0, HP - HB)))

    return jnp.concatenate([one(gate), one(up)], axis=-1)


def per_device(
    prompts, gain_first, gate_first, up_first, down_first, gain_second, gate_second, up_second, down_second
):
    wt = jnp.stack([tiles(gain_first, gate_first, up_first), tiles(gain_second, gate_second, up_second)])
    dn = jnp.stack([down_first.astype(BF), down_second.astype(BF)])
    xin = prompts.reshape(4, 4, 64, D)
    gu1, gu2, d1, d2, ps = run(xin, wt, dn)
    return (
        gu1[:, :HB], gu1[:, HP:HP + HB], d1,
        gu2[:, :HB], gu2[:, HP:HP + HB], d2,
        ps.reshape(1, 64, D),
    )


def solution(mesh):
    w = P("fs", "tp")
    return jax.shard_map(
        per_device,
        mesh=mesh,
        in_specs=(P("tp", None, None), P("fs"), w, w, w, P("fs"), w, w, w),
        out_specs=(
            P(None, "fs"), P(None, "fs"), P("fs", None),
            P(None, "fs"), P(None, "fs"), P("fs", None),
            P("tp", "fs", None),
        ),
        check_vma=False,
    )
```

```python
import functools

import jax
import jax.numpy as jnp
from jax import lax
from jax.experimental import pallas as pl
from jax.experimental.pallas import tpu as pltpu
from jax.sharding import PartitionSpec as P

D = 2048
FF = 5632
HB = 352
HP = 384
TOK = 1024
MESH = pl.DeviceIdType.MESH
BF = jnp.bfloat16
F32 = jnp.float32
VMEM_MB = 48
NA = 1152


def rem4(v):
    return lax.rem(v, 4)


def kernel(
    x_hbm, gn1, gt1, ut1, dn1, gn2, gt2, ut2, dn2,
    g1_o, u1_o, d1_o, g2_o, u2_o, d2_o, ps_o,
    nx, ng, xown, mid, raw_w, raw_d, raw_g, wt, dn, gu, dd, act, act2, part, part2,
    r2, ra, rb, tt, acc, sb, q2, qa, qb, qt, ost,
    r2a, raa, rba, ta, acca, sba, rpa, rzb, accb, sbb, r2b, qab, qbb, tb_,
    a_send, w_recv, w_send, d_recv, d_send, d_loc, dp_send, dp_recv,
    rs_send, rs_recv, ag_send, ag_recv, t_send, t_recv, x_sem, i_sem, o_sem,
):
    f = lax.axis_index("fs")
    t = lax.axis_index("tp")
    z = lax.div(f, 4)
    x = lax.rem(f, 4)
    y = lax.div(t, 2)
    core = lax.rem(t, 2)
    sib = (f, 2 * y + 1 - core)
    pending = []

    def send(src, dst, ssem, rsem, dev, cond=None):
        cp = pltpu.make_async_remote_copy(
            src_ref=src, dst_ref=dst, send_sem=ssem, recv_sem=rsem, device_id=dev, device_id_type=MESH
        )
        if cond is None:
            cp.start()
        else:
            pl.when(cond)(cp.start)
        pending.append((cp, cond))

    def drain():
        for cp, cond in pending:
            if cond is None:
                cp.wait_send()
            else:
                pl.when(cond)(cp.wait_send)
        pending.clear()

    def arrived(dst, sem):
        pltpu.make_async_copy(dst, dst, sem).wait()

    barrier = pltpu.get_barrier_semaphore()

    def greet(dev):
        pl.semaphore_signal(barrier, inc=1, device_id=dev, device_id_type=MESH)

    near = [(f, 2 * rem4(y + 1) + core), (f, 2 * rem4(y + 3) + core), sib]
    near += [(4 * z + rem4(x + 1), t), (4 * z + rem4(x + 3), t), (4 * rem4(z + 1) + x, t), (4 * rem4(z + 3) + x, t)]
    for dev in near:
        greet(dev)
    n_self = jnp.int32(0)
    for g, b in ((0, 0), (1, 0), (0, 1), (1, 1)):
        to = (4 * (3 - y if b else y) + 2 * core + g, 2 * x + lax.div(z, 2))
        fro = (4 * (2 * core + g) + y, 2 * (3 - z if b else z) + lax.div(x, 2))
        to_self = jnp.logical_and(to[0] == f, to[1] == t)
        fro_self = jnp.logical_and(fro[0] == f, fro[1] == t)
        pl.when(jnp.logical_not(to_self))(functools.partial(greet, to))
        pl.when(jnp.logical_not(fro_self))(functools.partial(greet, fro))
        n_self = n_self + to_self.astype(jnp.int32) + fro_self.astype(jnp.int32)

    icp = []
    for h, (gn, gt, ut, dw) in enumerate(((gn1, gt1, ut1, dn1), (gn2, gt2, ut2, dn2))):
        for k, (src, dst) in enumerate(
            ((gn, raw_g.at[h]), (gt, raw_w.at[h, 0]), (ut, raw_w.at[h, 1]), (dw, raw_d.at[h]))
        ):
            cp = pltpu.make_async_copy(src, dst, i_sem.at[h, k])
            cp.start()
            icp.append(cp)
    xcp = []
    for r in range(4):
        cp = pltpu.make_async_copy(x_hbm.at[r], nx.at[r], x_sem.at[r])
        cp.start()
        xcp.append(cp)
    own_in = pltpu.make_async_copy(x_hbm.at[z, x], xown, x_sem.at[4])
    own_in.start()

    yp, ym, y2 = rem4(y + 1), rem4(y + 3), rem4(y + 2)

    def tile_id(yy, cc, q):
        return 4 * (2 * cc + q) + yy

    def wv(h, ft):
        return gu.at[h, :, pl.ds(0, HB), pl.ds(pl.multiple_of(ft * 128, 128), 128)]

    a_dt = 2 * x + lax.div(z, 2)

    def stage_a(h):
        for g in range(2):
            src = wt.at[h, :, pl.ds(HB * g, HB), :]
            for slot in ((0,), (1, 2))[h]:
                df = 4 * (3 - y if slot == 2 else y) + 2 * core + g
                same = jnp.logical_and(df == f, a_dt == t)
                send(src, wv(slot, f), a_send.at[slot, g], w_recv.at[slot, f], (df, a_dt), jnp.logical_not(same))

                @pl.when(same)
                def _(src=src, slot=slot):
                    pltpu.make_async_copy(src, wv(slot, f), w_recv.at[slot, f]).start()

    def wsend(h, ft, k, dev):
        send(wv(h, ft), wv(h, ft), w_send.at[h, k], w_recv.at[h, ft], dev)

    up_dev, dn_dev = (f, 2 * yp + core), (f, 2 * ym + core)

    def w_own(h):
        for q in range(2):
            ft = tile_id(y, core, q)
            arrived(wv(h, ft), w_recv.at[h, ft])
            wsend(h, ft, 3 * q, up_dev)
            wsend(h, ft, 3 * q + 1, dn_dev)
            wsend(h, ft, 3 * q + 2, sib)

    def w_fwd(h):
        lo, hi = tile_id(ym, core, 0), tile_id(yp, core, 1)
        arrived(wv(h, lo), w_recv.at[h, lo])
        wsend(h, lo, 6, up_dev)
        arrived(wv(h, hi), w_recv.at[h, hi])
        wsend(h, hi, 7, dn_dev)
        wsend(h, lo, 8, sib)
        wsend(h, hi, 9, sib)

    def w_more(h):
        for k, ft in ((10, tile_id(ym, core, 1)), (11, tile_id(yp, core, 0))):
            arrived(wv(h, ft), w_recv.at[h, ft])
            wsend(h, ft, k, sib)
        for q in range(2):
            ft = tile_id(y2, core, q)
            arrived(wv(h, ft), w_recv.at[h, ft])
            wsend(h, ft, 12 + q, sib)

    def w_end(h):
        for yy in range(4):
            for q in range(2):
                ft = tile_id(yy, 1 - core, q)
                arrived(wv(h, ft), w_recv.at[h, ft])

    def dblk(h, tb, q):
        return dd.at[h, pl.ds(176 * q, 176), pl.ds(pl.multiple_of(tb * 256, 256), 256)]

    def d_local(h):
        return pltpu.make_async_copy(
            dn.at[h], dd.at[h, pl.ds(0, HB), pl.ds(pl.multiple_of(t * 256, 256), 256)], d_loc.at[h]
        )

    def dsend(h, tb, q, k, dev):
        send(dblk(h, tb, q), dblk(h, tb, q), d_send.at[h, k], d_recv.at[h, tb, q], dev)

    def d_own(h):
        if h < 2:
            d_local(h).start()
        else:
            arrived(dcols, dp_recv)
        for q in range(2):
            src = dn.at[h, pl.ds(176 * q, 176), :] if h < 2 else dblk(2, t, q)
            for j, dev in enumerate((up_dev, dn_dev, sib)):
                send(src, dblk(h, t, q), d_send.at[h, 3 * q + j], d_recv.at[h, t, q], dev)

    dcols = dd.at[2, pl.ds(0, HB), pl.ds(pl.multiple_of(t * 256, 256), 256)]

    def d_partner():
        send(dn.at[1], dcols, dp_send, dp_recv, (4 * (3 - z) + x, t))

    def d_fwd(h):
        tm, tp = 2 * ym + core, 2 * yp + core
        arrived(dblk(h, tm, 0), d_recv.at[h, tm, 0])
        dsend(h, tm, 0, 6, up_dev)
        arrived(dblk(h, tp, 1), d_recv.at[h, tp, 1])
        dsend(h, tp, 1, 7, dn_dev)
        dsend(h, tm, 0, 8, sib)
        dsend(h, tp, 1, 9, sib)

    def d_more(h):
        for k, tb, q in ((10, 2 * ym + core, 1), (11, 2 * yp + core, 0), (12, 2 * y2 + core, 0), (13, 2 * y2 + core, 1)):
            arrived(dblk(h, tb, q), d_recv.at[h, tb, q])
            dsend(h, tb, q, k, sib)

    def d_end(h):
        for yy in range(4):
            for q in range(2):
                tb = 2 * yy + 1 - core
                arrived(dblk(h, tb, q), d_recv.at[h, tb, q])
        if h < 2:
            d_local(h).wait()

    def norm_rows(v):
        w = v.astype(F32)
        return (w * lax.rsqrt(jnp.mean(w * w, axis=-1, keepdims=True) + 1e-06)).astype(BF)

    def gate_up(rows, slot):
        w = gu[slot].reshape(2 * HP, D)
        v = lax.dot_general(rows, w, (((1,), (1,)), ((), ())), preferred_element_type=F32)
        gt = v[:, :HP]
        return (gt * jax.nn.sigmoid(gt) * v[:, HP:]).astype(BF)

    def first_act():
        @pl.loop(0, 4)
        def _(r):
            act[r] = gate_up(nx[r].reshape(256, D), 0).reshape(4, 64, HP)

    def second_act():
        @pl.loop(0, 2)
        def _(r):
            rows = ng[r].reshape(256, D)
            for b in range(2):
                act2[r, :, :, HP * b:HP * (b + 1)] = gate_up(rows, 1 + b).reshape(4, 64, HP)

    def colsl(ab):
        return pl.ds(1024 * ab, 1024)

    def pv(h, ab, idx, q):
        if ab == 0:
            return part.at[h, pl.ds(2 * q, 2), idx, :, colsl(0)]
        return part.at[h, idx, pl.ds(2 * q, 2), :, colsl(1)]

    def dev1(ab, step):
        if ab == 0:
            return (4 * z + rem4(x + step + 4), t)
        return (4 * rem4(z + step + 4) + x, t)

    def me1(ab, step):
        return rem4((x if ab == 0 else z) + step + 4)

    def down_chunk(h, ab, idx):
        w = dd[h, :, 1024 * ab:1024 * ab + 1024]
        if ab == 0:
            a = act[:, pl.ds(idx, 1)].reshape(256, HP)
        else:
            a = act[idx].reshape(256, HP)
        v = jnp.dot(a, w, preferred_element_type=F32).astype(BF)
        if ab == 0:
            part[h, :, pl.ds(idx, 1), :, 0:1024] = v.reshape(4, 1, 64, 1024)
        else:
            part[h, idx, :, :, 1024:2048] = v.reshape(4, 64, 1024)

    def s1(h, ab, k, src, dst, step):
        send(src, dst, rs_send.at[h, 0, ab, k], rs_recv.at[h, 0, ab, k], dev1(ab, step))

    def s2(h, ab, k, src, dst, step):
        send(src, dst, rs_send.at[h, 1, ab, k], rs_recv.at[h, 1, ab, k], dev1(1 - ab, step))

    def rs_first(h, between=None):
        for ab in range(2):
            i2 = me1(ab, 2)
            down_chunk(h, ab, i2)
            s1(h, ab, 0, pv(h, ab, i2, 0), r2.at[h, ab, 0], 1)
            s1(h, ab, 1, pv(h, ab, i2, 1), r2.at[h, ab, 1], -1)
        for ab in range(2):
            ip = me1(ab, 1)
            down_chunk(h, ab, ip)
            s1(h, ab, 3, pv(h, ab, ip, 1), ra.at[h, ab, pl.ds(2, 2)], 1)
        for ab in range(2):
            im = me1(ab, -1)
            down_chunk(h, ab, im)
            s1(h, ab, 4, pv(h, ab, im, 0), rb.at[h, ab, pl.ds(0, 2)], -1)
        for ab in range(2):
            down_chunk(h, ab, me1(ab, 0))

    def rs_second(h):
        for ab in range(2):
            arrived(r2.at[h, ab, 0], rs_recv.at[h, 0, ab, 0])
            tt[h, ab, 0] = (r2[h, ab, 0].astype(F32) + pv(h, ab, me1(ab, 1), 0)[...].astype(F32)).astype(BF)
            s1(h, ab, 2, tt.at[h, ab, 0], ra.at[h, ab, pl.ds(0, 2)], 1)
            arrived(r2.at[h, ab, 1], rs_recv.at[h, 0, ab, 1])
            tt[h, ab, 1] = (r2[h, ab, 1].astype(F32) + pv(h, ab, me1(ab, -1), 1)[...].astype(F32)).astype(BF)
            s1(h, ab, 5, tt.at[h, ab, 1], rb.at[h, ab, pl.ds(2, 2)], -1)

    def rs_third(h):
        for ab in range(2):
            for q in range(2):
                sl = pl.ds(2 * q, 2)
                arrived(ra.at[h, ab, sl], rs_recv.at[h, 0, ab, 2 + q])
                arrived(rb.at[h, ab, sl], rs_recv.at[h, 0, ab, 4 + q])
                s = (
                    pv(h, ab, me1(ab, 0), q)[...].astype(F32)
                    + ra[h, ab, 2 * q:2 * q + 2].astype(F32)
                    + rb[h, ab, 2 * q:2 * q + 2].astype(F32)
                )
                acc[ab, 2 * q:2 * q + 2] = s
                sb[h, ab, 2 * q:2 * q + 2] = s.astype(BF)
            i2, ip, im = me1(1 - ab, 2), me1(1 - ab, 1), me1(1 - ab, -1)
            s2(h, ab, 0, sb.at[h, ab, i2, pl.ds(0, 32)], q2.at[h, ab, 0], 1)
            s2(h, ab, 1, sb.at[h, ab, i2, pl.ds(32, 32)], q2.at[h, ab, 1], -1)
            s2(h, ab, 3, sb.at[h, ab, ip, pl.ds(32, 32)], qa.at[h, ab, pl.ds(32, 32)], 1)
            s2(h, ab, 4, sb.at[h, ab, im, pl.ds(0, 32)], qb.at[h, ab, pl.ds(0, 32)], -1)

    def rs_fourth(h):
        for ab in range(2):
            ip, im = me1(1 - ab, 1), me1(1 - ab, -1)
            arrived(q2.at[h, ab, 0], rs_recv.at[h, 1, ab, 0])
            qt[h, ab, 0] = (q2[h, ab, 0].astype(F32) + acc[ab, ip, 0:32]).astype(BF)
            s2(h, ab, 2, qt.at[h, ab, 0], qa.at[h, ab, pl.ds(0, 32)], 1)
            arrived(q2.at[h, ab, 1], rs_recv.at[h, 1, ab, 1])
            qt[h, ab, 1] = (q2[h, ab, 1].astype(F32) + acc[ab, im, 32:64]).astype(BF)
            s2(h, ab, 5, qt.at[h, ab, 1], qb.at[h, ab, pl.ds(32, 32)], -1)
        out = []
        for ab in range(2):
            for q in range(2):
                arrived(qa.at[h, ab, pl.ds(32 * q, 32)], rs_recv.at[h, 1, ab, 2 + q])
                arrived(qb.at[h, ab, pl.ds(32 * q, 32)], rs_recv.at[h, 1, ab, 4 + q])
            out.append(acc[ab, me1(1 - ab, 0)] + qa[h, ab].astype(F32) + qb[h, ab].astype(F32))
        return jnp.concatenate(out, axis=-1)

    zz = lax.rem(z, 2)
    zo = 1 - zz
    pair = (4 * (z + 1 - 2 * zz) + x, t)
    xp, xm, x2 = rem4(x + 1), rem4(x + 3), rem4(x + 2)
    xp_dev, xm_dev = (4 * z + xp, t), (4 * z + xm, t)
    CA, CB = pl.ds(0, NA), pl.ds(NA, D - NA)
    lo, hi = pl.ds(0, 32), pl.ds(32, 32)

    def gv(i, j, cols, rows=slice(None)):
        return ng.at[i, j, rows, cols]

    def gsend(k, ref, dev):
        send(ref, ref, ag_send.at[k], ag_recv.at[k], dev)

    def ag_a():
        gsend(1, gv(zz, x, CA), xp_dev)
        gsend(2, gv(zz, x, CA), xm_dev)
        gsend(7, gv(zz, x, CB), xp_dev)
        gsend(8, gv(zz, x, CB), xm_dev)
        gsend(0, gv(zz, x, CA), pair)
        gsend(9, gv(zz, x, CB), pair)

    def ag_b():
        arrived(gv(zo, x, CA), ag_recv.at[0])
        gsend(3, gv(zo, x, CA), xp_dev)
        gsend(4, gv(zo, x, CA), xm_dev)
        arrived(gv(zz, xm, CA), ag_recv.at[1])
        gsend(5, gv(zz, xm, CA), xp_dev)
        arrived(gv(zz, xm, CB), ag_recv.at[7])
        gsend(10, gv(zz, xm, CB, lo), xp_dev)
        gsend(12, gv(zz, xm, CB), pair)
        arrived(gv(zz, xp, CB), ag_recv.at[8])
        gsend(11, gv(zz, xp, CB, hi), xm_dev)
        gsend(13, gv(zz, xp, CB), pair)
        arrived(gv(zo, xp, CA), ag_recv.at[4])
        gsend(6, gv(zo, xp, CA), xm_dev)
        arrived(gv(zz, x2, CB, lo), ag_recv.at[10])
        arrived(gv(zz, x2, CB, hi), ag_recv.at[11])
        gsend(14, gv(zz, x2, CB), pair)

    def ag_c():
        for k, i, j, c in (
            (2, zz, xp, CA), (3, zo, xm, CA), (5, zz, x2, CA), (6, zo, x2, CA),
            (9, zo, x, CB), (12, zo, xm, CB), (13, zo, xp, CB), (14, zo, x2, CB),
        ):
            arrived(gv(i, j, c), ag_recv.at[k])

    def down2_a(xi):
        w = dd[1:3, :, 0:NA].reshape(2 * HP, NA)
        v = jnp.dot(act2[:, pl.ds(xi, 1)].reshape(128, 2 * HP), w, preferred_element_type=F32).astype(BF)
        part2[:, pl.ds(xi, 1), :, 0:NA] = v.reshape(2, 1, 64, NA)

    def down2_b(zi):
        w = dd[1:3, :, NA:D].reshape(2 * HP, D - NA)
        v = jnp.dot(act2[zi].reshape(256, 2 * HP), w, preferred_element_type=F32).astype(BF)
        part2[zi, :, :, NA:D] = v.reshape(4, 64, D - NA)

    def tsend(k, src, dst, dev):
        send(src, dst, t_send.at[k], t_recv.at[k], dev)

    def rs2():
        down2_b(zo)
        for k, xi in enumerate((x2, xp, xm, x)):
            tsend(k, part2.at[zo, xi, :, CB], rzb.at[xi], pair)
        down2_a(x2)
        tsend(4, part2.at[0, x2, :, CA], r2a.at[0], xp_dev)
        tsend(5, part2.at[1, x2, :, CA], r2a.at[1], xm_dev)
        down2_a(xp)
        tsend(6, part2.at[1, xp, :, CA], raa.at[1], xp_dev)
        down2_a(xm)
        tsend(7, part2.at[0, xm, :, CA], rba.at[0], xm_dev)
        down2_b(zz)
        down2_a(x)

        def fold_b(k, xi):
            arrived(rzb.at[xi], t_recv.at[k])
            s = part2[zz, xi, :, NA:D].astype(F32) + rzb[xi].astype(F32)
            accb[xi] = s
            sbb[xi] = s.astype(BF)

        fold_b(0, x2)
        tsend(8, sbb.at[x2, lo], r2b.at[0], xp_dev)
        tsend(9, sbb.at[x2, hi], r2b.at[1], xm_dev)
        arrived(r2a.at[0], t_recv.at[4])
        ta[0] = (r2a[0].astype(F32) + part2[0, xp, :, 0:NA].astype(F32)).astype(BF)
        tsend(10, ta.at[0], raa.at[0], xp_dev)
        arrived(r2a.at[1], t_recv.at[5])
        ta[1] = (r2a[1].astype(F32) + part2[1, xm, :, 0:NA].astype(F32)).astype(BF)
        tsend(11, ta.at[1], rba.at[1], xm_dev)
        fold_b(1, xp)
        tsend(12, sbb.at[xp, hi], qab.at[hi], xp_dev)
        fold_b(2, xm)
        tsend(13, sbb.at[xm, lo], qbb.at[lo], xm_dev)
        arrived(r2b.at[0], t_recv.at[8])
        tb_[0] = (r2b[0].astype(F32) + accb[xp, 0:32]).astype(BF)
        tsend(14, tb_.at[0], qab.at[lo], xp_dev)
        arrived(r2b.at[1], t_recv.at[9])
        tb_[1] = (r2b[1].astype(F32) + accb[xm, 32:64]).astype(BF)
        tsend(15, tb_.at[1], qbb.at[hi], xm_dev)
        fold_b(3, x)
        arrived(raa.at[1], t_recv.at[6])
        arrived(rba.at[0], t_recv.at[7])
        arrived(raa.at[0], t_recv.at[10])
        arrived(rba.at[1], t_recv.at[11])
        s = part2[zo, x, :, 0:NA].astype(F32) + raa[zo].astype(F32) + rba[zo].astype(F32)
        sba[...] = s.astype(BF)
        tsend(16, sba, rpa, pair)
        own_a = part2[zz, x, :, 0:NA].astype(F32) + raa[zz].astype(F32) + rba[zz].astype(F32)
        arrived(qab.at[hi], t_recv.at[12])
        arrived(qbb.at[lo], t_recv.at[13])
        arrived(qab.at[lo], t_recv.at[14])
        arrived(qbb.at[hi], t_recv.at[15])
        own_b = accb[x] + qab[...].astype(F32) + qbb[...].astype(F32)
        ost[:, NA:D] = (mid[:, NA:D].astype(F32) + 0.5 * own_b).astype(BF)
        arrived(rpa, t_recv.at[16])
        ost[:, 0:NA] = (mid[:, 0:NA].astype(F32) + 0.5 * (own_a + rpa[...].astype(F32))).astype(BF)

    def put(src, dst, k):
        pltpu.make_async_copy(src, dst, o_sem.at[k]).start()

    def put_wait(src, dst, k):
        pltpu.make_async_copy(src, dst, o_sem.at[k]).wait()

    def fold(h):
        for k in range(4):
            icp[4 * h + k].wait()
        for k in range(2):
            wt[h, k] = (raw_g[h] * raw_w[h, k]).astype(BF)
        dn[h] = raw_d[h].astype(BF)

    def norm_first(r):
        xcp[r].wait()
        for k in range(4):
            nx[r, k] = norm_rows(nx[r, k])

    fold(0)
    pl.semaphore_wait(barrier, 15 - n_self)
    stage_a(0)
    d_own(0)
    for s_ in range(3):
        dd[s_, HB:HP, :] = jnp.zeros((HP - HB, D), BF)
        for k in range(2):
            gu[s_, k, HB:HP, :] = jnp.zeros((HP - HB, D), BF)
    for r in range(4):
        norm_first(r)
    fold(1)
    w_own(0)
    d_fwd(0)
    w_fwd(0)
    stage_a(1)
    d_partner()
    d_more(0)
    w_more(0)
    w_end(0)
    put(gu.at[0, 0, pl.ds(0, HB)], g1_o, 0)
    put(gu.at[0, 1, pl.ds(0, HB)], u1_o, 1)

    first_act()
    d_end(0)
    put(dd.at[0, pl.ds(0, HB)], d1_o, 2)
    rs_first(0)
    w_own(1)
    w_own(2)
    rs_second(0)
    d_own(1)
    d_own(2)
    rs_third(0)
    branch = rs_fourth(0)
    own_in.wait()
    m = (xown[...].astype(F32) + 0.5 * branch).astype(BF)
    mid[...] = m
    ng[zz, x] = norm_rows(m)
    ag_a()
    w_fwd(1)
    w_fwd(2)
    ag_b()
    d_fwd(1)
    d_fwd(2)
    for s_ in range(1, 3):
        w_more(s_)
        d_more(s_)
    ag_c()
    for s_ in range(1, 3):
        w_end(s_)
    put(gu.at[1, 0, pl.ds(0, HB)], g2_o, 3)
    put(gu.at[1, 1, pl.ds(0, HB)], u2_o, 4)
    second_act()
    for s_ in range(1, 3):
        d_end(s_)
    put(dd.at[1, pl.ds(0, HB)], d2_o, 5)
    rs2()
    put(ost, ps_o, 6)

    drain()
    put_wait(gu.at[0, 0, pl.ds(0, HB)], g1_o, 0)
    put_wait(gu.at[0, 1, pl.ds(0, HB)], u1_o, 1)
    put_wait(dd.at[0, pl.ds(0, HB)], d1_o, 2)
    put_wait(gu.at[1, 0, pl.ds(0, HB)], g2_o, 3)
    put_wait(gu.at[1, 1, pl.ds(0, HB)], u2_o, 4)
    put_wait(dd.at[1, pl.ds(0, HB)], d2_o, 5)
    put_wait(ost, ps_o, 6)


def copy_out(*refs):
    n = len(refs) // 2
    sems = refs[-1]
    cps = [pltpu.make_async_copy(refs[k], refs[n + k], sems.at[k]) for k in range(n)]
    for cp in cps:
        cp.start()
    for cp in cps:
        cp.wait()


def run(xin, *weights):
    vm = pltpu.VMEM
    dma = pltpu.SemaphoreType.DMA
    w_out = jax.ShapeDtypeStruct((HB, D), BF)
    out_shape = (w_out,) * 6 + (jax.ShapeDtypeStruct((64, D), BF),)
    NB = D - NA
    scratch = [
        vm((4, 4, 64, D), BF), vm((2, 4, 64, D), BF), vm((64, D), BF), vm((64, D), BF),
        vm((2, 2, 2 * HB, 128), F32), vm((2, HB, 256), F32), vm((2, 1, 128), F32),
        vm((2, 2, 2 * HB, 128), BF), vm((2, HB, 256), BF),
        vm((3, 2, HP, D), BF), vm((3, HP, D), BF), vm((4, 4, 64, HP), BF), vm((2, 4, 64, 2 * HP), BF),
        vm((1, 4, 4, 64, D), BF), vm((2, 4, 64, D), BF),
        vm((1, 2, 2, 2, 64, 1024), BF), vm((1, 2, 4, 64, 1024), BF), vm((1, 2, 4, 64, 1024), BF),
        vm((1, 2, 2, 2, 64, 1024), BF), vm((2, 4, 64, 1024), F32), vm((1, 2, 4, 64, 1024), BF),
        vm((1, 2, 2, 32, 1024), BF), vm((1, 2, 64, 1024), BF), vm((1, 2, 64, 1024), BF),
        vm((1, 2, 2, 32, 1024), BF), vm((64, D), BF),
        vm((2, 64, NA), BF), vm((2, 64, NA), BF), vm((2, 64, NA), BF), vm((2, 64, NA), BF),
        vm((2, 64, NA), F32), vm((64, NA), BF), vm((64, NA), BF),
        vm((4, 64, NB), BF), vm((4, 64, NB), F32), vm((4, 64, NB), BF),
        vm((2, 32, NB), BF), vm((64, NB), BF), vm((64, NB), BF), vm((2, 32, NB), BF),
        dma((3, 2)), dma((3, 16)), dma((3, 14)), dma((3, 8, 2)), dma((3, 14)), dma((2,)), dma, dma,
        dma((1, 2, 2, 6)), dma((1, 2, 2, 6)), dma((15,)), dma((15,)), dma((17,)), dma((17,)),
        dma((5,)), dma((2, 4)), dma((7,)),
    ]
    here = [pltpu.with_memory_space_constraint(v, pltpu.HBM) for v in (xin, *weights)]
    outs = pl.pallas_call(
        kernel,
        out_shape=tuple(pltpu.VMEM(o.shape, o.dtype) for o in out_shape),
        in_specs=[pl.BlockSpec(memory_space=pltpu.HBM)] * 9,
        out_specs=tuple(pl.BlockSpec(memory_space=pl.ANY) for _ in range(7)),
        scratch_shapes=scratch,
        compiler_params=pltpu.CompilerParams(
            collective_id=0, has_side_effects=True, vmem_limit_bytes=VMEM_MB * 1024 * 1024
        ),
    )(*here)
    return pl.pallas_call(
        copy_out,
        out_shape=out_shape,
        in_specs=[pl.BlockSpec(memory_space=pl.ANY)] * 7,
        out_specs=tuple(pl.BlockSpec(memory_space=pltpu.HBM) for _ in range(7)),
        scratch_shapes=[dma((7,))],
        compiler_params=pltpu.CompilerParams(vmem_limit_bytes=1024 * 1024),
    )(*outs)


def per_device(
    prompts, gain_first, gate_first, up_first, down_first, gain_second, gate_second, up_second, down_second
):
    xin = prompts.reshape(4, 4, 64, D)
    g1, u1, d1, g2, u2, d2, ps = run(
        xin,
        gain_first.reshape(1, 128), gate_first.T, up_first.T, down_first,
        gain_second.reshape(1, 128), gate_second.T, up_second.T, down_second,
    )
    return g1.T, u1.T, d1, g2.T, u2.T, d2, ps.reshape(1, 64, D)


def solution(mesh):
    w = P("fs", "tp")
    return jax.shard_map(
        per_device,
        mesh=mesh,
        in_specs=(P("tp", None, None), P("fs"), w, w, w, P("fs"), w, w, w),
        out_specs=(
            P(None, "fs"), P(None, "fs"), P("fs", None),
            P(None, "fs"), P(None, "fs"), P("fs", None),
            P("tp", "fs", None),
        ),
        check_vma=False,
    )
```

```python
import functools

import jax
import jax.numpy as jnp
from jax import lax
from jax.experimental import pallas as pl
from jax.experimental.pallas import tpu as pltpu
from jax.sharding import PartitionSpec as P

D = 2048
FF = 5632
HB = 352
HP = 384
TOK = 1024
MESH = pl.DeviceIdType.MESH
BF = jnp.bfloat16
F32 = jnp.float32
VMEM_MB = 48
NA = 1152


def rem4(v):
    return lax.rem(v, 4)


def kernel(
    x_hbm, gn1, gt1, ut1, dn1, gn2, gt2, ut2, dn2,
    g1_o, u1_o, d1_o, g2_o, u2_o, d2_o, ps_o,
    nx, ng, xown, mid, raw_w, raw_d, raw_g, wt, dn, gu, dd, act, act2, part, part2,
    r2, ra, rb, tt, acc, sb, q2, qa, qb, qt, ost,
    r2a, raa, rba, ta, acca, sba, rpa, rzb, accb, sbb, r2b, qab, qbb, tb_,
    a_send, w_recv, w_send, d_recv, d_send, d_loc, dp_send, dp_recv,
    rs_send, rs_recv, ag_send, ag_recv, t_send, t_recv, x_sem, i_sem, o_sem,
):
    f = lax.axis_index("fs")
    t = lax.axis_index("tp")
    z = lax.div(f, 4)
    x = lax.rem(f, 4)
    y = lax.div(t, 2)
    core = lax.rem(t, 2)
    sib = (f, 2 * y + 1 - core)
    pending = []

    def remote(src, dst, ssem, rsem, dev):
        return pltpu.make_async_remote_copy(
            src_ref=src, dst_ref=dst, send_sem=ssem, recv_sem=rsem, device_id=dev, device_id_type=MESH
        )

    def send(src, dst, ssem, rsem, dev, cond=None):
        if cond is None:
            remote(src, dst, ssem, rsem, dev).start()
        else:
            pl.when(cond)(lambda: remote(src, dst, ssem, rsem, dev).start())
        pending.append((src, dst, ssem, rsem, dev, cond))

    def drain():
        for *args, cond in pending:
            if cond is None:
                remote(*args).wait_send()
            else:
                pl.when(cond)(lambda args=args: remote(*args).wait_send())
        pending.clear()

    def arrived(dst, sem):
        pltpu.make_async_copy(dst, dst, sem).wait()

    barrier = pltpu.get_barrier_semaphore()

    def greet(dev):
        pl.semaphore_signal(barrier, inc=1, device_id=dev, device_id_type=MESH)

    near = [(f, 2 * rem4(y + 1) + core), (f, 2 * rem4(y + 3) + core), sib]
    near += [(4 * z + rem4(x + 1), t), (4 * z + rem4(x + 3), t), (4 * rem4(z + 1) + x, t), (4 * rem4(z + 3) + x, t)]
    for dev in near:
        greet(dev)
    n_self = jnp.int32(0)
    for g in range(2):
        to = (4 * y + 2 * core + g, 2 * x + lax.div(z, 2))
        fro = (4 * (2 * core + g) + y, 2 * z + lax.div(x, 2))
        to_self = jnp.logical_and(to[0] == f, to[1] == t)
        fro_self = jnp.logical_and(fro[0] == f, fro[1] == t)
        pl.when(jnp.logical_not(to_self))(functools.partial(greet, to))
        pl.when(jnp.logical_not(fro_self))(functools.partial(greet, fro))
        n_self = n_self + to_self.astype(jnp.int32) + fro_self.astype(jnp.int32)

    par = lax.rem(x + z, 2)
    for zd in (y, 3 - y):
        for g in range(2):
            to = (4 * zd + 2 * core + g, 2 * y + par)
            to_self = jnp.logical_and(to[0] == f, to[1] == t)
            pl.when(jnp.logical_not(to_self))(functools.partial(greet, to))
            n_self = n_self + to_self.astype(jnp.int32)
    n_fro = jnp.int32(0)
    for zs in (z, 3 - z):
        for z2 in range(4):
            for k in range(2):
                fr = (4 * z2 + 2 * k + lax.rem(z2 + core, 2), 2 * y + lax.div(x, 2))
                here = y == zs
                is_self = jnp.logical_and(fr[0] == f, fr[1] == t)
                pl.when(jnp.logical_and(here, jnp.logical_not(is_self)))(functools.partial(greet, fr))
                n_fro = n_fro + jnp.logical_and(here, jnp.logical_not(is_self)).astype(jnp.int32)

    icp = []
    for h, (gn, gt, ut, dw) in enumerate(((gn1, gt1, ut1, dn1), (gn2, gt2, ut2, dn2))):
        for k, (src, dst) in enumerate(
            ((gn, raw_g.at[h]), (gt, raw_w.at[h, 0]), (ut, raw_w.at[h, 1]), (dw, raw_d.at[h]))
        ):
            cp = pltpu.make_async_copy(src, dst, i_sem.at[h, k])
            cp.start()
            icp.append(cp)
    xcp = []
    for r in range(4):
        cp = pltpu.make_async_copy(x_hbm.at[r], nx.at[r], x_sem.at[r])
        cp.start()
        xcp.append(cp)
    own_in = pltpu.make_async_copy(x_hbm.at[z, x], xown, x_sem.at[4])
    own_in.start()

    yp, ym, y2 = rem4(y + 1), rem4(y + 3), rem4(y + 2)

    def tile_id(yy, cc, q):
        return 4 * (2 * cc + q) + yy

    def wv(h, ft):
        return gu.at[h, :, pl.ds(0, HB), pl.ds(pl.multiple_of(ft * 128, 128), 128)]

    a_dt = 2 * x + lax.div(z, 2)

    def tile_to(h, g, slot, dev):
        src = wt.at[h, :, pl.ds(HB * g, HB), :]
        same = jnp.logical_and(dev[0] == f, dev[1] == t)
        send(src, wv(slot, f), a_send.at[slot, g], w_recv.at[slot, f], dev, jnp.logical_not(same))

        @pl.when(same)
        def _():
            pltpu.make_async_copy(src, wv(slot, f), w_recv.at[slot, f]).start()

    def stage_a():
        for g in range(2):
            tile_to(0, g, 0, (4 * y + 2 * core + g, a_dt))

    def stage_a2():
        for g in range(2):
            for slot, zd in ((1, y), (2, 3 - y)):
                tile_to(1, g, slot, (4 * zd + 2 * core + g, 2 * y + par))

    dist = {}
    for slot, y0 in ((1, z), (2, 3 - z)):
        dist[slot] = rem4(jnp.where(core == 0, y - y0, y0 - y) + 4)
    nxt = (f, 2 * rem4(y + 1 + 2 * core) + core)

    def hop(d, batch):
        for slot in (1, 2):
            def go(slot=slot):
                for i in range(4 * batch, 4 * batch + 4):
                    z2, k = i // 2, i % 2
                    ft = 4 * z2 + 2 * k + lax.rem(z2 + core, 2)
                    tile = wv(slot, ft)
                    arrived(tile, w_recv.at[slot, ft])
                    if d < 3:
                        remote(tile, tile, w_send.at[slot, i], w_recv.at[slot, ft], nxt).start()
                    remote(tile, tile, w_send.at[slot, 8 + i], w_recv.at[slot, ft], sib).start()
            pl.when(dist[slot] == d)(go)

    def hop_end():
        for slot in (1, 2):
            for i in range(8):
                z2, k = i // 2, i % 2
                ft = 4 * z2 + 2 * k + lax.rem(z2 + core, 2)
                tile = wv(slot, ft)
                pending.append((tile, tile, w_send.at[slot, i], w_recv.at[slot, ft], nxt, dist[slot] < 3))
                pending.append((tile, tile, w_send.at[slot, 8 + i], w_recv.at[slot, ft], sib, None))
                fo = 4 * z2 + 2 * k + lax.rem(z2 + 1 - core, 2)
                arrived(wv(slot, fo), w_recv.at[slot, fo])

    def wsend(h, ft, k, dev):
        send(wv(h, ft), wv(h, ft), w_send.at[h, k], w_recv.at[h, ft], dev)

    up_dev, dn_dev = (f, 2 * yp + core), (f, 2 * ym + core)

    def w_own(h):
        for q in range(2):
            ft = tile_id(y, core, q)
            arrived(wv(h, ft), w_recv.at[h, ft])
            wsend(h, ft, 3 * q, up_dev)
            wsend(h, ft, 3 * q + 1, dn_dev)
            wsend(h, ft, 3 * q + 2, sib)

    def w_fwd(h):
        lo, hi = tile_id(ym, core, 0), tile_id(yp, core, 1)
        arrived(wv(h, lo), w_recv.at[h, lo])
        wsend(h, lo, 6, up_dev)
        arrived(wv(h, hi), w_recv.at[h, hi])
        wsend(h, hi, 7, dn_dev)
        wsend(h, lo, 8, sib)
        wsend(h, hi, 9, sib)

    def w_more(h):
        for k, ft in ((10, tile_id(ym, core, 1)), (11, tile_id(yp, core, 0))):
            arrived(wv(h, ft), w_recv.at[h, ft])
            wsend(h, ft, k, sib)
        for q in range(2):
            ft = tile_id(y2, core, q)
            arrived(wv(h, ft), w_recv.at[h, ft])
            wsend(h, ft, 12 + q, sib)

    def w_end(h):
        for yy in range(4):
            for q in range(2):
                ft = tile_id(yy, 1 - core, q)
                arrived(wv(h, ft), w_recv.at[h, ft])

    def dblk(h, tb, q):
        return dd.at[h, pl.ds(176 * q, 176), pl.ds(pl.multiple_of(tb * 256, 256), 256)]

    def d_local(h):
        return pltpu.make_async_copy(
            dn.at[h], dd.at[h, pl.ds(0, HB), pl.ds(pl.multiple_of(t * 256, 256), 256)], d_loc.at[h]
        )

    def dsend(h, tb, q, k, dev):
        send(dblk(h, tb, q), dblk(h, tb, q), d_send.at[h, k], d_recv.at[h, tb, q], dev)

    def d_own(h):
        if h < 2:
            d_local(h).start()
        else:
            arrived(dcols, dp_recv)
        for q in range(2):
            src = dn.at[h, pl.ds(176 * q, 176), :] if h < 2 else dblk(2, t, q)
            for j, dev in enumerate((up_dev, dn_dev, sib)):
                send(src, dblk(h, t, q), d_send.at[h, 3 * q + j], d_recv.at[h, t, q], dev)

    dcols = dd.at[2, pl.ds(0, HB), pl.ds(pl.multiple_of(t * 256, 256), 256)]

    def d_partner():
        send(dn.at[1], dcols, dp_send, dp_recv, (4 * (3 - z) + x, t))

    def d_fwd(h):
        tm, tp = 2 * ym + core, 2 * yp + core
        arrived(dblk(h, tm, 0), d_recv.at[h, tm, 0])
        dsend(h, tm, 0, 6, up_dev)
        arrived(dblk(h, tp, 1), d_recv.at[h, tp, 1])
        dsend(h, tp, 1, 7, dn_dev)
        dsend(h, tm, 0, 8, sib)
        dsend(h, tp, 1, 9, sib)

    def d_more(h):
        for k, tb, q in ((10, 2 * ym + core, 1), (11, 2 * yp + core, 0), (12, 2 * y2 + core, 0), (13, 2 * y2 + core, 1)):
            arrived(dblk(h, tb, q), d_recv.at[h, tb, q])
            dsend(h, tb, q, k, sib)

    def d_end(h):
        for yy in range(4):
            for q in range(2):
                tb = 2 * yy + 1 - core
                arrived(dblk(h, tb, q), d_recv.at[h, tb, q])
        if h < 2:
            d_local(h).wait()

    def norm_rows(v):
        w = v.astype(F32)
        return (w * lax.rsqrt(jnp.mean(w * w, axis=-1, keepdims=True) + 1e-06)).astype(BF)

    def gate_up(rows, slot):
        w = gu[slot].reshape(2 * HP, D)
        v = lax.dot_general(rows, w, (((1,), (1,)), ((), ())), preferred_element_type=F32)
        gt = v[:, :HP]
        return (gt * jax.nn.sigmoid(gt) * v[:, HP:]).astype(BF)

    def act_row(zi):
        act[zi] = gate_up(nx[zi].reshape(256, D), 0).reshape(4, 64, HP)

    def act_col(xi):
        rows = nx[:, pl.ds(xi, 1)].reshape(256, D)
        act[:, pl.ds(xi, 1)] = gate_up(rows, 0).reshape(4, 1, 64, HP)

    def act2_row(r):
        rows = ng[r].reshape(256, D)
        for b in range(2):
            act2[r, :, :, HP * b:HP * (b + 1)] = gate_up(rows, 1 + b).reshape(4, 64, HP)

    OFF = (2, 3, 1, 0)

    def pv(ab, i, o):
        j = rem4((z if ab == 0 else x) + o)
        if ab == 0:
            return part.at[0, j, i, :, pl.ds(0, 1024)]
        return part.at[0, i, j, :, pl.ds(1024, 1024)]

    def dev1(ab, step):
        if ab == 0:
            return (4 * z + rem4(x + step + 4), t)
        return (4 * rem4(z + step + 4) + x, t)

    def me1(ab, step):
        return rem4((x if ab == 0 else z) + step + 4)

    def down_chunk(ab, step):
        idx = me1(ab, step)
        w = dd[0, :, 1024 * ab:1024 * ab + 1024]
        if ab == 0:
            a = act[:, pl.ds(idx, 1)].reshape(256, HP)
        else:
            a = act[idx].reshape(256, HP)
        v = jnp.dot(a, w, preferred_element_type=F32).astype(BF)
        if ab == 0:
            part[0, :, pl.ds(idx, 1), :, 0:1024] = v.reshape(4, 1, 64, 1024)
        else:
            part[0, idx, :, :, 1024:2048] = v.reshape(4, 64, 1024)

    def s1(ab, k, src, dst, dev):
        send(src, dst, rs_send.at[ab, k], rs_recv.at[ab, k], dev)

    def rs_away(ab):
        for o in OFF:
            s1(ab, o, pv(ab, me1(ab, 2), o), r2.at[ab, o], dev1(ab, 1 if o in (2, 1) else -1))

    def rs_direct(ab, o):
        if o in (2, 1):
            s1(ab, 8 + o, pv(ab, me1(ab, -1), o), rb.at[ab, o], dev1(ab, -1))
        else:
            s1(ab, 8 + o, pv(ab, me1(ab, 1), o), ra.at[ab, o], dev1(ab, 1))

    def rs_turn(ab, o):
        arrived(r2.at[ab, o], rs_recv.at[ab, o])
        step = 1 if o in (2, 1) else -1
        tt[ab, o] = (r2[ab, o].astype(F32) + pv(ab, me1(ab, step), o)[...].astype(F32)).astype(BF)
        s1(ab, 4 + o, tt.at[ab, o], (ra if step == 1 else rb).at[ab, o], dev1(ab, step))

    def rs_fin(ab, o):
        ka, kb = (4 + o, 8 + o) if o in (2, 1) else (8 + o, 4 + o)
        arrived(ra.at[ab, o], rs_recv.at[ab, ka])
        arrived(rb.at[ab, o], rs_recv.at[ab, kb])
        s = pv(ab, me1(ab, 0), o)[...].astype(F32) + ra[ab, o].astype(F32) + rb[ab, o].astype(F32)
        acc[ab, o] = s
        up2, dn2_ = dev1(1 - ab, 1), dev1(1 - ab, -1)
        lo, hi = pl.ds(0, 32), pl.ds(32, 32)
        if o != 0:
            sb[ab, o] = s.astype(BF)
        if o == 2:
            s1(ab, 12, sb.at[ab, o, lo], q2.at[ab, 0], up2)
            s1(ab, 13, sb.at[ab, o, hi], q2.at[ab, 1], dn2_)
        if o == 1:
            s1(ab, 15, sb.at[ab, o, hi], qa.at[ab, hi], up2)
        if o == 3:
            s1(ab, 16, sb.at[ab, o, lo], qb.at[ab, lo], dn2_)

    def rs_turn2(ab, o):
        if o == 1:
            arrived(q2.at[ab, 0], rs_recv.at[ab, 12])
            qt[ab, 0] = (q2[ab, 0].astype(F32) + acc[ab, 1, 0:32]).astype(BF)
            s1(ab, 14, qt.at[ab, 0], qa.at[ab, pl.ds(0, 32)], dev1(1 - ab, 1))
        else:
            arrived(q2.at[ab, 1], rs_recv.at[ab, 13])
            qt[ab, 1] = (q2[ab, 1].astype(F32) + acc[ab, 3, 32:64]).astype(BF)
            s1(ab, 17, qt.at[ab, 1], qb.at[ab, pl.ds(32, 32)], dev1(1 - ab, -1))

    def rs_out(ab):
        arrived(qa.at[ab, pl.ds(32, 32)], rs_recv.at[ab, 15])
        arrived(qb.at[ab, pl.ds(0, 32)], rs_recv.at[ab, 16])
        arrived(qa.at[ab, pl.ds(0, 32)], rs_recv.at[ab, 14])
        arrived(qb.at[ab, pl.ds(32, 32)], rs_recv.at[ab, 17])
        return acc[ab, 0] + qa[ab].astype(F32) + qb[ab].astype(F32)

    zz = lax.rem(z, 2)
    zo = 1 - zz
    pair = (4 * (z + 1 - 2 * zz) + x, t)
    xp, xm, x2 = rem4(x + 1), rem4(x + 3), rem4(x + 2)
    xp_dev, xm_dev = (4 * z + xp, t), (4 * z + xm, t)
    CA, CB = pl.ds(0, NA), pl.ds(NA, D - NA)
    lo, hi = pl.ds(0, 32), pl.ds(32, 32)

    def gv(i, j, cols, rows=slice(None)):
        return ng.at[i, j, rows, cols]

    def gsend(k, ref, dev):
        send(ref, ref, ag_send.at[k], ag_recv.at[k], dev)

    def ag_a():
        gsend(1, gv(zz, x, CA), xp_dev)
        gsend(2, gv(zz, x, CA), xm_dev)
        gsend(7, gv(zz, x, CB), xp_dev)
        gsend(8, gv(zz, x, CB), xm_dev)
        gsend(0, gv(zz, x, CA), pair)
        gsend(9, gv(zz, x, CB), pair)

    def ag_b():
        arrived(gv(zo, x, CA), ag_recv.at[0])
        gsend(3, gv(zo, x, CA), xp_dev)
        gsend(4, gv(zo, x, CA), xm_dev)
        arrived(gv(zz, xm, CA), ag_recv.at[1])
        gsend(5, gv(zz, xm, CA), xp_dev)
        arrived(gv(zz, xm, CB), ag_recv.at[7])
        gsend(10, gv(zz, xm, CB, lo), xp_dev)
        gsend(12, gv(zz, xm, CB), pair)
        arrived(gv(zz, xp, CB), ag_recv.at[8])
        gsend(11, gv(zz, xp, CB, hi), xm_dev)
        gsend(13, gv(zz, xp, CB), pair)
        arrived(gv(zo, xp, CA), ag_recv.at[4])
        gsend(6, gv(zo, xp, CA), xm_dev)
        arrived(gv(zz, x2, CB, lo), ag_recv.at[10])
        arrived(gv(zz, x2, CB, hi), ag_recv.at[11])
        gsend(14, gv(zz, x2, CB), pair)

    def ag_own_row():
        for k, j, c in ((2, xp, CA), (5, x2, CA)):
            arrived(gv(zz, j, c), ag_recv.at[k])

    def ag_other_row():
        for k, i, j, c in (
            (3, zo, xm, CA), (6, zo, x2, CA),
            (9, zo, x, CB), (12, zo, xm, CB), (13, zo, xp, CB), (14, zo, x2, CB),
        ):
            arrived(gv(i, j, c), ag_recv.at[k])

    def down2_a(xi):
        w = dd[1:3, :, 0:NA].reshape(2 * HP, NA)
        v = jnp.dot(act2[:, pl.ds(xi, 1)].reshape(128, 2 * HP), w, preferred_element_type=F32).astype(BF)
        part2[:, pl.ds(xi, 1), :, 0:NA] = v.reshape(2, 1, 64, NA)

    def down2_b(zi):
        w = dd[1:3, :, NA:D].reshape(2 * HP, D - NA)
        v = jnp.dot(act2[zi].reshape(256, 2 * HP), w, preferred_element_type=F32).astype(BF)
        part2[zi, :, :, NA:D] = v.reshape(4, 64, D - NA)

    def tsend(k, src, dst, dev):
        send(src, dst, t_send.at[k], t_recv.at[k], dev)

    def rs2():
        down2_b(zo)
        for k, xi in enumerate((x2, xp, xm, x)):
            tsend(k, part2.at[zo, xi, :, CB], rzb.at[xi], pair)
        down2_a(x2)
        tsend(4, part2.at[zo, x2, :, CA], r2a.at[0], xp_dev)
        tsend(5, part2.at[zz, x2, :, CA], r2a.at[1], xm_dev)
        down2_a(xm)
        tsend(7, part2.at[zo, xm, :, CA], rba.at[0], xm_dev)
        down2_a(xp)
        tsend(6, part2.at[zz, xp, :, CA], raa.at[1], xp_dev)
        down2_b(zz)
        down2_a(x)

        def fold_b(k, xi):
            arrived(rzb.at[xi], t_recv.at[k])
            s = part2[zz, xi, :, NA:D].astype(F32) + rzb[xi].astype(F32)
            accb[xi] = s
            sbb[xi] = s.astype(BF)

        fold_b(0, x2)
        tsend(8, sbb.at[x2, lo], r2b.at[0], xp_dev)
        tsend(9, sbb.at[x2, hi], r2b.at[1], xm_dev)
        arrived(r2a.at[0], t_recv.at[4])
        ta[0] = (r2a[0].astype(F32) + part2[zo, xp, :, 0:NA].astype(F32)).astype(BF)
        tsend(10, ta.at[0], raa.at[0], xp_dev)
        arrived(r2a.at[1], t_recv.at[5])
        ta[1] = (r2a[1].astype(F32) + part2[zz, xm, :, 0:NA].astype(F32)).astype(BF)
        tsend(11, ta.at[1], rba.at[1], xm_dev)
        fold_b(1, xp)
        tsend(12, sbb.at[xp, hi], qab.at[hi], xp_dev)
        fold_b(2, xm)
        tsend(13, sbb.at[xm, lo], qbb.at[lo], xm_dev)
        arrived(rba.at[0], t_recv.at[7])
        arrived(raa.at[0], t_recv.at[10])
        s = part2[zo, x, :, 0:NA].astype(F32) + raa[0].astype(F32) + rba[0].astype(F32)
        sba[...] = s.astype(BF)
        tsend(16, sba, rpa, pair)
        arrived(r2b.at[0], t_recv.at[8])
        tb_[0] = (r2b[0].astype(F32) + accb[xp, 0:32]).astype(BF)
        tsend(14, tb_.at[0], qab.at[lo], xp_dev)
        arrived(r2b.at[1], t_recv.at[9])
        tb_[1] = (r2b[1].astype(F32) + accb[xm, 32:64]).astype(BF)
        tsend(15, tb_.at[1], qbb.at[hi], xm_dev)
        fold_b(3, x)
        arrived(raa.at[1], t_recv.at[6])
        arrived(rba.at[1], t_recv.at[11])
        own_a = part2[zz, x, :, 0:NA].astype(F32) + raa[1].astype(F32) + rba[1].astype(F32)
        arrived(qab.at[hi], t_recv.at[12])
        arrived(qbb.at[lo], t_recv.at[13])
        arrived(qab.at[lo], t_recv.at[14])
        arrived(qbb.at[hi], t_recv.at[15])
        own_b = accb[x] + qab[...].astype(F32) + qbb[...].astype(F32)
        ost[:, NA:D] = (mid[:, NA:D].astype(F32) + 0.5 * own_b).astype(BF)
        arrived(rpa, t_recv.at[16])
        ost[:, 0:NA] = (mid[:, 0:NA].astype(F32) + 0.5 * (own_a + rpa[...].astype(F32))).astype(BF)

    def put(src, dst, k):
        pltpu.make_async_copy(src, dst, o_sem.at[k]).start()

    def put_wait(src, dst, k):
        pltpu.make_async_copy(src, dst, o_sem.at[k]).wait()

    def fold(h):
        for k in range(4):
            icp[4 * h + k].wait()
        for k in range(2):
            wt[h, k] = (raw_g[h] * raw_w[h, k]).astype(BF)
        dn[h] = raw_d[h].astype(BF)

    def norm_first(r):
        xcp[r].wait()
        for k in range(4):
            nx[r, k] = norm_rows(nx[r, k])

    fold(0)
    pl.semaphore_wait(barrier, 15 - n_self + n_fro)
    stage_a()
    for s_ in range(3):
        dd[s_, HB:HP, :] = jnp.zeros((HP - HB, D), BF)
        for k in range(2):
            gu[s_, k, HB:HP, :] = jnp.zeros((HP - HB, D), BF)
    for r in range(4):
        norm_first(r)
    fold(1)
    w_own(0)
    stage_a2()
    d_partner()
    w_fwd(0)
    d_own(0)
    w_more(0)
    w_end(0)
    put(gu.at[0, 0, pl.ds(0, HB)], g1_o, 0)
    put(gu.at[0, 1, pl.ds(0, HB)], u1_o, 1)
    act_col(me1(0, 2))
    d_fwd(0)
    act_row(me1(1, 2))
    d_more(0)
    d_end(0)
    down_chunk(0, 2)
    rs_away(0)
    down_chunk(1, 2)
    rs_away(1)
    put(dd.at[0, pl.ds(0, HB)], d1_o, 2)
    hop(0, 0)
    hop(0, 1)
    act_row(me1(1, -1))
    down_chunk(1, -1)
    rs_direct(1, 2)
    act_row(me1(1, 1))
    down_chunk(1, 1)
    rs_direct(1, 3)
    act_row(me1(1, 0))
    down_chunk(0, -1)
    rs_direct(0, 2)
    down_chunk(0, 1)
    rs_direct(0, 3)
    for o in (2, 3):
        for ab in range(2):
            rs_turn(ab, o)
    for o in (1, 0):
        for ab in range(2):
            rs_direct(ab, o)
    for ab in range(2):
        down_chunk(ab, 0)
    d_own(1)
    d_own(2)
    for o in (1, 0):
        for ab in range(2):
            rs_turn(ab, o)
    hop(1, 0)
    for ab in range(2):
        rs_fin(ab, 2)
    for ab in range(2):
        rs_fin(ab, 3)
    hop(1, 1)
    for ab in range(2):
        rs_turn2(ab, 3)
    for ab in range(2):
        rs_fin(ab, 1)
    for ab in range(2):
        rs_turn2(ab, 1)
    for ab in range(2):
        rs_fin(ab, 0)
    hop(2, 0)
    branch = jnp.concatenate([rs_out(0), rs_out(1)], axis=-1)
    own_in.wait()
    m = (xown[...].astype(F32) + 0.5 * branch).astype(BF)
    mid[...] = m
    ng[zz, x] = norm_rows(m)
    ag_a()
    hop(2, 1)
    d_fwd(1)
    d_fwd(2)
    ag_b()
    hop(3, 0)
    d_more(1)
    d_more(2)
    hop(3, 1)
    hop_end()
    put(gu.at[1, 0, pl.ds(0, HB)], g2_o, 3)
    put(gu.at[1, 1, pl.ds(0, HB)], u2_o, 4)
    ag_own_row()
    act2_row(zz)
    for s_ in range(1, 3):
        d_end(s_)
    put(dd.at[1, pl.ds(0, HB)], d2_o, 5)
    ag_other_row()
    act2_row(zo)
    rs2()
    put(ost, ps_o, 6)

    drain()
    put_wait(gu.at[0, 0, pl.ds(0, HB)], g1_o, 0)
    put_wait(gu.at[0, 1, pl.ds(0, HB)], u1_o, 1)
    put_wait(dd.at[0, pl.ds(0, HB)], d1_o, 2)
    put_wait(gu.at[1, 0, pl.ds(0, HB)], g2_o, 3)
    put_wait(gu.at[1, 1, pl.ds(0, HB)], u2_o, 4)
    put_wait(dd.at[1, pl.ds(0, HB)], d2_o, 5)
    put_wait(ost, ps_o, 6)


def copy_out(*refs):
    n = len(refs) // 2
    sems = refs[-1]
    cps = [pltpu.make_async_copy(refs[k], refs[n + k], sems.at[k]) for k in range(n)]
    for cp in cps:
        cp.start()
    for cp in cps:
        cp.wait()


def run(xin, *weights):
    vm = pltpu.VMEM
    dma = pltpu.SemaphoreType.DMA
    w_out = jax.ShapeDtypeStruct((HB, D), BF)
    out_shape = (w_out,) * 6 + (jax.ShapeDtypeStruct((64, D), BF),)
    NB = D - NA
    scratch = [
        vm((4, 4, 64, D), BF), vm((2, 4, 64, D), BF), vm((64, D), BF), vm((64, D), BF),
        vm((2, 2, 2 * HB, 128), F32), vm((2, HB, 256), F32), vm((2, 1, 128), F32),
        vm((2, 2, 2 * HB, 128), BF), vm((2, HB, 256), BF),
        vm((3, 2, HP, D), BF), vm((3, HP, D), BF), vm((4, 4, 64, HP), BF), vm((2, 4, 64, 2 * HP), BF),
        vm((1, 4, 4, 64, D), BF), vm((2, 4, 64, D), BF),
        vm((2, 4, 64, 1024), BF), vm((2, 4, 64, 1024), BF), vm((2, 4, 64, 1024), BF),
        vm((2, 4, 64, 1024), BF), vm((2, 4, 64, 1024), F32), vm((2, 4, 64, 1024), BF),
        vm((2, 2, 32, 1024), BF), vm((2, 64, 1024), BF), vm((2, 64, 1024), BF),
        vm((2, 2, 32, 1024), BF), vm((64, D), BF),
        vm((2, 64, NA), BF), vm((2, 64, NA), BF), vm((2, 64, NA), BF), vm((2, 64, NA), BF),
        vm((2, 64, NA), F32), vm((64, NA), BF), vm((64, NA), BF),
        vm((4, 64, NB), BF), vm((4, 64, NB), F32), vm((4, 64, NB), BF),
        vm((2, 32, NB), BF), vm((64, NB), BF), vm((64, NB), BF), vm((2, 32, NB), BF),
        dma((3, 2)), dma((3, 16)), dma((3, 16)), dma((3, 8, 2)), dma((3, 14)), dma((2,)), dma, dma,
        dma((2, 18)), dma((2, 18)), dma((15,)), dma((15,)), dma((17,)), dma((17,)),
        dma((5,)), dma((2, 4)), dma((7,)),
    ]
    here = [pltpu.with_memory_space_constraint(v, pltpu.HBM) for v in (xin, *weights)]
    outs = pl.pallas_call(
        kernel,
        out_shape=tuple(pltpu.VMEM(o.shape, o.dtype) for o in out_shape),
        in_specs=[pl.BlockSpec(memory_space=pltpu.HBM)] * 9,
        out_specs=tuple(pl.BlockSpec(memory_space=pl.ANY) for _ in range(7)),
        scratch_shapes=scratch,
        compiler_params=pltpu.CompilerParams(
            collective_id=0, has_side_effects=True, vmem_limit_bytes=VMEM_MB * 1024 * 1024
        ),
    )(*here)
    return pl.pallas_call(
        copy_out,
        out_shape=out_shape,
        in_specs=[pl.BlockSpec(memory_space=pl.ANY)] * 7,
        out_specs=tuple(pl.BlockSpec(memory_space=pltpu.HBM) for _ in range(7)),
        scratch_shapes=[dma((7,))],
        compiler_params=pltpu.CompilerParams(vmem_limit_bytes=1024 * 1024),
    )(*outs)


def per_device(
    prompts, gain_first, gate_first, up_first, down_first, gain_second, gate_second, up_second, down_second
):
    xin = prompts.reshape(4, 4, 64, D)
    g1, u1, d1, g2, u2, d2, ps = run(
        xin,
        gain_first.reshape(1, 128), gate_first.T, up_first.T, down_first,
        gain_second.reshape(1, 128), gate_second.T, up_second.T, down_second,
    )
    return g1.T, u1.T, d1, g2.T, u2.T, d2, ps.reshape(1, 64, D)


def solution(mesh):
    w = P("fs", "tp")
    return jax.shard_map(
        per_device,
        mesh=mesh,
        in_specs=(P("tp", None, None), P("fs"), w, w, w, P("fs"), w, w, w),
        out_specs=(
            P(None, "fs"), P(None, "fs"), P("fs", None),
            P(None, "fs"), P(None, "fs"), P("fs", None),
            P("tp", "fs", None),
        ),
        check_vma=False,
    )
```

```python
import functools

import jax
import jax.numpy as jnp
from jax import lax
from jax.experimental import pallas as pl
from jax.experimental.pallas import tpu as pltpu
from jax.sharding import PartitionSpec as P

D = 2048
FF = 5632
HB = 352
HP = 384
TOK = 1024
MESH = pl.DeviceIdType.MESH
BF = jnp.bfloat16
F32 = jnp.float32
VMEM_MB = 53
POOL = 64


def rem4(v):
    return lax.rem(v, 4)


def kernel(
    x_hbm, gn1, gt1, ut1, dn1, gn2, gt2, ut2, dn2,
    g1_o, u1_o, d1_o, g2_o, u2_o, d2_o, ps_o,
    nx, ng, xown, mid, raw_w, raw_d, raw_g, wt, dn, gu, dd, act, part,
    gates, r2, ra, rb, tt, acc, sb, q2, qa, qb, qt, ost,
    pool, w1_recv, w_recv, w_send, d_recv, d_loc, rs_recv, ag_recv, x_sem, i_sem, o_sem,
):
    f = lax.axis_index("fs")
    t = lax.axis_index("tp")
    z = lax.div(f, 4)
    x = lax.rem(f, 4)
    y = lax.div(t, 2)
    core = lax.rem(t, 2)
    sib = (f, 2 * y + 1 - core)
    pending = []

    def remote(src, dst, ssem, rsem, dev):
        return pltpu.make_async_remote_copy(
            src_ref=src, dst_ref=dst, send_sem=ssem, recv_sem=rsem, device_id=dev, device_id_type=MESH
        )

    taken = []

    def settle(src, dst, ssem, rsem, dev, cond):
        if cond is None:
            remote(src, dst, ssem, rsem, dev).wait_send()
        else:
            pl.when(cond)(lambda: remote(src, dst, ssem, rsem, dev).wait_send())

    def send(src, dst, rsem, dev, cond=None):
        k = len(taken)
        if k >= POOL:
            settle(*taken[k - POOL])
        ssem = pool.at[k % POOL]
        if cond is None:
            remote(src, dst, ssem, rsem, dev).start()
        else:
            pl.when(cond)(lambda: remote(src, dst, ssem, rsem, dev).start())
        taken.append((src, dst, ssem, rsem, dev, cond))

    def drain():
        for item in taken[-POOL:] + pending:
            settle(*item)

    def arrived(dst, sem):
        pltpu.make_async_copy(dst, dst, sem).wait()

    def a_dt(g):
        return 2 * rem4(y + 2 + x - 2 * core - g + 4) + lax.div(z, 2)

    def tile_id(yy, cc, q):
        return 4 * (2 * cc + q) + rem4(yy - z + 2 + x + 4)

    barrier = pltpu.get_barrier_semaphore()

    def greet(dev):
        pl.semaphore_signal(barrier, inc=1, device_id=dev, device_id_type=MESH)

    near = [(f, 2 * rem4(y + 1) + core), (f, 2 * rem4(y + 3) + core), sib]
    near += [(4 * z + rem4(x + 1), t), (4 * z + rem4(x + 3), t), (4 * rem4(z + 1) + x, t), (4 * rem4(z + 3) + x, t)]
    for dev in near:
        greet(dev)
    n_self = jnp.int32(0)
    for g in range(2):
        to = (4 * y + 2 * core + g, a_dt(g))
        fro = (tile_id(y, core, g), 2 * z + lax.div(x, 2))
        to_self = jnp.logical_and(to[0] == f, to[1] == t)
        fro_self = jnp.logical_and(fro[0] == f, fro[1] == t)
        pl.when(jnp.logical_not(to_self))(functools.partial(greet, to))
        pl.when(jnp.logical_not(fro_self))(functools.partial(greet, fro))
        n_self = n_self + to_self.astype(jnp.int32) + fro_self.astype(jnp.int32)

    par = lax.rem(x + z, 2)
    for g in range(2):
        to = (4 * y + 2 * core + g, 2 * y + par)
        to_self = jnp.logical_and(to[0] == f, to[1] == t)
        pl.when(jnp.logical_not(to_self))(functools.partial(greet, to))
        n_self = n_self + to_self.astype(jnp.int32)
    n_fro = jnp.int32(0)
    for z2 in range(4):
        for k in range(2):
            fr = (4 * z2 + 2 * k + lax.rem(z2 + core, 2), 2 * y + lax.div(x, 2))
            is_self = jnp.logical_and(fr[0] == f, fr[1] == t)
            there = jnp.logical_and(y == z, jnp.logical_not(is_self))
            pl.when(there)(functools.partial(greet, fr))
            n_fro = n_fro + there.astype(jnp.int32)

    icp = []
    for h, (gn, gt, ut, dw) in enumerate(((gn1, gt1, ut1, dn1), (gn2, gt2, ut2, dn2))):
        for k, (src, dst) in enumerate(
            ((gn, raw_g.at[h]), (gt, raw_w.at[h, 0]), (ut, raw_w.at[h, 1]), (dw, raw_d.at[h]))
        ):
            cp = pltpu.make_async_copy(src, dst, i_sem.at[h, k])
            cp.start()
            icp.append(cp)
    xcp = []
    for r in range(4):
        cp = pltpu.make_async_copy(x_hbm.at[r], nx.at[r], x_sem.at[r])
        cp.start()
        xcp.append(cp)
    own_in = pltpu.make_async_copy(x_hbm.at[z, x], xown, x_sem.at[4])
    own_in.start()

    yp, ym, y2 = rem4(y + 1), rem4(y + 3), rem4(y + 2)


    def w1(k, ft):
        return gu.at[0, k, pl.ds(0, HB), pl.ds(pl.multiple_of(ft * 128, 128), 128)]

    def stage_a():
        for k in range(2):
            for g in range(2):
                src = wt.at[0, k, pl.ds(HB * g, HB), :]
                dev = (4 * y + 2 * core + g, a_dt(g))
                same = jnp.logical_and(dev[0] == f, dev[1] == t)
                send(src, w1(k, f), w1_recv.at[k, f], dev, jnp.logical_not(same))

                @pl.when(same)
                def _(src=src, k=k):
                    pltpu.make_async_copy(src, w1(k, f), w1_recv.at[k, f]).start()

    def wv(ft):
        return gu.at[1, :, pl.ds(0, HB), pl.ds(pl.multiple_of(ft * 128, 128), 128)]

    def stage_a2():
        for g in range(2):
            src = wt.at[1, :, pl.ds(HB * g, HB), :]
            dev = (4 * y + 2 * core + g, 2 * y + par)
            same = jnp.logical_and(dev[0] == f, dev[1] == t)
            send(src, wv(f), w_recv.at[f], dev, jnp.logical_not(same))

            @pl.when(same)
            def _(src=src):
                pltpu.make_async_copy(src, wv(f), w_recv.at[f]).start()

    nxt = (f, 2 * rem4(y + 1 + 2 * core) + core)
    dist = rem4(jnp.where(core == 0, y - z, z - y) + 4)

    def chain_tile(i, cc):
        z2, k = i // 2, i % 2
        return 4 * z2 + 2 * k + lax.rem(z2 + cc, 2)

    def hop(d, batch):
        @pl.when(dist == d)
        def _():
            for i in range(4 * batch, 4 * batch + 4):
                ft = chain_tile(i, core)
                tile = wv(ft)
                arrived(tile, w_recv.at[ft])
                if d < 3:
                    remote(tile, tile, w_send.at[i], w_recv.at[ft], nxt).start()
                remote(tile, tile, w_send.at[8 + i], w_recv.at[ft], sib).start()

    def hop_end():
        for i in range(8):
            ft = chain_tile(i, core)
            tile = wv(ft)
            pending.append((tile, tile, w_send.at[i], w_recv.at[ft], nxt, dist < 3))
            pending.append((tile, tile, w_send.at[8 + i], w_recv.at[ft], sib, None))
            fo = chain_tile(i, 1 - core)
            arrived(wv(fo), w_recv.at[fo])

    def wsend(k, ft, dev):
        send(w1(k, ft), w1(k, ft), w1_recv.at[k, ft], dev)

    def wgot(k, ft):
        arrived(w1(k, ft), w1_recv.at[k, ft])

    up_dev, dn_dev = (f, 2 * yp + core), (f, 2 * ym + core)

    def w_own():
        for k in range(2):
            for q in range(2):
                ft = tile_id(y, core, q)
                wgot(k, ft)
                for dev in (up_dev, dn_dev, sib):
                    wsend(k, ft, dev)

    def w_fwd(k):
        lo, hi = tile_id(ym, core, 0), tile_id(yp, core, 1)
        wgot(k, lo)
        wsend(k, lo, up_dev)
        wgot(k, hi)
        wsend(k, hi, dn_dev)
        wsend(k, lo, sib)
        wsend(k, hi, sib)

    def w_more(k):
        for ft in (tile_id(ym, core, 1), tile_id(yp, core, 0)):
            wgot(k, ft)
            wsend(k, ft, sib)
        for q in range(2):
            ft = tile_id(y2, core, q)
            wgot(k, ft)
            wsend(k, ft, sib)

    def w_end(k):
        for yy in range(4):
            for q in range(2):
                wgot(k, tile_id(yy, 1 - core, q))

    def dblk(h, tb, q):
        return dd.at[h, pl.ds(176 * q, 176), pl.ds(pl.multiple_of(tb * 256, 256), 256)]

    def d_local(h):
        return pltpu.make_async_copy(
            dn.at[h], dd.at[h, pl.ds(0, HB), pl.ds(pl.multiple_of(t * 256, 256), 256)], d_loc.at[h]
        )

    def dsend(h, tb, q, dev):
        send(dblk(h, tb, q), dblk(h, tb, q), d_recv.at[h, tb, q], dev)

    def d_own(h):
        d_local(h).start()
        for q in range(2):
            src = dn.at[h, pl.ds(176 * q, 176), :]
            for dev in (up_dev, dn_dev, sib):
                send(src, dblk(h, t, q), d_recv.at[h, t, q], dev)

    def d_fwd(h):
        tm, tp = 2 * ym + core, 2 * yp + core
        arrived(dblk(h, tm, 0), d_recv.at[h, tm, 0])
        dsend(h, tm, 0, up_dev)
        arrived(dblk(h, tp, 1), d_recv.at[h, tp, 1])
        dsend(h, tp, 1, dn_dev)
        dsend(h, tm, 0, sib)
        dsend(h, tp, 1, sib)

    def d_more(h):
        for tb, q in ((2 * ym + core, 1), (2 * yp + core, 0), (2 * y2 + core, 0), (2 * y2 + core, 1)):
            arrived(dblk(h, tb, q), d_recv.at[h, tb, q])
            dsend(h, tb, q, sib)

    def d_end(h):
        for yy in range(4):
            for q in range(2):
                tb = 2 * yy + 1 - core
                arrived(dblk(h, tb, q), d_recv.at[h, tb, q])
        d_local(h).wait()

    def norm_rows(v):
        w = v.astype(F32)
        return (w * lax.rsqrt(jnp.mean(w * w, axis=-1, keepdims=True) + 1e-06)).astype(BF)

    def gate_up(rows, slot):
        w = gu[slot].reshape(2 * HP, D)
        v = lax.dot_general(rows, w, (((1,), (1,)), ((), ())), preferred_element_type=F32)
        gt = v[:, :HP]
        return (gt * jax.nn.sigmoid(gt) * v[:, HP:]).astype(BF)

    def nt_dot(rows, w):
        return lax.dot_general(rows, w, (((1,), (1,)), ((), ())), preferred_element_type=F32)

    def gate_row(zi):
        gates[zi] = nt_dot(nx[zi].reshape(256, D), gu[0, 0]).reshape(4, 64, HP)

    def with_gate(gt, rows):
        return (gt * jax.nn.sigmoid(gt) * nt_dot(rows, gu[0, 1])).astype(BF)

    def act_row(h, zi):
        if h == 1:
            act[zi] = gate_up(ng[zi].reshape(256, D), 1).reshape(4, 64, HP)
        else:
            act[zi] = with_gate(gates[zi].reshape(256, HP), nx[zi].reshape(256, D)).reshape(4, 64, HP)

    def act_col(xi):
        rows = nx[:, pl.ds(xi, 1)].reshape(256, D)
        act[:, pl.ds(xi, 1)] = with_gate(gates[:, pl.ds(xi, 1)].reshape(256, HP), rows).reshape(4, 1, 64, HP)

    OFF = (2, 3, 1, 0)

    def pv(h, ab, i, o):
        j = rem4((z if ab == 0 else x) + o)
        if ab == 0:
            return part.at[h, j, i, :, pl.ds(0, 1024)]
        return part.at[h, i, j, :, pl.ds(1024, 1024)]

    def dev1(ab, step):
        if ab == 0:
            return (4 * z + rem4(x + step + 4), t)
        return (4 * rem4(z + step + 4) + x, t)

    def me1(ab, step):
        return rem4((x if ab == 0 else z) + step + 4)

    def down_chunk(h, ab, step):
        idx = me1(ab, step)
        w = dd[h, :, 1024 * ab:1024 * ab + 1024]
        if ab == 0:
            a = act[:, pl.ds(idx, 1)].reshape(256, HP)
        else:
            a = act[idx].reshape(256, HP)
        v = jnp.dot(a, w, preferred_element_type=F32).astype(BF)
        if ab == 0:
            part[h, :, pl.ds(idx, 1), :, 0:1024] = v.reshape(4, 1, 64, 1024)
        else:
            part[h, idx, :, :, 1024:2048] = v.reshape(4, 64, 1024)

    def s1(h, ab, k, src, dst, dev):
        send(src, dst, rs_recv.at[ab, k], dev)

    def rs_away(h, ab):
        for o in OFF:
            s1(h, ab, o, pv(h, ab, me1(ab, 2), o), r2.at[h, ab, o], dev1(ab, 1 if o in (2, 1) else -1))

    def rs_direct(h, ab, o):
        if o in (2, 1):
            s1(h, ab, 8 + o, pv(h, ab, me1(ab, -1), o), rb.at[h, ab, o], dev1(ab, -1))
        else:
            s1(h, ab, 8 + o, pv(h, ab, me1(ab, 1), o), ra.at[h, ab, o], dev1(ab, 1))

    def rs_turn(h, ab, o):
        arrived(r2.at[h, ab, o], rs_recv.at[ab, o])
        step = 1 if o in (2, 1) else -1
        tt[h, ab, o] = (r2[h, ab, o].astype(F32) + pv(h, ab, me1(ab, step), o)[...].astype(F32)).astype(BF)
        s1(h, ab, 4 + o, tt.at[h, ab, o], (ra if step == 1 else rb).at[h, ab, o], dev1(ab, step))

    def rs_fin(h, ab, o):
        ka, kb = (4 + o, 8 + o) if o in (2, 1) else (8 + o, 4 + o)
        arrived(ra.at[h, ab, o], rs_recv.at[ab, ka])
        arrived(rb.at[h, ab, o], rs_recv.at[ab, kb])
        s = pv(h, ab, me1(ab, 0), o)[...].astype(F32) + ra[h, ab, o].astype(F32) + rb[h, ab, o].astype(F32)
        acc[ab, o] = s
        up2, dn2_ = dev1(1 - ab, 1), dev1(1 - ab, -1)
        lo, hi = pl.ds(0, 32), pl.ds(32, 32)
        if o != 0:
            sb[h, ab, o] = s.astype(BF)
        if o == 2:
            s1(h, ab, 12, sb.at[h, ab, o, lo], q2.at[h, ab, 0], up2)
            s1(h, ab, 13, sb.at[h, ab, o, hi], q2.at[h, ab, 1], dn2_)
        if o == 1:
            s1(h, ab, 15, sb.at[h, ab, o, hi], qa.at[h, ab, hi], up2)
        if o == 3:
            s1(h, ab, 16, sb.at[h, ab, o, lo], qb.at[h, ab, lo], dn2_)

    def rs_turn2(h, ab, o):
        if o == 1:
            arrived(q2.at[h, ab, 0], rs_recv.at[ab, 12])
            qt[h, ab, 0] = (q2[h, ab, 0].astype(F32) + acc[ab, 1, 0:32]).astype(BF)
            s1(h, ab, 14, qt.at[h, ab, 0], qa.at[h, ab, pl.ds(0, 32)], dev1(1 - ab, 1))
        else:
            arrived(q2.at[h, ab, 1], rs_recv.at[ab, 13])
            qt[h, ab, 1] = (q2[h, ab, 1].astype(F32) + acc[ab, 3, 32:64]).astype(BF)
            s1(h, ab, 17, qt.at[h, ab, 1], qb.at[h, ab, pl.ds(32, 32)], dev1(1 - ab, -1))

    def rs_out(h, ab):
        arrived(qa.at[h, ab, pl.ds(32, 32)], rs_recv.at[ab, 15])
        arrived(qb.at[h, ab, pl.ds(0, 32)], rs_recv.at[ab, 16])
        arrived(qa.at[h, ab, pl.ds(0, 32)], rs_recv.at[ab, 14])
        arrived(qb.at[h, ab, pl.ds(32, 32)], rs_recv.at[ab, 17])
        return acc[ab, 0] + qa[h, ab].astype(F32) + qb[h, ab].astype(F32)

    def rs_run(h, points):
        def point(k):
            for fn in points.get(k, ()):
                fn()

        down_chunk(h, 0, 2)
        rs_away(h, 0)
        down_chunk(h, 1, 2)
        rs_away(h, 1)
        point(0)
        down_chunk(h, 1, -1)
        rs_direct(h, 1, 2)
        point(1)
        down_chunk(h, 1, 1)
        point(2)
        down_chunk(h, 0, -1)
        rs_direct(h, 0, 2)
        down_chunk(h, 0, 1)
        for ab in (1, 0):
            rs_turn(h, ab, 2)
            rs_direct(h, ab, 3)
            rs_turn(h, ab, 3)
        point(3)
        for ab in (1, 0):
            rs_turn(h, ab, 1)
            rs_direct(h, ab, 1)
        for ab in range(2):
            down_chunk(h, ab, 0)
        for ab in (1, 0):
            rs_fin(h, ab, 2)
        for ab in (1, 0):
            rs_direct(h, ab, 0)
        for ab in (1, 0):
            rs_fin(h, ab, 3)
            rs_turn(h, ab, 0)
        point(4)
        for ab in (1, 0):
            rs_fin(h, ab, 1)
        point(5)
        for ab in (1, 0):
            rs_turn2(h, ab, 3)
            rs_turn2(h, ab, 1)
        for ab in (1, 0):
            rs_fin(h, ab, 0)
        point(6)
        return jnp.concatenate([rs_out(h, 0), rs_out(h, 1)], axis=-1)

    lo_rows, hi_rows = pl.ds(0, 32), pl.ds(32, 32)
    waited = set()

    def gv(ab, i, j, rows=slice(None)):
        zi, xi = (i, j) if ab == 0 else (j, i)
        return ng.at[rem4(z + zi), rem4(x + xi), rows, pl.ds(1024 * ab, 1024)]

    LAND = {
        0: (3, 0), 1: (1, 0), 2: (2, 0, lo_rows), 3: (2, 0, hi_rows),
        4: (0, 3), 5: (1, 3), 6: (2, 3), 7: (3, 3),
        8: (0, 1), 9: (1, 1), 10: (2, 1), 11: (3, 1),
        12: (0, 2), 13: (1, 2), 14: (3, 2), 15: (2, 2),
    }

    def got(ab, *slots):
        for k in slots:
            if (ab, k) not in waited:
                waited.add((ab, k))
                arrived(gv(ab, *LAND[k]), ag_recv.at[ab, k])

    def snd(ab, k, ref, second, step):
        send(ref, ref, ag_recv.at[ab, k], dev1(ab if second else 1 - ab, step))

    def ag_start():
        for ab in range(2):
            own = gv(ab, 0, 0)
            snd(ab, 0, own, False, 1)
            snd(ab, 1, own, False, -1)
            snd(ab, 4, own, True, 1)
            snd(ab, 8, own, True, -1)

    def ag_first():
        for ab in range(2):
            got(ab, 0)
            snd(ab, 2, gv(ab, 3, 0, lo_rows), False, 1)
            got(ab, 1)
            snd(ab, 3, gv(ab, 1, 0, hi_rows), False, -1)
            snd(ab, 5, gv(ab, 1, 0), True, 1)
            snd(ab, 11, gv(ab, 3, 0), True, -1)
            snd(ab, 7, gv(ab, 3, 0), True, 1)
            snd(ab, 9, gv(ab, 1, 0), True, -1)

    def ag_second():
        for ab in range(2):
            got(ab, 4)
            snd(ab, 12, gv(ab, 0, 3), True, 1)
        for ab in range(2):
            got(ab, 2, 3)
            snd(ab, 10, gv(ab, 2, 0), True, -1)
            snd(ab, 6, gv(ab, 2, 0), True, 1)

    def ag_third():
        for ab in range(2):
            got(ab, 5)
            snd(ab, 13, gv(ab, 1, 3), True, 1)
            got(ab, 8, 11)
            snd(ab, 14, gv(ab, 3, 1), True, -1)

    def ag_fourth():
        for ab in range(2):
            got(ab, 9, 10)
            snd(ab, 15, gv(ab, 2, 1), True, -1)

    def ag_row(oz):
        for k, v in LAND.items():
            if v[0] == oz:
                got(0, k)
            if v[1] == oz:
                got(1, k)

    def put(src, dst, k):
        pltpu.make_async_copy(src, dst, o_sem.at[k]).start()

    def put_wait(src, dst, k):
        pltpu.make_async_copy(src, dst, o_sem.at[k]).wait()

    def fold(h):
        for k in range(4):
            icp[4 * h + k].wait()
        for k in range(2):
            wt[h, k] = (raw_g[h] * raw_w[h, k]).astype(BF)
        dn[h] = raw_d[h].astype(BF)

    def norm_first(r):
        xcp[r].wait()
        for k in range(4):
            nx[r, k] = norm_rows(nx[r, k])

    fold(0)
    pl.semaphore_wait(barrier, 13 - n_self + n_fro)
    stage_a()
    d_own(0)
    for s_ in range(2):
        dd[s_, HB:HP, :] = jnp.zeros((HP - HB, D), BF)
        for k in range(2):
            gu[s_, k, HB:HP, :] = jnp.zeros((HP - HB, D), BF)
    for r in range(4):
        norm_first(r)
    fold(1)
    w_own()
    stage_a2()
    w_fwd(0)
    w_fwd(1)
    d_fwd(0)
    w_more(0)
    w_end(0)
    gate_row(0)
    gate_row(1)
    w_more(1)
    gate_row(2)
    gate_row(3)
    w_end(1)
    put(gu.at[0, 0, pl.ds(0, HB)], g1_o, 0)
    put(gu.at[0, 1, pl.ds(0, HB)], u1_o, 1)
    act_col(rem4(x + 2))
    act_row(0, rem4(z + 2))
    d_more(0)
    d_end(0)
    put(dd.at[0, pl.ds(0, HB)], d1_o, 2)
    branch = rs_run(0, {
        0: (lambda: hop(0, 0), lambda: hop(0, 1), lambda: act_row(0, rem4(z + 3))),
        1: (lambda: act_row(0, rem4(z + 1)),),
        2: (lambda: act_row(0, z),),
        3: (lambda: hop(1, 0),),
        4: (lambda: hop(1, 1),),
        5: (lambda: hop(2, 0),),
        6: (lambda: d_own(1),),
    })
    own_in.wait()
    m = (xown[...].astype(F32) + 0.5 * branch).astype(BF)
    mid[...] = m
    ng[z, x] = norm_rows(m)
    ag_start()
    hop(2, 1)
    ag_first()
    ag_second()
    d_fwd(1)
    hop(3, 0)
    ag_third()
    hop(3, 1)
    hop_end()
    ag_row(0)
    act_row(1, z)
    ag_fourth()
    put(gu.at[1, 0, pl.ds(0, HB)], g2_o, 3)
    put(gu.at[1, 1, pl.ds(0, HB)], u2_o, 4)
    for oz in (1, 3):
        ag_row(oz)
        act_row(1, rem4(z + oz))
    d_more(1)
    ag_row(2)
    act_row(1, rem4(z + 2))
    d_end(1)
    put(dd.at[1, pl.ds(0, HB)], d2_o, 5)
    branch = rs_run(1, {})
    ost[...] = (mid[...].astype(F32) + 0.5 * branch).astype(BF)
    put(ost, ps_o, 6)

    drain()
    put_wait(gu.at[0, 0, pl.ds(0, HB)], g1_o, 0)
    put_wait(gu.at[0, 1, pl.ds(0, HB)], u1_o, 1)
    put_wait(dd.at[0, pl.ds(0, HB)], d1_o, 2)
    put_wait(gu.at[1, 0, pl.ds(0, HB)], g2_o, 3)
    put_wait(gu.at[1, 1, pl.ds(0, HB)], u2_o, 4)
    put_wait(dd.at[1, pl.ds(0, HB)], d2_o, 5)
    put_wait(ost, ps_o, 6)


def copy_out(*refs):
    n = len(refs) // 2
    sems = refs[-1]
    cps = [pltpu.make_async_copy(refs[k], refs[n + k], sems.at[k]) for k in range(n)]
    for cp in cps:
        cp.start()
    for cp in cps:
        cp.wait()


def run(xin, *weights):
    vm = pltpu.VMEM
    dma = pltpu.SemaphoreType.DMA
    w_out = jax.ShapeDtypeStruct((HB, D), BF)
    out_shape = (w_out,) * 6 + (jax.ShapeDtypeStruct((64, D), BF),)
    unit = (2, 2, 4, 64, 1024)
    half = (2, 2, 2, 32, 1024)
    one = (2, 2, 64, 1024)
    scratch = [
        vm((4, 4, 64, D), BF), vm((4, 4, 64, D), BF), vm((64, D), BF), vm((64, D), BF),
        vm((2, 2, 2 * HB, 128), F32), vm((2, HB, 256), F32), vm((2, 1, 128), F32),
        vm((2, 2, 2 * HB, 128), BF), vm((2, HB, 256), BF),
        vm((2, 2, HP, D), BF), vm((2, HP, D), BF), vm((4, 4, 64, HP), BF), vm((2, 4, 4, 64, D), BF),
        vm((4, 4, 64, HP), F32),
        vm(unit, BF), vm(unit, BF), vm(unit, BF), vm(unit, BF), vm((2, 4, 64, 1024), F32), vm(unit, BF),
        vm(half, BF), vm(one, BF), vm(one, BF), vm(half, BF), vm((64, D), BF),
        dma((POOL,)), dma((2, 16)), dma((16,)), dma((16,)), dma((2, 8, 2)), dma((2,)), dma((2, 18)), dma((2, 16)),
        dma((5,)), dma((2, 4)), dma((7,)),
    ]
    here = [pltpu.with_memory_space_constraint(v, pltpu.HBM) for v in (xin, *weights)]
    outs = pl.pallas_call(
        kernel,
        out_shape=tuple(pltpu.VMEM(o.shape, o.dtype) for o in out_shape),
        in_specs=[pl.BlockSpec(memory_space=pltpu.HBM)] * 9,
        out_specs=tuple(pl.BlockSpec(memory_space=pl.ANY) for _ in range(7)),
        scratch_shapes=scratch,
        compiler_params=pltpu.CompilerParams(
            collective_id=0, has_side_effects=True, vmem_limit_bytes=VMEM_MB * 1024 * 1024
        ),
    )(*here)
    return pl.pallas_call(
        copy_out,
        out_shape=out_shape,
        in_specs=[pl.BlockSpec(memory_space=pl.ANY)] * 7,
        out_specs=tuple(pl.BlockSpec(memory_space=pltpu.HBM) for _ in range(7)),
        scratch_shapes=[dma((7,))],
        compiler_params=pltpu.CompilerParams(vmem_limit_bytes=1024 * 1024),
    )(*outs)


def per_device(
    prompts, gain_first, gate_first, up_first, down_first, gain_second, gate_second, up_second, down_second
):
    xin = prompts.reshape(4, 4, 64, D)
    g1, u1, d1, g2, u2, d2, ps = run(
        xin,
        gain_first.reshape(1, 128), gate_first.T, up_first.T, down_first,
        gain_second.reshape(1, 128), gate_second.T, up_second.T, down_second,
    )
    return g1.T, u1.T, d1, g2.T, u2.T, d2, ps.reshape(1, 64, D)


def solution(mesh):
    w = P("fs", "tp")
    return jax.shard_map(
        per_device,
        mesh=mesh,
        in_specs=(P("tp", None, None), P("fs"), w, w, w, P("fs"), w, w, w),
        out_specs=(
            P(None, "fs"), P(None, "fs"), P("fs", None),
            P(None, "fs"), P(None, "fs"), P("fs", None),
            P("tp", "fs", None),
        ),
        check_vma=False,
    )
```

```python
import functools

import jax
import jax.numpy as jnp
from jax import lax
from jax.experimental import pallas as pl
from jax.experimental.pallas import tpu as pltpu
from jax.sharding import PartitionSpec as P

D = 2048
FF = 5632
HB = 352
HP = 384
TOK = 1024
MESH = pl.DeviceIdType.MESH
BF = jnp.bfloat16
F32 = jnp.float32
VMEM_MB = 53
POOL = 56


def rem4(v):
    return lax.rem(v, 4)


def kernel(
    x_hbm, gn1, gt1, ut1, dn1, gn2, gt2, ut2, dn2,
    g1_o, u1_o, d1_o, g2_o, u2_o, d2_o, ps_o,
    nx, ng, xown, mid, raw_w, raw_d, raw_g, wt, dn, gu, dd, act, part,
    gates, r2, ra, rb, tt, acc, sb, q2, qa, qb, qt, ost,
    pool, w1_recv, w_recv, w_send, d_recv, d_loc, rs_recv, ag_recv, x_sem, i_sem,
):
    f = lax.axis_index("fs")
    t = lax.axis_index("tp")
    z = lax.div(f, 4)
    x = lax.rem(f, 4)
    y = lax.div(t, 2)
    core = lax.rem(t, 2)
    sib = (f, 2 * y + 1 - core)
    pending = []

    def remote(src, dst, ssem, rsem, dev):
        return pltpu.make_async_remote_copy(
            src_ref=src, dst_ref=dst, send_sem=ssem, recv_sem=rsem, device_id=dev, device_id_type=MESH
        )

    taken = []

    def settle(src, dst, ssem, rsem, dev, cond):
        if cond is None:
            remote(src, dst, ssem, rsem, dev).wait_send()
        else:
            pl.when(cond)(lambda: remote(src, dst, ssem, rsem, dev).wait_send())

    def send(src, dst, rsem, dev, cond=None):
        k = len(taken)
        if k >= POOL:
            settle(*taken[k - POOL])
        ssem = pool.at[k % POOL]
        if cond is None:
            remote(src, dst, ssem, rsem, dev).start()
        else:
            pl.when(cond)(lambda: remote(src, dst, ssem, rsem, dev).start())
        taken.append((src, dst, ssem, rsem, dev, cond))

    def drain():
        for item in taken[-POOL:] + pending:
            settle(*item)

    def arrived(dst, sem):
        pltpu.make_async_copy(dst, dst, sem).wait()

    def a_dt(g):
        return 2 * rem4(y + 2 + x - 2 * core - g + 4) + lax.div(z, 2)

    def tile_id(yy, cc, q):
        return 4 * (2 * cc + q) + rem4(yy - z + 2 + x + 4)

    barrier = pltpu.get_barrier_semaphore()

    def greet(dev):
        pl.semaphore_signal(barrier, inc=1, device_id=dev, device_id_type=MESH)

    near = [(f, 2 * rem4(y + 1) + core), (f, 2 * rem4(y + 3) + core), sib]
    near += [(4 * z + rem4(x + 1), t), (4 * z + rem4(x + 3), t), (4 * rem4(z + 1) + x, t), (4 * rem4(z + 3) + x, t)]
    for dev in near:
        greet(dev)
    n_self = jnp.int32(0)
    for g in range(2):
        to = (4 * y + 2 * core + g, a_dt(g))
        fro = (tile_id(y, core, g), 2 * z + lax.div(x, 2))
        to_self = jnp.logical_and(to[0] == f, to[1] == t)
        fro_self = jnp.logical_and(fro[0] == f, fro[1] == t)
        pl.when(jnp.logical_not(to_self))(functools.partial(greet, to))
        pl.when(jnp.logical_not(fro_self))(functools.partial(greet, fro))
        n_self = n_self + to_self.astype(jnp.int32) + fro_self.astype(jnp.int32)

    par = lax.rem(x + z, 2)
    for g in range(2):
        to = (4 * y + 2 * core + g, 2 * y + par)
        to_self = jnp.logical_and(to[0] == f, to[1] == t)
        pl.when(jnp.logical_not(to_self))(functools.partial(greet, to))
        n_self = n_self + to_self.astype(jnp.int32)
    n_fro = jnp.int32(0)
    for z2 in range(4):
        for k in range(2):
            fr = (4 * z2 + 2 * k + lax.rem(z2 + core, 2), 2 * y + lax.div(x, 2))
            is_self = jnp.logical_and(fr[0] == f, fr[1] == t)
            there = jnp.logical_and(y == z, jnp.logical_not(is_self))
            pl.when(there)(functools.partial(greet, fr))
            n_fro = n_fro + there.astype(jnp.int32)

    icp = []
    for h, (gn, gt, ut, dw) in enumerate(((gn1, gt1, ut1, dn1), (gn2, gt2, ut2, dn2))):
        for k, (src, dst) in enumerate(
            ((gn, raw_g.at[h]), (gt, raw_w.at[h, 0]), (ut, raw_w.at[h, 1]), (dw, raw_d.at[h]))
        ):
            cp = pltpu.make_async_copy(src, dst, i_sem.at[h, k])
            cp.start()
            icp.append(cp)
    xcp = []
    for r in range(4):
        cp = pltpu.make_async_copy(x_hbm.at[r], nx.at[r], x_sem.at[r])
        cp.start()
        xcp.append(cp)
    own_in = pltpu.make_async_copy(x_hbm.at[z, x], xown, x_sem.at[4])
    own_in.start()

    yp, ym, y2 = rem4(y + 1), rem4(y + 3), rem4(y + 2)


    def w1(k, ft):
        return gu.at[0, k, pl.ds(0, HB), pl.ds(pl.multiple_of(ft * 128, 128), 128)]

    def stage_a():
        for k in range(2):
            for g in range(2):
                src = wt.at[0, k, pl.ds(HB * g, HB), :]
                dev = (4 * y + 2 * core + g, a_dt(g))
                same = jnp.logical_and(dev[0] == f, dev[1] == t)
                send(src, w1(k, f), w1_recv.at[k, f], dev, jnp.logical_not(same))

                @pl.when(same)
                def _(src=src, k=k):
                    pltpu.make_async_copy(src, w1(k, f), w1_recv.at[k, f]).start()

    def wv(ft):
        return gu.at[1, :, pl.ds(0, HB), pl.ds(pl.multiple_of(ft * 128, 128), 128)]

    def stage_a2():
        for g in range(2):
            src = wt.at[1, :, pl.ds(HB * g, HB), :]
            dev = (4 * y + 2 * core + g, 2 * y + par)
            same = jnp.logical_and(dev[0] == f, dev[1] == t)
            send(src, wv(f), w_recv.at[f], dev, jnp.logical_not(same))

            @pl.when(same)
            def _(src=src):
                pltpu.make_async_copy(src, wv(f), w_recv.at[f]).start()

    nxt = (f, 2 * rem4(y + 1 + 2 * core) + core)
    dist = rem4(jnp.where(core == 0, y - z, z - y) + 4)

    def chain_tile(i, cc):
        z2, k = i // 2, i % 2
        return 4 * z2 + 2 * k + lax.rem(z2 + cc, 2)

    def hop(d, batch):
        @pl.when(dist == d)
        def _():
            for i in range(4 * batch, 4 * batch + 4):
                ft = chain_tile(i, core)
                tile = wv(ft)
                arrived(tile, w_recv.at[ft])
                if d < 3:
                    remote(tile, tile, w_send.at[i], w_recv.at[ft], nxt).start()
                remote(tile, tile, w_send.at[8 + i], w_recv.at[ft], sib).start()

    def hop_end():
        for i in range(8):
            ft = chain_tile(i, core)
            tile = wv(ft)
            pending.append((tile, tile, w_send.at[i], w_recv.at[ft], nxt, dist < 3))
            pending.append((tile, tile, w_send.at[8 + i], w_recv.at[ft], sib, None))
            fo = chain_tile(i, 1 - core)
            arrived(wv(fo), w_recv.at[fo])

    def wsend(k, ft, dev):
        send(w1(k, ft), w1(k, ft), w1_recv.at[k, ft], dev)

    def wgot(k, ft):
        arrived(w1(k, ft), w1_recv.at[k, ft])

    up_dev, dn_dev = (f, 2 * yp + core), (f, 2 * ym + core)

    def w_own():
        for k in range(2):
            for q in range(2):
                ft = tile_id(y, core, q)
                wgot(k, ft)
                for dev in (up_dev, dn_dev, sib):
                    wsend(k, ft, dev)

    def w_fwd(k):
        lo, hi = tile_id(ym, core, 0), tile_id(yp, core, 1)
        wgot(k, lo)
        wsend(k, lo, up_dev)
        wgot(k, hi)
        wsend(k, hi, dn_dev)
        wsend(k, lo, sib)
        wsend(k, hi, sib)

    def w_more(k):
        for ft in (tile_id(ym, core, 1), tile_id(yp, core, 0)):
            wgot(k, ft)
            wsend(k, ft, sib)
        for q in range(2):
            ft = tile_id(y2, core, q)
            wgot(k, ft)
            wsend(k, ft, sib)

    def w_end(k):
        for yy in range(4):
            for q in range(2):
                wgot(k, tile_id(yy, 1 - core, q))

    def dblk(h, tb, q):
        return dd.at[h, pl.ds(176 * q, 176), pl.ds(pl.multiple_of(tb * 256, 256), 256)]

    def d_local(h):
        return pltpu.make_async_copy(
            dn.at[h], dd.at[h, pl.ds(0, HB), pl.ds(pl.multiple_of(t * 256, 256), 256)], d_loc.at[h]
        )

    def dsend(h, tb, q, dev):
        send(dblk(h, tb, q), dblk(h, tb, q), d_recv.at[h, tb, q], dev)

    def d_own(h):
        d_local(h).start()
        for q in range(2):
            src = dn.at[h, pl.ds(176 * q, 176), :]
            for dev in (up_dev, dn_dev, sib):
                send(src, dblk(h, t, q), d_recv.at[h, t, q], dev)

    def d_fwd(h):
        tm, tp = 2 * ym + core, 2 * yp + core
        arrived(dblk(h, tm, 0), d_recv.at[h, tm, 0])
        dsend(h, tm, 0, up_dev)
        arrived(dblk(h, tp, 1), d_recv.at[h, tp, 1])
        dsend(h, tp, 1, dn_dev)
        dsend(h, tm, 0, sib)
        dsend(h, tp, 1, sib)

    def d_more(h):
        for tb, q in ((2 * ym + core, 1), (2 * yp + core, 0), (2 * y2 + core, 0), (2 * y2 + core, 1)):
            arrived(dblk(h, tb, q), d_recv.at[h, tb, q])
            dsend(h, tb, q, sib)

    def d_end(h):
        for yy in range(4):
            for q in range(2):
                tb = 2 * yy + 1 - core
                arrived(dblk(h, tb, q), d_recv.at[h, tb, q])
        d_local(h).wait()

    def norm_rows(v):
        w = v.astype(F32)
        return (w * lax.rsqrt(jnp.mean(w * w, axis=-1, keepdims=True) + 1e-06)).astype(BF)

    def gate_up(rows, slot):
        w = gu[slot].reshape(2 * HP, D)
        v = lax.dot_general(rows, w, (((1,), (1,)), ((), ())), preferred_element_type=F32)
        gt = v[:, :HP]
        return (gt * jax.nn.sigmoid(gt) * v[:, HP:]).astype(BF)

    def nt_dot(rows, w):
        return lax.dot_general(rows, w, (((1,), (1,)), ((), ())), preferred_element_type=F32)

    def gate_row(zi):
        gates[zi] = nt_dot(nx[zi].reshape(256, D), gu[0, 0]).reshape(4, 64, HP)

    def with_gate(gt, rows):
        return (gt * jax.nn.sigmoid(gt) * nt_dot(rows, gu[0, 1])).astype(BF)

    def act_row(h, zi):
        if h == 1:
            act[zi] = gate_up(ng[zi].reshape(256, D), 1).reshape(4, 64, HP)
        else:
            act[zi] = with_gate(gates[zi].reshape(256, HP), nx[zi].reshape(256, D)).reshape(4, 64, HP)

    def act_col(xi):
        rows = nx[:, pl.ds(xi, 1)].reshape(256, D)
        act[:, pl.ds(xi, 1)] = with_gate(gates[:, pl.ds(xi, 1)].reshape(256, HP), rows).reshape(4, 1, 64, HP)

    OFF = (2, 3, 1, 0)

    def pv(h, ab, i, o):
        j = rem4((z if ab == 0 else x) + o)
        if ab == 0:
            return part.at[h, j, i, :, pl.ds(0, 1024)]
        return part.at[h, i, j, :, pl.ds(1024, 1024)]

    def dev1(ab, step):
        if ab == 0:
            return (4 * z + rem4(x + step + 4), t)
        return (4 * rem4(z + step + 4) + x, t)

    def me1(ab, step):
        return rem4((x if ab == 0 else z) + step + 4)

    def down_chunk(h, ab, step):
        idx = me1(ab, step)
        w = dd[h, :, 1024 * ab:1024 * ab + 1024]
        if ab == 0:
            a = act[:, pl.ds(idx, 1)].reshape(256, HP)
        else:
            a = act[idx].reshape(256, HP)
        v = jnp.dot(a, w, preferred_element_type=F32).astype(BF)
        if ab == 0:
            part[h, :, pl.ds(idx, 1), :, 0:1024] = v.reshape(4, 1, 64, 1024)
        else:
            part[h, idx, :, :, 1024:2048] = v.reshape(4, 64, 1024)

    def s1(h, ab, k, src, dst, dev):
        send(src, dst, rs_recv.at[ab, k], dev)

    def rs_away(h, ab):
        for o in OFF:
            s1(h, ab, o, pv(h, ab, me1(ab, 2), o), r2.at[h, ab, o], dev1(ab, 1 if o in (2, 1) else -1))

    def rs_direct(h, ab, o):
        if o in (2, 1):
            s1(h, ab, 8 + o, pv(h, ab, me1(ab, -1), o), rb.at[h, ab, o], dev1(ab, -1))
        else:
            s1(h, ab, 8 + o, pv(h, ab, me1(ab, 1), o), ra.at[h, ab, o], dev1(ab, 1))

    def rs_turn(h, ab, o):
        arrived(r2.at[h, ab, o], rs_recv.at[ab, o])
        step = 1 if o in (2, 1) else -1
        tt[h, ab, o] = (r2[h, ab, o].astype(F32) + pv(h, ab, me1(ab, step), o)[...].astype(F32)).astype(BF)
        s1(h, ab, 4 + o, tt.at[h, ab, o], (ra if step == 1 else rb).at[h, ab, o], dev1(ab, step))

    def rs_fin(h, ab, o):
        ka, kb = (4 + o, 8 + o) if o in (2, 1) else (8 + o, 4 + o)
        arrived(ra.at[h, ab, o], rs_recv.at[ab, ka])
        arrived(rb.at[h, ab, o], rs_recv.at[ab, kb])
        s = pv(h, ab, me1(ab, 0), o)[...].astype(F32) + ra[h, ab, o].astype(F32) + rb[h, ab, o].astype(F32)
        acc[ab, o] = s
        up2, dn2_ = dev1(1 - ab, 1), dev1(1 - ab, -1)
        lo, hi = pl.ds(0, 32), pl.ds(32, 32)
        if o != 0:
            sb[h, ab, o] = s.astype(BF)
        if o == 2:
            s1(h, ab, 12, sb.at[h, ab, o, lo], q2.at[h, ab, 0], up2)
            s1(h, ab, 13, sb.at[h, ab, o, hi], q2.at[h, ab, 1], dn2_)
        if o == 1:
            s1(h, ab, 15, sb.at[h, ab, o, hi], qa.at[h, ab, hi], up2)
        if o == 3:
            s1(h, ab, 16, sb.at[h, ab, o, lo], qb.at[h, ab, lo], dn2_)

    def rs_turn2(h, ab, o):
        if o == 1:
            arrived(q2.at[h, ab, 0], rs_recv.at[ab, 12])
            qt[h, ab, 0] = (q2[h, ab, 0].astype(F32) + acc[ab, 1, 0:32]).astype(BF)
            s1(h, ab, 14, qt.at[h, ab, 0], qa.at[h, ab, pl.ds(0, 32)], dev1(1 - ab, 1))
        else:
            arrived(q2.at[h, ab, 1], rs_recv.at[ab, 13])
            qt[h, ab, 1] = (q2[h, ab, 1].astype(F32) + acc[ab, 3, 32:64]).astype(BF)
            s1(h, ab, 17, qt.at[h, ab, 1], qb.at[h, ab, pl.ds(32, 32)], dev1(1 - ab, -1))

    def rs_out(h, ab):
        arrived(qa.at[h, ab, pl.ds(32, 32)], rs_recv.at[ab, 15])
        arrived(qb.at[h, ab, pl.ds(0, 32)], rs_recv.at[ab, 16])
        arrived(qa.at[h, ab, pl.ds(0, 32)], rs_recv.at[ab, 14])
        arrived(qb.at[h, ab, pl.ds(32, 32)], rs_recv.at[ab, 17])
        return acc[ab, 0] + qa[h, ab].astype(F32) + qb[h, ab].astype(F32)

    def rs_run(h, points):
        def point(k):
            for fn in points.get(k, ()):
                fn()

        down_chunk(h, 0, 2)
        rs_away(h, 0)
        down_chunk(h, 1, 2)
        rs_away(h, 1)
        point(0)
        down_chunk(h, 1, -1)
        rs_direct(h, 1, 2)
        point(1)
        down_chunk(h, 1, 1)
        point(2)
        down_chunk(h, 0, -1)
        rs_direct(h, 0, 2)
        down_chunk(h, 0, 1)
        for ab in (1, 0):
            rs_turn(h, ab, 2)
            rs_direct(h, ab, 3)
            rs_turn(h, ab, 3)
        point(3)
        for ab in (1, 0):
            rs_turn(h, ab, 1)
            rs_direct(h, ab, 1)
        for ab in range(2):
            down_chunk(h, ab, 0)
        for ab in (1, 0):
            rs_fin(h, ab, 2)
        for ab in (1, 0):
            rs_direct(h, ab, 0)
        for ab in (1, 0):
            rs_fin(h, ab, 3)
            rs_turn(h, ab, 0)
        point(4)
        for ab in (1, 0):
            rs_fin(h, ab, 1)
        point(5)
        for ab in (1, 0):
            rs_turn2(h, ab, 3)
            rs_turn2(h, ab, 1)
        for ab in (1, 0):
            rs_fin(h, ab, 0)
        point(6)
        return jnp.concatenate([rs_out(h, 0), rs_out(h, 1)], axis=-1)

    lo_rows, hi_rows = pl.ds(0, 32), pl.ds(32, 32)
    waited = set()

    def gv(ab, i, j, rows=slice(None)):
        zi, xi = (i, j) if ab == 0 else (j, i)
        return ng.at[rem4(z + zi), rem4(x + xi), rows, pl.ds(1024 * ab, 1024)]

    LAND = {
        0: (3, 0), 1: (1, 0), 2: (2, 0, lo_rows), 3: (2, 0, hi_rows),
        4: (0, 3), 5: (1, 3), 6: (2, 3), 7: (3, 3),
        8: (0, 1), 9: (1, 1), 10: (2, 1), 11: (3, 1),
        12: (0, 2), 13: (1, 2), 14: (3, 2), 15: (2, 2),
    }

    def got(ab, *slots):
        for k in slots:
            if (ab, k) not in waited:
                waited.add((ab, k))
                arrived(gv(ab, *LAND[k]), ag_recv.at[ab, k])

    def snd(ab, k, ref, second, step):
        send(ref, ref, ag_recv.at[ab, k], dev1(ab if second else 1 - ab, step))

    def ag_start():
        for ab in range(2):
            snd(ab, 0, gv(ab, 0, 0), False, 1)
            snd(ab, 1, gv(ab, 0, 0), False, -1)
        for ab in range(2):
            snd(ab, 4, gv(ab, 0, 0), True, 1)
            snd(ab, 8, gv(ab, 0, 0), True, -1)

    def ag_first():
        for ab in range(2):
            got(ab, 0)
            snd(ab, 2, gv(ab, 3, 0, lo_rows), False, 1)
            got(ab, 1)
            snd(ab, 3, gv(ab, 1, 0, hi_rows), False, -1)
        for ab in range(2):
            snd(ab, 5, gv(ab, 1, 0), True, 1)
            snd(ab, 11, gv(ab, 3, 0), True, -1)
            snd(ab, 7, gv(ab, 3, 0), True, 1)
            snd(ab, 9, gv(ab, 1, 0), True, -1)

    def ag_second():
        for ab in range(2):
            got(ab, 4)
            snd(ab, 12, gv(ab, 0, 3), True, 1)
        for ab in range(2):
            got(ab, 2, 3)
            snd(ab, 10, gv(ab, 2, 0), True, -1)
            snd(ab, 6, gv(ab, 2, 0), True, 1)

    def ag_third():
        for ab in range(2):
            got(ab, 5)
            snd(ab, 13, gv(ab, 1, 3), True, 1)
            got(ab, 8, 11)
            snd(ab, 14, gv(ab, 3, 1), True, -1)

    def ag_fourth():
        for ab in range(2):
            got(ab, 9, 10)
            snd(ab, 15, gv(ab, 2, 1), True, -1)

    def ag_row(oz):
        for k, v in LAND.items():
            if v[0] == oz:
                got(0, k)
            if v[1] == oz:
                got(1, k)

    def put(src, dst, k):
        pltpu.make_async_copy(src, dst, i_sem.at[k // 4, k % 4]).start()

    def put_wait(src, dst, k):
        pltpu.make_async_copy(src, dst, i_sem.at[k // 4, k % 4]).wait()

    def fold(h):
        for k in range(4):
            icp[4 * h + k].wait()
        for k in range(2):
            wt[h, k] = (raw_g[h] * raw_w[h, k]).astype(BF)
        dn[h] = raw_d[h].astype(BF)

    def norm_first(r):
        xcp[r].wait()
        for k in range(4):
            nx[r, k] = norm_rows(nx[r, k])

    fold(0)
    pl.semaphore_wait(barrier, 13 - n_self + n_fro)
    stage_a()
    d_own(0)
    for s_ in range(2):
        dd[s_, HB:HP, :] = jnp.zeros((HP - HB, D), BF)
        for k in range(2):
            gu[s_, k, HB:HP, :] = jnp.zeros((HP - HB, D), BF)
    for r in range(4):
        norm_first(r)
    fold(1)
    w_own()
    stage_a2()
    w_fwd(0)
    w_fwd(1)
    d_fwd(0)
    w_more(0)
    w_end(0)
    gate_row(0)
    gate_row(1)
    w_more(1)
    gate_row(2)
    gate_row(3)
    w_end(1)
    put(gu.at[0, 0, pl.ds(0, HB)], g1_o, 0)
    put(gu.at[0, 1, pl.ds(0, HB)], u1_o, 1)
    act_col(rem4(x + 2))
    act_row(0, rem4(z + 2))
    d_more(0)
    d_end(0)
    put(dd.at[0, pl.ds(0, HB)], d1_o, 2)
    branch = rs_run(0, {
        0: (lambda: hop(0, 0), lambda: hop(0, 1), lambda: act_row(0, rem4(z + 3))),
        1: (lambda: act_row(0, rem4(z + 1)),),
        2: (lambda: act_row(0, z),),
        3: (lambda: hop(1, 0),),
        4: (lambda: hop(1, 1),),
        5: (lambda: hop(2, 0), lambda: d_own(1)),
    })
    own_in.wait()
    m = (xown[...].astype(F32) + 0.5 * branch).astype(BF)
    mid[...] = m
    ng[z, x] = norm_rows(m)
    ag_start()
    hop(2, 1)
    ag_first()
    ag_second()
    hop(3, 0)
    ag_third()
    d_fwd(1)
    ag_fourth()
    hop(3, 1)
    hop_end()
    ag_row(0)
    act_row(1, z)
    put(gu.at[1, 0, pl.ds(0, HB)], g2_o, 3)
    put(gu.at[1, 1, pl.ds(0, HB)], u2_o, 4)
    for oz in (1, 3):
        ag_row(oz)
        act_row(1, rem4(z + oz))
        if oz == 1:
            d_more(1)
    ag_row(2)
    act_row(1, rem4(z + 2))
    d_end(1)
    put(dd.at[1, pl.ds(0, HB)], d2_o, 5)
    branch = rs_run(1, {})
    ost[...] = (mid[...].astype(F32) + 0.5 * branch).astype(BF)
    put(ost, ps_o, 6)

    drain()
    put_wait(gu.at[0, 0, pl.ds(0, HB)], g1_o, 0)
    put_wait(gu.at[0, 1, pl.ds(0, HB)], u1_o, 1)
    put_wait(dd.at[0, pl.ds(0, HB)], d1_o, 2)
    put_wait(gu.at[1, 0, pl.ds(0, HB)], g2_o, 3)
    put_wait(gu.at[1, 1, pl.ds(0, HB)], u2_o, 4)
    put_wait(dd.at[1, pl.ds(0, HB)], d2_o, 5)
    put_wait(ost, ps_o, 6)


def copy_out(*refs):
    n = len(refs) // 2
    sems = refs[-1]
    cps = [pltpu.make_async_copy(refs[k], refs[n + k], sems.at[k]) for k in range(n)]
    for cp in cps:
        cp.start()
    for cp in cps:
        cp.wait()


def run(xin, *weights):
    vm = pltpu.VMEM
    dma = pltpu.SemaphoreType.DMA
    w_out = jax.ShapeDtypeStruct((HB, D), BF)
    out_shape = (w_out,) * 6 + (jax.ShapeDtypeStruct((64, D), BF),)
    unit = (2, 2, 4, 64, 1024)
    half = (2, 2, 2, 32, 1024)
    one = (2, 2, 64, 1024)
    scratch = [
        vm((4, 4, 64, D), BF), vm((4, 4, 64, D), BF), vm((64, D), BF), vm((64, D), BF),
        vm((2, 2, 2 * HB, 128), F32), vm((2, HB, 256), F32), vm((2, 1, 128), F32),
        vm((2, 2, 2 * HB, 128), BF), vm((2, HB, 256), BF),
        vm((2, 2, HP, D), BF), vm((2, HP, D), BF), vm((4, 4, 64, HP), BF), vm((2, 4, 4, 64, D), BF),
        vm((4, 4, 64, HP), F32),
        vm(unit, BF), vm(unit, BF), vm(unit, BF), vm(unit, BF), vm((2, 4, 64, 1024), F32), vm(unit, BF),
        vm(half, BF), vm(one, BF), vm(one, BF), vm(half, BF), vm((64, D), BF),
        dma((POOL,)), dma((2, 16)), dma((16,)), dma((16,)), dma((2, 8, 2)), dma((2,)), dma((2, 18)), dma((2, 16)),
        dma((5,)), dma((2, 4)),
    ]
    here = [pltpu.with_memory_space_constraint(v, pltpu.HBM) for v in (xin, *weights)]
    outs = pl.pallas_call(
        kernel,
        out_shape=tuple(pltpu.VMEM(o.shape, o.dtype) for o in out_shape),
        in_specs=[pl.BlockSpec(memory_space=pltpu.HBM)] * 9,
        out_specs=tuple(pl.BlockSpec(memory_space=pl.ANY) for _ in range(7)),
        scratch_shapes=scratch,
        compiler_params=pltpu.CompilerParams(
            collective_id=0, has_side_effects=True, vmem_limit_bytes=VMEM_MB * 1024 * 1024
        ),
    )(*here)
    return pl.pallas_call(
        copy_out,
        out_shape=out_shape,
        in_specs=[pl.BlockSpec(memory_space=pl.ANY)] * 7,
        out_specs=tuple(pl.BlockSpec(memory_space=pltpu.HBM) for _ in range(7)),
        scratch_shapes=[dma((7,))],
        compiler_params=pltpu.CompilerParams(vmem_limit_bytes=1024 * 1024),
    )(*outs)


def per_device(
    prompts, gain_first, gate_first, up_first, down_first, gain_second, gate_second, up_second, down_second
):
    xin = prompts.reshape(4, 4, 64, D)
    g1, u1, d1, g2, u2, d2, ps = run(
        xin,
        gain_first.reshape(1, 128), gate_first.T, up_first.T, down_first,
        gain_second.reshape(1, 128), gate_second.T, up_second.T, down_second,
    )
    return g1.T, u1.T, d1, g2.T, u2.T, d2, ps.reshape(1, 64, D)


def solution(mesh):
    w = P("fs", "tp")
    return jax.shard_map(
        per_device,
        mesh=mesh,
        in_specs=(P("tp", None, None), P("fs"), w, w, w, P("fs"), w, w, w),
        out_specs=(
            P(None, "fs"), P(None, "fs"), P("fs", None),
            P(None, "fs"), P(None, "fs"), P("fs", None),
            P("tp", "fs", None),
        ),
        check_vma=False,
    )
```

```python
import functools

import jax
import jax.numpy as jnp
from jax import lax
from jax.experimental import pallas as pl
from jax.experimental.pallas import tpu as pltpu
from jax.sharding import PartitionSpec as P

D = 2048
FF = 5632
HB = 352
HP = 384
TOK = 1024
MESH = pl.DeviceIdType.MESH
BF = jnp.bfloat16
F32 = jnp.float32
VMEM_MB = 53
POOL = 40


def rem4(v):
    return lax.rem(v, 4)


def kernel(
    x_hbm, gn1, gt1, ut1, dn1, gn2, gt2, ut2, dn2,
    g1_o, u1_o, d1_o, g2_o, u2_o, d2_o, ps_o,
    nx, ng, xown, mid, raw_w, raw_d, raw_g, wt, dn, gu, dd, act, part,
    gates, r2, ra, rb, tt, acc, sb, q2, qa, qb, qt, ost,
    pool, w1_recv, w_recv, w_send, d_recv, d_loc, rs_recv, x_sem, i_sem,
):
    f = lax.axis_index("fs")
    t = lax.axis_index("tp")
    z = lax.div(f, 4)
    x = lax.rem(f, 4)
    y = lax.div(t, 2)
    core = lax.rem(t, 2)
    sib = (f, 2 * y + 1 - core)
    pending = []

    def remote(src, dst, ssem, rsem, dev):
        return pltpu.make_async_remote_copy(
            src_ref=src, dst_ref=dst, send_sem=ssem, recv_sem=rsem, device_id=dev, device_id_type=MESH
        )

    taken = []

    def settle(src, dst, ssem, rsem, dev, cond):
        if cond is None:
            remote(src, dst, ssem, rsem, dev).wait_send()
        else:
            pl.when(cond)(lambda: remote(src, dst, ssem, rsem, dev).wait_send())

    def send(src, dst, rsem, dev, cond=None):
        k = len(taken)
        if k >= POOL:
            settle(*taken[k - POOL])
        ssem = pool.at[k % POOL]
        if cond is None:
            remote(src, dst, ssem, rsem, dev).start()
        else:
            pl.when(cond)(lambda: remote(src, dst, ssem, rsem, dev).start())
        taken.append((src, dst, ssem, rsem, dev, cond))

    def drain():
        for item in taken[-POOL:] + pending:
            settle(*item)

    def arrived(dst, sem):
        pltpu.make_async_copy(dst, dst, sem).wait()

    def a_dt(g):
        return 2 * rem4(y + 2 + x - 2 * core - g + 4) + lax.div(z, 2)

    def tile_id(yy, cc, q):
        return 4 * (2 * cc + q) + rem4(yy - z + 2 + x + 4)

    barrier = pltpu.get_barrier_semaphore()

    def greet(dev):
        pl.semaphore_signal(barrier, inc=1, device_id=dev, device_id_type=MESH)

    near = [(f, 2 * rem4(y + 1) + core), (f, 2 * rem4(y + 3) + core), sib]
    near += [(4 * z + rem4(x + 1), t), (4 * z + rem4(x + 3), t), (4 * rem4(z + 1) + x, t), (4 * rem4(z + 3) + x, t)]
    for dev in near:
        greet(dev)
    n_self = jnp.int32(0)
    for g in range(2):
        to = (4 * y + 2 * core + g, a_dt(g))
        fro = (tile_id(y, core, g), 2 * z + lax.div(x, 2))
        to_self = jnp.logical_and(to[0] == f, to[1] == t)
        fro_self = jnp.logical_and(fro[0] == f, fro[1] == t)
        pl.when(jnp.logical_not(to_self))(functools.partial(greet, to))
        pl.when(jnp.logical_not(fro_self))(functools.partial(greet, fro))
        n_self = n_self + to_self.astype(jnp.int32) + fro_self.astype(jnp.int32)

    par = lax.rem(x + z, 2)
    for g in range(2):
        to = (4 * y + 2 * core + g, 2 * y + par)
        to_self = jnp.logical_and(to[0] == f, to[1] == t)
        pl.when(jnp.logical_not(to_self))(functools.partial(greet, to))
        n_self = n_self + to_self.astype(jnp.int32)
    n_fro = jnp.int32(0)
    for z2 in range(4):
        for k in range(2):
            fr = (4 * z2 + 2 * k + lax.rem(z2 + core, 2), 2 * y + lax.div(x, 2))
            is_self = jnp.logical_and(fr[0] == f, fr[1] == t)
            there = jnp.logical_and(y == z, jnp.logical_not(is_self))
            pl.when(there)(functools.partial(greet, fr))
            n_fro = n_fro + there.astype(jnp.int32)

    icp = []
    for h, (gn, gt, ut, dw) in enumerate(((gn1, gt1, ut1, dn1), (gn2, gt2, ut2, dn2))):
        for k, (src, dst) in enumerate(
            ((gn, raw_g.at[h]), (gt, raw_w.at[h, 0]), (ut, raw_w.at[h, 1]), (dw, raw_d.at[h]))
        ):
            cp = pltpu.make_async_copy(src, dst, i_sem.at[h, k])
            cp.start()
            icp.append(cp)
    xcp = []
    for r in range(4):
        cp = pltpu.make_async_copy(x_hbm.at[r], nx.at[r], x_sem.at[r])
        cp.start()
        xcp.append(cp)
    own_in = pltpu.make_async_copy(x_hbm.at[z, x], xown, x_sem.at[4])
    own_in.start()

    yp, ym, y2 = rem4(y + 1), rem4(y + 3), rem4(y + 2)


    def w1(k, ft):
        return gu.at[0, k, pl.ds(0, HB), pl.ds(pl.multiple_of(ft * 128, 128), 128)]

    def stage_a():
        for k in range(2):
            for g in range(2):
                src = wt.at[0, k, pl.ds(HB * g, HB), :]
                dev = (4 * y + 2 * core + g, a_dt(g))
                same = jnp.logical_and(dev[0] == f, dev[1] == t)
                send(src, w1(k, f), w1_recv.at[k, f], dev, jnp.logical_not(same))

                @pl.when(same)
                def _(src=src, k=k):
                    pltpu.make_async_copy(src, w1(k, f), w1_recv.at[k, f]).start()

    def wv(ft):
        return gu.at[1, :, pl.ds(0, HB), pl.ds(pl.multiple_of(ft * 128, 128), 128)]

    def stage_a2():
        for g in range(2):
            src = wt.at[1, :, pl.ds(HB * g, HB), :]
            dev = (4 * y + 2 * core + g, 2 * y + par)
            same = jnp.logical_and(dev[0] == f, dev[1] == t)
            send(src, wv(f), w_recv.at[f], dev, jnp.logical_not(same))

            @pl.when(same)
            def _(src=src):
                pltpu.make_async_copy(src, wv(f), w_recv.at[f]).start()

    nxt = (f, 2 * rem4(y + 1 + 2 * core) + core)
    dist = rem4(jnp.where(core == 0, y - z, z - y) + 4)

    def chain_tile(i, cc):
        z2, k = i // 2, i % 2
        return 4 * z2 + 2 * k + lax.rem(z2 + cc, 2)

    def hop(d, batch):
        @pl.when(dist == d)
        def _():
            for i in range(4 * batch, 4 * batch + 4):
                ft = chain_tile(i, core)
                tile = wv(ft)
                arrived(tile, w_recv.at[ft])
                if d < 3:
                    remote(tile, tile, w_send.at[i], w_recv.at[ft], nxt).start()
                remote(tile, tile, w_send.at[8 + i], w_recv.at[ft], sib).start()

    def hop_end():
        for i in range(8):
            ft = chain_tile(i, core)
            tile = wv(ft)
            pending.append((tile, tile, w_send.at[i], w_recv.at[ft], nxt, dist < 3))
            pending.append((tile, tile, w_send.at[8 + i], w_recv.at[ft], sib, None))
            fo = chain_tile(i, 1 - core)
            arrived(wv(fo), w_recv.at[fo])

    def wsend(k, ft, dev):
        send(w1(k, ft), w1(k, ft), w1_recv.at[k, ft], dev)

    def wgot(k, ft):
        arrived(w1(k, ft), w1_recv.at[k, ft])

    up_dev, dn_dev = (f, 2 * yp + core), (f, 2 * ym + core)

    def w_own():
        for k in range(2):
            for q in range(2):
                ft = tile_id(y, core, q)
                wgot(k, ft)
                for dev in (up_dev, dn_dev, sib):
                    wsend(k, ft, dev)

    def w_fwd(k):
        lo, hi = tile_id(ym, core, 0), tile_id(yp, core, 1)
        wgot(k, lo)
        wsend(k, lo, up_dev)
        wgot(k, hi)
        wsend(k, hi, dn_dev)
        wsend(k, lo, sib)
        wsend(k, hi, sib)

    def w_more(k):
        for ft in (tile_id(ym, core, 1), tile_id(yp, core, 0)):
            wgot(k, ft)
            wsend(k, ft, sib)
        for q in range(2):
            ft = tile_id(y2, core, q)
            wgot(k, ft)
            wsend(k, ft, sib)

    def w_end(k):
        for yy in range(4):
            for q in range(2):
                wgot(k, tile_id(yy, 1 - core, q))

    def dblk(h, tb, q):
        return dd.at[h, pl.ds(176 * q, 176), pl.ds(pl.multiple_of(tb * 256, 256), 256)]

    def d_local(h):
        return pltpu.make_async_copy(
            dn.at[h], dd.at[h, pl.ds(0, HB), pl.ds(pl.multiple_of(t * 256, 256), 256)], d_loc.at[h]
        )

    def dsend(h, tb, q, dev):
        send(dblk(h, tb, q), dblk(h, tb, q), d_recv.at[h, tb, q], dev)

    def d_own(h):
        d_local(h).start()
        for q in range(2):
            src = dn.at[h, pl.ds(176 * q, 176), :]
            for dev in (up_dev, dn_dev, sib):
                send(src, dblk(h, t, q), d_recv.at[h, t, q], dev)

    def d_fwd(h):
        tm, tp = 2 * ym + core, 2 * yp + core
        arrived(dblk(h, tm, 0), d_recv.at[h, tm, 0])
        dsend(h, tm, 0, up_dev)
        arrived(dblk(h, tp, 1), d_recv.at[h, tp, 1])
        dsend(h, tp, 1, dn_dev)
        dsend(h, tm, 0, sib)
        dsend(h, tp, 1, sib)

    def d_more(h):
        for tb, q in ((2 * ym + core, 1), (2 * yp + core, 0), (2 * y2 + core, 0), (2 * y2 + core, 1)):
            arrived(dblk(h, tb, q), d_recv.at[h, tb, q])
            dsend(h, tb, q, sib)

    def d_end(h):
        for yy in range(4):
            for q in range(2):
                tb = 2 * yy + 1 - core
                arrived(dblk(h, tb, q), d_recv.at[h, tb, q])
        d_local(h).wait()

    def norm_rows(v):
        w = v.astype(F32)
        return (w * lax.rsqrt(jnp.mean(w * w, axis=-1, keepdims=True) + 1e-06)).astype(BF)

    def gate_up(rows, slot):
        w = gu[slot].reshape(2 * HP, D)
        v = lax.dot_general(rows, w, (((1,), (1,)), ((), ())), preferred_element_type=F32)
        gt = v[:, :HP]
        return (gt * jax.nn.sigmoid(gt) * v[:, HP:]).astype(BF)

    def nt_dot(rows, w):
        return lax.dot_general(rows, w, (((1,), (1,)), ((), ())), preferred_element_type=F32)

    def gate_row(zi):
        gates[zi] = nt_dot(nx[zi].reshape(256, D), gu[0, 0]).reshape(4, 64, HP)

    def with_gate(gt, rows):
        return (gt * jax.nn.sigmoid(gt) * nt_dot(rows, gu[0, 1])).astype(BF)

    def act_row(h, zi):
        if h == 1:
            act[zi] = gate_up(ng[zi].reshape(256, D), 1).reshape(4, 64, HP)
        else:
            act[zi] = with_gate(gates[zi].reshape(256, HP), nx[zi].reshape(256, D)).reshape(4, 64, HP)

    def act_col(xi):
        rows = nx[:, pl.ds(xi, 1)].reshape(256, D)
        act[:, pl.ds(xi, 1)] = with_gate(gates[:, pl.ds(xi, 1)].reshape(256, HP), rows).reshape(4, 1, 64, HP)

    OFF = (2, 3, 1, 0)

    def pv(h, ab, i, o):
        j = rem4((z if ab == 0 else x) + o)
        if ab == 0:
            return part.at[h, j, i, :, pl.ds(0, 1024)]
        return part.at[h, i, j, :, pl.ds(1024, 1024)]

    def dev1(ab, step):
        if ab == 0:
            return (4 * z + rem4(x + step + 4), t)
        return (4 * rem4(z + step + 4) + x, t)

    def me1(ab, step):
        return rem4((x if ab == 0 else z) + step + 4)

    def down_chunk(h, ab, step):
        idx = me1(ab, step)
        w = dd[h, :, 1024 * ab:1024 * ab + 1024]
        if ab == 0:
            a = act[:, pl.ds(idx, 1)].reshape(256, HP)
        else:
            a = act[idx].reshape(256, HP)
        v = jnp.dot(a, w, preferred_element_type=F32).astype(BF)
        if ab == 0:
            part[h, :, pl.ds(idx, 1), :, 0:1024] = v.reshape(4, 1, 64, 1024)
        else:
            part[h, idx, :, :, 1024:2048] = v.reshape(4, 64, 1024)

    def s1(h, ab, k, src, dst, dev):
        send(src, dst, rs_recv.at[ab, k], dev)

    def rs_away(h, ab):
        for o in OFF:
            s1(h, ab, o, pv(h, ab, me1(ab, 2), o), r2.at[h, ab, o], dev1(ab, 1 if o in (2, 1) else -1))

    def rs_direct(h, ab, o):
        if o in (2, 1):
            s1(h, ab, 8 + o, pv(h, ab, me1(ab, -1), o), rb.at[h, ab, o], dev1(ab, -1))
        else:
            s1(h, ab, 8 + o, pv(h, ab, me1(ab, 1), o), ra.at[h, ab, o], dev1(ab, 1))

    def rs_turn(h, ab, o):
        arrived(r2.at[h, ab, o], rs_recv.at[ab, o])
        step = 1 if o in (2, 1) else -1
        tt[h, ab, o] = (r2[h, ab, o].astype(F32) + pv(h, ab, me1(ab, step), o)[...].astype(F32)).astype(BF)
        s1(h, ab, 4 + o, tt.at[h, ab, o], (ra if step == 1 else rb).at[h, ab, o], dev1(ab, step))

    def rs_fin(h, ab, o):
        ka, kb = (4 + o, 8 + o) if o in (2, 1) else (8 + o, 4 + o)
        arrived(ra.at[h, ab, o], rs_recv.at[ab, ka])
        arrived(rb.at[h, ab, o], rs_recv.at[ab, kb])
        s = pv(h, ab, me1(ab, 0), o)[...].astype(F32) + ra[h, ab, o].astype(F32) + rb[h, ab, o].astype(F32)
        acc[ab, o] = s
        up2, dn2_ = dev1(1 - ab, 1), dev1(1 - ab, -1)
        lo, hi = pl.ds(0, 32), pl.ds(32, 32)
        if o != 0:
            sb[h, ab, o] = s.astype(BF)
        if o == 2:
            s1(h, ab, 12, sb.at[h, ab, o, lo], q2.at[h, ab, 0], up2)
            s1(h, ab, 13, sb.at[h, ab, o, hi], q2.at[h, ab, 1], dn2_)
        if o == 1:
            s1(h, ab, 15, sb.at[h, ab, o, hi], qa.at[h, ab, hi], up2)
        if o == 3:
            s1(h, ab, 16, sb.at[h, ab, o, lo], qb.at[h, ab, lo], dn2_)

    def rs_turn2(h, ab, o):
        if o == 1:
            arrived(q2.at[h, ab, 0], rs_recv.at[ab, 12])
            qt[h, ab, 0] = (q2[h, ab, 0].astype(F32) + acc[ab, 1, 0:32]).astype(BF)
            s1(h, ab, 14, qt.at[h, ab, 0], qa.at[h, ab, pl.ds(0, 32)], dev1(1 - ab, 1))
        else:
            arrived(q2.at[h, ab, 1], rs_recv.at[ab, 13])
            qt[h, ab, 1] = (q2[h, ab, 1].astype(F32) + acc[ab, 3, 32:64]).astype(BF)
            s1(h, ab, 17, qt.at[h, ab, 1], qb.at[h, ab, pl.ds(32, 32)], dev1(1 - ab, -1))

    def rs_out(h, ab):
        arrived(qa.at[h, ab, pl.ds(32, 32)], rs_recv.at[ab, 15])
        arrived(qb.at[h, ab, pl.ds(0, 32)], rs_recv.at[ab, 16])
        arrived(qa.at[h, ab, pl.ds(0, 32)], rs_recv.at[ab, 14])
        arrived(qb.at[h, ab, pl.ds(32, 32)], rs_recv.at[ab, 17])
        return acc[ab, 0] + qa[h, ab].astype(F32) + qb[h, ab].astype(F32)

    def rs_run(h, points):
        def point(k):
            for fn in points.get(k, ()):
                fn()

        down_chunk(h, 0, 2)
        rs_away(h, 0)
        down_chunk(h, 1, 2)
        rs_away(h, 1)
        point(0)
        down_chunk(h, 1, -1)
        rs_direct(h, 1, 2)
        point(1)
        down_chunk(h, 1, 1)
        point(2)
        down_chunk(h, 0, -1)
        rs_direct(h, 0, 2)
        down_chunk(h, 0, 1)
        for ab in (1, 0):
            rs_turn(h, ab, 2)
            rs_direct(h, ab, 3)
            rs_turn(h, ab, 3)
        for ab in (1, 0):
            rs_turn(h, ab, 1)
            rs_direct(h, ab, 1)
        for ab in range(2):
            down_chunk(h, ab, 0)
        for ab in (1, 0):
            rs_fin(h, ab, 2)
        for ab in (1, 0):
            rs_direct(h, ab, 0)
        point(3)
        for ab in (1, 0):
            rs_fin(h, ab, 3)
            rs_turn(h, ab, 0)
        point(4)
        for ab in (1, 0):
            rs_fin(h, ab, 1)
        point(5)
        for ab in (1, 0):
            rs_turn2(h, ab, 3)
            rs_turn2(h, ab, 1)
        for ab in (1, 0):
            rs_fin(h, ab, 0)
        point(6)
        return jnp.concatenate([rs_out(h, 0), rs_out(h, 1)], axis=-1)

    lo_rows, hi_rows = pl.ds(0, 32), pl.ds(32, 32)
    waited = set()

    def gv(ab, i, j, rows=slice(None)):
        zi, xi = (i, j) if ab == 0 else (j, i)
        return ng.at[rem4(z + zi), rem4(x + xi), rows, pl.ds(1024 * ab, 1024)]

    LAND = {
        0: (3, 0), 1: (1, 0), 2: (2, 0, lo_rows), 3: (2, 0, hi_rows),
        4: (0, 3), 5: (1, 3), 6: (2, 3), 7: (3, 3),
        8: (0, 1), 9: (1, 1), 10: (2, 1), 11: (3, 1),
        12: (0, 2), 13: (1, 2), 14: (3, 2), 15: (2, 2),
    }

    def got(ab, *slots):
        for k in slots:
            if (ab, k) not in waited:
                waited.add((ab, k))
                arrived(gv(ab, *LAND[k]), w1_recv.at[ab, k])

    def snd(ab, k, ref, second, step):
        send(ref, ref, w1_recv.at[ab, k], dev1(ab if second else 1 - ab, step))

    def ag_start():
        for ab in range(2):
            snd(ab, 0, gv(ab, 0, 0), False, 1)
            snd(ab, 1, gv(ab, 0, 0), False, -1)
        for ab in range(2):
            snd(ab, 4, gv(ab, 0, 0), True, 1)
            snd(ab, 8, gv(ab, 0, 0), True, -1)

    def ag_first():
        for ab in range(2):
            got(ab, 0)
            snd(ab, 2, gv(ab, 3, 0, lo_rows), False, 1)
            got(ab, 1)
            snd(ab, 3, gv(ab, 1, 0, hi_rows), False, -1)
        for ab in range(2):
            snd(ab, 5, gv(ab, 1, 0), True, 1)
            snd(ab, 11, gv(ab, 3, 0), True, -1)
            snd(ab, 7, gv(ab, 3, 0), True, 1)
            snd(ab, 9, gv(ab, 1, 0), True, -1)

    def ag_second():
        for ab in range(2):
            got(ab, 4)
            snd(ab, 12, gv(ab, 0, 3), True, 1)
        for ab in range(2):
            got(ab, 2, 3)
            snd(ab, 10, gv(ab, 2, 0), True, -1)
            snd(ab, 6, gv(ab, 2, 0), True, 1)

    def ag_third():
        for ab in range(2):
            got(ab, 5)
            snd(ab, 13, gv(ab, 1, 3), True, 1)
            got(ab, 8, 11)
            snd(ab, 14, gv(ab, 3, 1), True, -1)

    def ag_fourth():
        for ab in range(2):
            got(ab, 9, 10)
            snd(ab, 15, gv(ab, 2, 1), True, -1)

    def ag_row(oz):
        for k, v in LAND.items():
            if v[0] == oz:
                got(0, k)
            if v[1] == oz:
                got(1, k)

    def put(src, dst, k):
        pltpu.make_async_copy(src, dst, i_sem.at[k // 4, k % 4]).start()

    def put_wait(src, dst, k):
        pltpu.make_async_copy(src, dst, i_sem.at[k // 4, k % 4]).wait()

    def fold(h):
        for k in range(4):
            icp[4 * h + k].wait()
        for k in range(2):
            wt[h, k] = (raw_g[h] * raw_w[h, k]).astype(BF)
        dn[h] = raw_d[h].astype(BF)

    def norm_first(r):
        xcp[r].wait()
        for k in range(4):
            nx[r, k] = norm_rows(nx[r, k])

    fold(0)
    pl.semaphore_wait(barrier, 13 - n_self + n_fro)
    stage_a()
    d_own(0)
    for s_ in range(2):
        dd[s_, HB:HP, :] = jnp.zeros((HP - HB, D), BF)
        for k in range(2):
            gu[s_, k, HB:HP, :] = jnp.zeros((HP - HB, D), BF)
    for r in range(4):
        norm_first(r)
    fold(1)
    w_own()
    stage_a2()
    w_fwd(0)
    w_fwd(1)
    d_fwd(0)
    w_more(0)
    w_end(0)
    gate_row(0)
    gate_row(1)
    w_more(1)
    gate_row(2)
    gate_row(3)
    w_end(1)
    d_more(0)
    put(gu.at[0, 0, pl.ds(0, HB)], g1_o, 0)
    put(gu.at[0, 1, pl.ds(0, HB)], u1_o, 1)
    act_col(rem4(x + 2))
    act_row(0, rem4(z + 2))
    d_end(0)
    put(dd.at[0, pl.ds(0, HB)], d1_o, 2)
    branch = rs_run(0, {
        0: (lambda: hop(0, 0), lambda: hop(0, 1), lambda: act_row(0, rem4(z + 3))),
        1: (lambda: act_row(0, rem4(z + 1)),),
        2: (lambda: act_row(0, z),),
        3: (lambda: hop(1, 0),),
        5: (lambda: hop(1, 1), lambda: d_own(1)),
    })
    own_in.wait()
    m = (xown[...].astype(F32) + 0.5 * branch).astype(BF)
    mid[...] = m
    ng[z, x] = norm_rows(m)
    ag_start()
    hop(2, 0)
    ag_first()
    hop(2, 1)
    ag_second()
    ag_third()
    d_fwd(1)
    ag_fourth()
    hop(3, 0)
    hop(3, 1)
    hop_end()
    ag_row(0)
    act_row(1, z)
    put(gu.at[1, 0, pl.ds(0, HB)], g2_o, 3)
    put(gu.at[1, 1, pl.ds(0, HB)], u2_o, 4)
    for oz in (1, 3):
        ag_row(oz)
        act_row(1, rem4(z + oz))
        if oz == 1:
            d_more(1)
    ag_row(2)
    act_row(1, rem4(z + 2))
    d_end(1)
    put(dd.at[1, pl.ds(0, HB)], d2_o, 5)
    branch = rs_run(1, {})
    ost[...] = (mid[...].astype(F32) + 0.5 * branch).astype(BF)
    put(ost, ps_o, 6)

    drain()
    put_wait(gu.at[0, 0, pl.ds(0, HB)], g1_o, 0)
    put_wait(gu.at[0, 1, pl.ds(0, HB)], u1_o, 1)
    put_wait(dd.at[0, pl.ds(0, HB)], d1_o, 2)
    put_wait(gu.at[1, 0, pl.ds(0, HB)], g2_o, 3)
    put_wait(gu.at[1, 1, pl.ds(0, HB)], u2_o, 4)
    put_wait(dd.at[1, pl.ds(0, HB)], d2_o, 5)
    put_wait(ost, ps_o, 6)


def copy_out(*refs):
    n = len(refs) // 2
    sems = refs[-1]
    cps = [pltpu.make_async_copy(refs[k], refs[n + k], sems.at[k]) for k in range(n)]
    for cp in cps:
        cp.start()
    for cp in cps:
        cp.wait()


def run(xin, *weights):
    vm = pltpu.VMEM
    dma = pltpu.SemaphoreType.DMA
    w_out = jax.ShapeDtypeStruct((HB, D), BF)
    out_shape = (w_out,) * 6 + (jax.ShapeDtypeStruct((64, D), BF),)
    unit = (2, 2, 4, 64, 1024)
    half = (2, 2, 2, 32, 1024)
    one = (2, 2, 64, 1024)
    scratch = [
        vm((4, 4, 64, D), BF), vm((4, 4, 64, D), BF), vm((64, D), BF), vm((64, D), BF),
        vm((2, 2, 2 * HB, 128), F32), vm((2, HB, 256), F32), vm((2, 1, 128), F32),
        vm((2, 2, 2 * HB, 128), BF), vm((2, HB, 256), BF),
        vm((2, 2, HP, D), BF), vm((2, HP, D), BF), vm((4, 4, 64, HP), BF), vm((2, 4, 4, 64, D), BF),
        vm((4, 4, 64, HP), F32),
        vm(unit, BF), vm(unit, BF), vm(unit, BF), vm(unit, BF), vm((2, 4, 64, 1024), F32), vm(unit, BF),
        vm(half, BF), vm(one, BF), vm(one, BF), vm(half, BF), vm((64, D), BF),
        dma((POOL,)), dma((2, 16)), dma((16,)), dma((16,)), dma((2, 8, 2)), dma((2,)), dma((2, 18)),
        dma((5,)), dma((2, 4)),
    ]
    here = [pltpu.with_memory_space_constraint(v, pltpu.HBM) for v in (xin, *weights)]
    outs = pl.pallas_call(
        kernel,
        out_shape=tuple(pltpu.VMEM(o.shape, o.dtype) for o in out_shape),
        in_specs=[pl.BlockSpec(memory_space=pltpu.HBM)] * 9,
        out_specs=tuple(pl.BlockSpec(memory_space=pl.ANY) for _ in range(7)),
        scratch_shapes=scratch,
        compiler_params=pltpu.CompilerParams(
            collective_id=0, has_side_effects=True, vmem_limit_bytes=VMEM_MB * 1024 * 1024
        ),
    )(*here)
    return pl.pallas_call(
        copy_out,
        out_shape=out_shape,
        in_specs=[pl.BlockSpec(memory_space=pl.ANY)] * 7,
        out_specs=tuple(pl.BlockSpec(memory_space=pltpu.HBM) for _ in range(7)),
        scratch_shapes=[dma((7,))],
        compiler_params=pltpu.CompilerParams(vmem_limit_bytes=1024 * 1024),
    )(*outs)


def per_device(
    prompts, gain_first, gate_first, up_first, down_first, gain_second, gate_second, up_second, down_second
):
    xin = prompts.reshape(4, 4, 64, D)
    g1, u1, d1, g2, u2, d2, ps = run(
        xin,
        gain_first.reshape(1, 128), gate_first.T, up_first.T, down_first,
        gain_second.reshape(1, 128), gate_second.T, up_second.T, down_second,
    )
    return g1.T, u1.T, d1, g2.T, u2.T, d2, ps.reshape(1, 64, D)


def solution(mesh):
    w = P("fs", "tp")
    return jax.shard_map(
        per_device,
        mesh=mesh,
        in_specs=(P("tp", None, None), P("fs"), w, w, w, P("fs"), w, w, w),
        out_specs=(
            P(None, "fs"), P(None, "fs"), P("fs", None),
            P(None, "fs"), P(None, "fs"), P("fs", None),
            P("tp", "fs", None),
        ),
        check_vma=False,
    )
```

```python
import functools

import jax
import jax.numpy as jnp
from jax import lax
from jax.experimental import pallas as pl
from jax.experimental.pallas import tpu as pltpu
from jax.sharding import PartitionSpec as P

D = 2048
FF = 5632
HB = 352
HP = 384
TOK = 1024
MESH = pl.DeviceIdType.MESH
BF = jnp.bfloat16
F32 = jnp.float32
VMEM_MB = 53
POOL = 32


def rem4(v):
    return lax.rem(v, 4)


def kernel(
    x_hbm, gn1, gt1, ut1, dn1, gn2, gt2, ut2, dn2,
    g1_o, u1_o, d1_o, g2_o, u2_o, d2_o, ps_o,
    nx, ng, xown, mid, raw_w, raw_d, raw_g, wt, dn, gu, dd, act, part,
    gates, r2, ra, rb, tt, acc, sb, q2, qa, qb, qt, ost,
    pool, w1_recv, w_recv, w_send, d_recv, d_loc, rs_recv, x_sem, i_sem,
):
    f = lax.axis_index("fs")
    t = lax.axis_index("tp")
    z = lax.div(f, 4)
    x = lax.rem(f, 4)
    y = lax.div(t, 2)
    core = lax.rem(t, 2)
    sib = (f, 2 * y + 1 - core)
    pending = []

    def remote(src, dst, ssem, rsem, dev):
        return pltpu.make_async_remote_copy(
            src_ref=src, dst_ref=dst, send_sem=ssem, recv_sem=rsem, device_id=dev, device_id_type=MESH
        )

    taken = []

    def settle(src, dst, ssem, rsem, dev, cond):
        if cond is None:
            remote(src, dst, ssem, rsem, dev).wait_send()
        else:
            pl.when(cond)(lambda: remote(src, dst, ssem, rsem, dev).wait_send())

    def send(src, dst, rsem, dev, cond=None):
        k = len(taken)
        if k >= POOL:
            settle(*taken[k - POOL])
        ssem = pool.at[k % POOL]
        if cond is None:
            remote(src, dst, ssem, rsem, dev).start()
        else:
            pl.when(cond)(lambda: remote(src, dst, ssem, rsem, dev).start())
        taken.append((src, dst, ssem, rsem, dev, cond))

    def drain():
        for item in taken[-POOL:] + pending:
            settle(*item)

    def arrived(dst, sem):
        pltpu.make_async_copy(dst, dst, sem).wait()

    def a_dt(g):
        return 2 * rem4(y + 2 + x - 2 * core - g + 4) + lax.div(z, 2)

    def tile_id(yy, cc, q):
        return 4 * (2 * cc + q) + rem4(yy - z + 2 + x + 4)

    barrier = pltpu.get_barrier_semaphore()

    def greet(dev):
        pl.semaphore_signal(barrier, inc=1, device_id=dev, device_id_type=MESH)

    near = [(f, 2 * rem4(y + 1) + core), (f, 2 * rem4(y + 3) + core), sib]
    near += [(4 * z + rem4(x + 1), t), (4 * z + rem4(x + 3), t), (4 * rem4(z + 1) + x, t), (4 * rem4(z + 3) + x, t)]
    for dev in near:
        greet(dev)
    n_self = jnp.int32(0)
    for g in range(2):
        to = (4 * y + 2 * core + g, a_dt(g))
        fro = (tile_id(y, core, g), 2 * z + lax.div(x, 2))
        to_self = jnp.logical_and(to[0] == f, to[1] == t)
        fro_self = jnp.logical_and(fro[0] == f, fro[1] == t)
        pl.when(jnp.logical_not(to_self))(functools.partial(greet, to))
        pl.when(jnp.logical_not(fro_self))(functools.partial(greet, fro))
        n_self = n_self + to_self.astype(jnp.int32) + fro_self.astype(jnp.int32)

    par = lax.rem(x + z, 2)
    for g in range(2):
        to = (4 * y + 2 * core + g, 2 * y + par)
        to_self = jnp.logical_and(to[0] == f, to[1] == t)
        pl.when(jnp.logical_not(to_self))(functools.partial(greet, to))
        n_self = n_self + to_self.astype(jnp.int32)
    n_fro = jnp.int32(0)
    for z2 in range(4):
        for k in range(2):
            fr = (4 * z2 + 2 * k + lax.rem(z2 + core, 2), 2 * y + lax.div(x, 2))
            is_self = jnp.logical_and(fr[0] == f, fr[1] == t)
            there = jnp.logical_and(y == z, jnp.logical_not(is_self))
            pl.when(there)(functools.partial(greet, fr))
            n_fro = n_fro + there.astype(jnp.int32)

    icp = []
    for h, (gn, gt, ut, dw) in enumerate(((gn1, gt1, ut1, dn1), (gn2, gt2, ut2, dn2))):
        for k, (src, dst) in enumerate(
            ((gn, raw_g.at[h]), (gt, raw_w.at[h, 0]), (ut, raw_w.at[h, 1]), (dw, raw_d.at[h]))
        ):
            cp = pltpu.make_async_copy(src, dst, i_sem.at[h, k])
            cp.start()
            icp.append(cp)
    xcp = []
    for r in range(4):
        cp = pltpu.make_async_copy(x_hbm.at[r], nx.at[r], x_sem.at[r])
        cp.start()
        xcp.append(cp)
    own_in = pltpu.make_async_copy(x_hbm.at[z, x], xown, x_sem.at[4])
    own_in.start()

    yp, ym, y2 = rem4(y + 1), rem4(y + 3), rem4(y + 2)


    def w1(k, ft):
        return gu.at[0, k, pl.ds(0, HB), pl.ds(pl.multiple_of(ft * 128, 128), 128)]

    def stage_a():
        for k in range(2):
            for g in range(2):
                src = wt.at[0, k, pl.ds(HB * g, HB), :]
                dev = (4 * y + 2 * core + g, a_dt(g))
                same = jnp.logical_and(dev[0] == f, dev[1] == t)
                send(src, w1(k, f), w1_recv.at[k, f], dev, jnp.logical_not(same))

                @pl.when(same)
                def _(src=src, k=k):
                    pltpu.make_async_copy(src, w1(k, f), w1_recv.at[k, f]).start()

    def wv(ft):
        return gu.at[1, :, pl.ds(0, HB), pl.ds(pl.multiple_of(ft * 128, 128), 128)]

    def stage_a2():
        for g in range(2):
            src = wt.at[1, :, pl.ds(HB * g, HB), :]
            dev = (4 * y + 2 * core + g, 2 * y + par)
            same = jnp.logical_and(dev[0] == f, dev[1] == t)
            send(src, wv(f), w_recv.at[f], dev, jnp.logical_not(same))

            @pl.when(same)
            def _(src=src):
                pltpu.make_async_copy(src, wv(f), w_recv.at[f]).start()

    nxt = (f, 2 * rem4(y + 1 + 2 * core) + core)
    dist = rem4(jnp.where(core == 0, y - z, z - y) + 4)

    def chain_tile(i, cc):
        z2, k = i // 2, i % 2
        return 4 * z2 + 2 * k + lax.rem(z2 + cc, 2)

    def hop(d, batch):
        @pl.when(dist == d)
        def _():
            for i in range(4 * batch, 4 * batch + 4):
                ft = chain_tile(i, core)
                tile = wv(ft)
                arrived(tile, w_recv.at[ft])
                if d < 3:
                    remote(tile, tile, w_send.at[i], w_recv.at[ft], nxt).start()
                remote(tile, tile, w_send.at[8 + i], w_recv.at[ft], sib).start()

    def hop_end():
        for i in range(8):
            ft = chain_tile(i, core)
            tile = wv(ft)
            pending.append((tile, tile, w_send.at[i], w_recv.at[ft], nxt, dist < 3))
            pending.append((tile, tile, w_send.at[8 + i], w_recv.at[ft], sib, None))
            fo = chain_tile(i, 1 - core)
            arrived(wv(fo), w_recv.at[fo])

    def wsend(k, ft, dev):
        send(w1(k, ft), w1(k, ft), w1_recv.at[k, ft], dev)

    def wgot(k, ft):
        arrived(w1(k, ft), w1_recv.at[k, ft])

    up_dev, dn_dev = (f, 2 * yp + core), (f, 2 * ym + core)

    def w_own():
        for k in range(2):
            for q in range(2):
                ft = tile_id(y, core, q)
                wgot(k, ft)
                for dev in (up_dev, dn_dev, sib):
                    wsend(k, ft, dev)

    def w_fwd(k):
        lo, hi = tile_id(ym, core, 0), tile_id(yp, core, 1)
        wgot(k, lo)
        wsend(k, lo, up_dev)
        wgot(k, hi)
        wsend(k, hi, dn_dev)
        wsend(k, lo, sib)
        wsend(k, hi, sib)

    def w_more(k):
        for ft in (tile_id(ym, core, 1), tile_id(yp, core, 0)):
            wgot(k, ft)
            wsend(k, ft, sib)
        for q in range(2):
            ft = tile_id(y2, core, q)
            wgot(k, ft)
            wsend(k, ft, sib)

    def w_end(k):
        for yy in range(4):
            for q in range(2):
                wgot(k, tile_id(yy, 1 - core, q))

    def dblk(h, tb, q):
        return dd.at[h, pl.ds(176 * q, 176), pl.ds(pl.multiple_of(tb * 256, 256), 256)]

    def d_local(h):
        return pltpu.make_async_copy(
            dn.at[h], dd.at[h, pl.ds(0, HB), pl.ds(pl.multiple_of(t * 256, 256), 256)], d_loc.at[h]
        )

    def dsend(h, tb, q, dev):
        send(dblk(h, tb, q), dblk(h, tb, q), d_recv.at[h, tb, q], dev)

    def d_own(h):
        d_local(h).start()
        for q in range(2):
            src = dn.at[h, pl.ds(176 * q, 176), :]
            for dev in (up_dev, dn_dev, sib):
                send(src, dblk(h, t, q), d_recv.at[h, t, q], dev)

    def d_fwd(h):
        tm, tp = 2 * ym + core, 2 * yp + core
        arrived(dblk(h, tm, 0), d_recv.at[h, tm, 0])
        dsend(h, tm, 0, up_dev)
        arrived(dblk(h, tp, 1), d_recv.at[h, tp, 1])
        dsend(h, tp, 1, dn_dev)
        dsend(h, tm, 0, sib)
        dsend(h, tp, 1, sib)

    def d_more(h):
        for tb, q in ((2 * ym + core, 1), (2 * yp + core, 0), (2 * y2 + core, 0), (2 * y2 + core, 1)):
            arrived(dblk(h, tb, q), d_recv.at[h, tb, q])
            dsend(h, tb, q, sib)

    def d_end(h):
        for yy in range(4):
            for q in range(2):
                tb = 2 * yy + 1 - core
                arrived(dblk(h, tb, q), d_recv.at[h, tb, q])
        d_local(h).wait()

    def norm_rows(v):
        w = v.astype(F32)
        return (w * lax.rsqrt(jnp.mean(w * w, axis=-1, keepdims=True) + 1e-06)).astype(BF)

    def gate_up(rows, slot):
        w = gu[slot].reshape(2 * HP, D)
        v = lax.dot_general(rows, w, (((1,), (1,)), ((), ())), preferred_element_type=F32)
        gt = v[:, :HP]
        return (gt * jax.nn.sigmoid(gt) * v[:, HP:]).astype(BF)

    def nt_dot(rows, w):
        return lax.dot_general(rows, w, (((1,), (1,)), ((), ())), preferred_element_type=F32)

    def gate_row(zi):
        gates[zi] = nt_dot(nx[zi].reshape(256, D), gu[0, 0]).reshape(4, 64, HP)

    def with_gate(gt, rows):
        return (gt * jax.nn.sigmoid(gt) * nt_dot(rows, gu[0, 1])).astype(BF)

    def act_row(h, zi):
        if h == 1:
            act[zi] = gate_up(ng[zi].reshape(256, D), 1).reshape(4, 64, HP)
        else:
            act[zi] = with_gate(gates[zi].reshape(256, HP), nx[zi].reshape(256, D)).reshape(4, 64, HP)

    def act_col(xi):
        rows = nx[:, pl.ds(xi, 1)].reshape(256, D)
        act[:, pl.ds(xi, 1)] = with_gate(gates[:, pl.ds(xi, 1)].reshape(256, HP), rows).reshape(4, 1, 64, HP)

    OFF = (2, 3, 1, 0)

    def pv(h, ab, i, o):
        j = rem4((z if ab == 0 else x) + o)
        if ab == 0:
            return part.at[h, j, i, :, pl.ds(0, 1024)]
        return part.at[h, i, j, :, pl.ds(1024, 1024)]

    def dev1(ab, step):
        if ab == 0:
            return (4 * z + rem4(x + step + 4), t)
        return (4 * rem4(z + step + 4) + x, t)

    def me1(ab, step):
        return rem4((x if ab == 0 else z) + step + 4)

    def down_chunk(h, ab, step):
        idx = me1(ab, step)
        w = dd[h, :, 1024 * ab:1024 * ab + 1024]
        if ab == 0:
            a = act[:, pl.ds(idx, 1)].reshape(256, HP)
        else:
            a = act[idx].reshape(256, HP)
        v = jnp.dot(a, w, preferred_element_type=F32).astype(BF)
        if ab == 0:
            part[h, :, pl.ds(idx, 1), :, 0:1024] = v.reshape(4, 1, 64, 1024)
        else:
            part[h, idx, :, :, 1024:2048] = v.reshape(4, 64, 1024)

    def s1(h, ab, k, src, dst, dev):
        send(src, dst, rs_recv.at[ab, k], dev)

    def rs_away(h, ab):
        for o in OFF:
            s1(h, ab, o, pv(h, ab, me1(ab, 2), o), r2.at[h, ab, o], dev1(ab, 1 if o in (2, 1) else -1))

    def rs_direct(h, ab, o):
        if o in (2, 1):
            s1(h, ab, 8 + o, pv(h, ab, me1(ab, -1), o), rb.at[h, ab, o], dev1(ab, -1))
        else:
            s1(h, ab, 8 + o, pv(h, ab, me1(ab, 1), o), ra.at[h, ab, o], dev1(ab, 1))

    def rs_turn(h, ab, o):
        arrived(r2.at[h, ab, o], rs_recv.at[ab, o])
        step = 1 if o in (2, 1) else -1
        tt[h, ab, o] = (r2[h, ab, o].astype(F32) + pv(h, ab, me1(ab, step), o)[...].astype(F32)).astype(BF)
        s1(h, ab, 4 + o, tt.at[h, ab, o], (ra if step == 1 else rb).at[h, ab, o], dev1(ab, step))

    def rs_fin(h, ab, o):
        ka, kb = (4 + o, 8 + o) if o in (2, 1) else (8 + o, 4 + o)
        arrived(ra.at[h, ab, o], rs_recv.at[ab, ka])
        arrived(rb.at[h, ab, o], rs_recv.at[ab, kb])
        s = pv(h, ab, me1(ab, 0), o)[...].astype(F32) + ra[h, ab, o].astype(F32) + rb[h, ab, o].astype(F32)
        acc[ab, o] = s
        up2, dn2_ = dev1(1 - ab, 1), dev1(1 - ab, -1)
        lo, hi = pl.ds(0, 32), pl.ds(32, 32)
        if o != 0:
            sb[h, ab, o] = s.astype(BF)
        if o == 2:
            s1(h, ab, 12, sb.at[h, ab, o, lo], q2.at[h, ab, 0], up2)
            s1(h, ab, 13, sb.at[h, ab, o, hi], q2.at[h, ab, 1], dn2_)
        if o == 1:
            s1(h, ab, 15, sb.at[h, ab, o, hi], qa.at[h, ab, hi], up2)
        if o == 3:
            s1(h, ab, 16, sb.at[h, ab, o, lo], qb.at[h, ab, lo], dn2_)

    def rs_turn2(h, ab, o):
        if o == 1:
            arrived(q2.at[h, ab, 0], rs_recv.at[ab, 12])
            qt[h, ab, 0] = (q2[h, ab, 0].astype(F32) + acc[ab, 1, 0:32]).astype(BF)
            s1(h, ab, 14, qt.at[h, ab, 0], qa.at[h, ab, pl.ds(0, 32)], dev1(1 - ab, 1))
        else:
            arrived(q2.at[h, ab, 1], rs_recv.at[ab, 13])
            qt[h, ab, 1] = (q2[h, ab, 1].astype(F32) + acc[ab, 3, 32:64]).astype(BF)
            s1(h, ab, 17, qt.at[h, ab, 1], qb.at[h, ab, pl.ds(32, 32)], dev1(1 - ab, -1))

    def rs_out(h, ab):
        arrived(qa.at[h, ab, pl.ds(32, 32)], rs_recv.at[ab, 15])
        arrived(qb.at[h, ab, pl.ds(0, 32)], rs_recv.at[ab, 16])
        arrived(qa.at[h, ab, pl.ds(0, 32)], rs_recv.at[ab, 14])
        arrived(qb.at[h, ab, pl.ds(32, 32)], rs_recv.at[ab, 17])
        return acc[ab, 0] + qa[h, ab].astype(F32) + qb[h, ab].astype(F32)

    def rs_run(h, points):
        def point(k):
            for fn in points.get(k, ()):
                fn()

        down_chunk(h, 0, 2)
        rs_away(h, 0)
        down_chunk(h, 1, 2)
        rs_away(h, 1)
        point(0)
        down_chunk(h, 1, -1)
        rs_direct(h, 1, 2)
        point(1)
        down_chunk(h, 1, 1)
        point(2)
        down_chunk(h, 0, -1)
        rs_direct(h, 0, 2)
        down_chunk(h, 0, 1)
        for ab in (1, 0):
            rs_turn(h, ab, 2)
            rs_direct(h, ab, 3)
            rs_turn(h, ab, 3)
        for ab in (1, 0):
            rs_turn(h, ab, 1)
            rs_direct(h, ab, 1)
        for ab in range(2):
            down_chunk(h, ab, 0)
        for ab in (1, 0):
            rs_fin(h, ab, 2)
        for ab in (1, 0):
            rs_direct(h, ab, 0)
        point(3)
        for ab in (1, 0):
            rs_fin(h, ab, 3)
            rs_turn(h, ab, 0)
        point(4)
        for ab in (1, 0):
            rs_fin(h, ab, 1)
        point(5)
        for ab in (1, 0):
            rs_turn2(h, ab, 3)
            rs_turn2(h, ab, 1)
        for ab in (1, 0):
            rs_fin(h, ab, 0)
        point(6)
        return jnp.concatenate([rs_out(h, 0), rs_out(h, 1)], axis=-1)

    lo_rows, hi_rows = pl.ds(0, 32), pl.ds(32, 32)
    waited = set()

    def gv(ab, i, j, rows=slice(None)):
        zi, xi = (i, j) if ab == 0 else (j, i)
        return ng.at[rem4(z + zi), rem4(x + xi), rows, pl.ds(1024 * ab, 1024)]

    LAND = {
        0: (3, 0), 1: (1, 0), 2: (2, 0, lo_rows), 3: (2, 0, hi_rows),
        4: (0, 3), 5: (1, 3), 6: (2, 3), 7: (3, 3),
        8: (0, 1), 9: (1, 1), 10: (2, 1), 11: (3, 1),
        12: (0, 2), 13: (1, 2), 14: (3, 2), 15: (2, 2),
    }

    def got(ab, *slots):
        for k in slots:
            if (ab, k) not in waited:
                waited.add((ab, k))
                arrived(gv(ab, *LAND[k]), w1_recv.at[ab, k])

    def snd(ab, k, ref, second, step):
        send(ref, ref, w1_recv.at[ab, k], dev1(ab if second else 1 - ab, step))

    def ag_start():
        for ab in range(2):
            snd(ab, 0, gv(ab, 0, 0), False, 1)
            snd(ab, 1, gv(ab, 0, 0), False, -1)
        for ab in range(2):
            snd(ab, 4, gv(ab, 0, 0), True, 1)
            snd(ab, 8, gv(ab, 0, 0), True, -1)

    def ag_first():
        for ab in range(2):
            got(ab, 0)
            snd(ab, 2, gv(ab, 3, 0, lo_rows), False, 1)
            got(ab, 1)
            snd(ab, 3, gv(ab, 1, 0, hi_rows), False, -1)
        for ab in range(2):
            snd(ab, 5, gv(ab, 1, 0), True, 1)
            snd(ab, 11, gv(ab, 3, 0), True, -1)
            snd(ab, 7, gv(ab, 3, 0), True, 1)
            snd(ab, 9, gv(ab, 1, 0), True, -1)

    def ag_second():
        for ab in range(2):
            got(ab, 4)
            snd(ab, 12, gv(ab, 0, 3), True, 1)
        for ab in range(2):
            got(ab, 2, 3)
            snd(ab, 10, gv(ab, 2, 0), True, -1)
            snd(ab, 6, gv(ab, 2, 0), True, 1)

    def ag_third():
        for ab in range(2):
            got(ab, 5)
            snd(ab, 13, gv(ab, 1, 3), True, 1)
            got(ab, 8, 11)
            snd(ab, 14, gv(ab, 3, 1), True, -1)

    def ag_fourth():
        for ab in range(2):
            got(ab, 9, 10)
            snd(ab, 15, gv(ab, 2, 1), True, -1)

    def ag_row(oz):
        for k, v in LAND.items():
            if v[0] == oz:
                got(0, k)
            if v[1] == oz:
                got(1, k)

    def put(src, dst, k):
        pltpu.make_async_copy(src, dst, i_sem.at[k // 4, k % 4]).start()

    def put_wait(src, dst, k):
        pltpu.make_async_copy(src, dst, i_sem.at[k // 4, k % 4]).wait()

    def fold(h):
        for k in range(4):
            icp[4 * h + k].wait()
        for k in range(2):
            wt[h, k] = (raw_g[h] * raw_w[h, k]).astype(BF)
        dn[h] = raw_d[h].astype(BF)

    def norm_first(r):
        xcp[r].wait()
        for k in range(4):
            nx[r, k] = norm_rows(nx[r, k])

    fold(0)
    pl.semaphore_wait(barrier, 13 - n_self + n_fro)
    stage_a()
    d_own(0)
    for s_ in range(2):
        dd[s_, HB:HP, :] = jnp.zeros((HP - HB, D), BF)
        for k in range(2):
            gu[s_, k, HB:HP, :] = jnp.zeros((HP - HB, D), BF)
    for r in range(4):
        norm_first(r)
    fold(1)
    w_own()
    stage_a2()
    w_fwd(0)
    w_fwd(1)
    d_fwd(0)
    w_more(0)
    w_end(0)
    gate_row(0)
    gate_row(1)
    w_more(1)
    gate_row(2)
    gate_row(3)
    w_end(1)
    d_more(0)
    put(gu.at[0, 0, pl.ds(0, HB)], g1_o, 0)
    put(gu.at[0, 1, pl.ds(0, HB)], u1_o, 1)
    act_col(rem4(x + 2))
    act_row(0, rem4(z + 2))
    d_end(0)
    put(dd.at[0, pl.ds(0, HB)], d1_o, 2)
    branch = rs_run(0, {
        0: (lambda: hop(0, 0), lambda: hop(0, 1), lambda: act_row(0, rem4(z + 3))),
        1: (lambda: act_row(0, rem4(z + 1)),),
        2: (lambda: act_row(0, z),),
        3: (lambda: hop(1, 0),),
        5: (lambda: hop(1, 1), lambda: d_own(1)),
    })
    own_in.wait()
    m = (xown[...].astype(F32) + 0.5 * branch).astype(BF)
    mid[...] = m
    ng[z, x] = norm_rows(m)
    ag_start()
    hop(2, 0)
    ag_first()
    hop(2, 1)
    ag_second()
    ag_third()
    d_fwd(1)
    ag_fourth()
    hop(3, 0)
    hop(3, 1)
    hop_end()
    ag_row(0)
    act_row(1, z)
    put(gu.at[1, 0, pl.ds(0, HB)], g2_o, 3)
    put(gu.at[1, 1, pl.ds(0, HB)], u2_o, 4)
    for oz in (1, 3):
        ag_row(oz)
        act_row(1, rem4(z + oz))
    d_more(1)
    ag_row(2)
    act_row(1, rem4(z + 2))
    d_end(1)
    put(dd.at[1, pl.ds(0, HB)], d2_o, 5)
    branch = rs_run(1, {})
    ost[...] = (mid[...].astype(F32) + 0.5 * branch).astype(BF)
    put(ost, ps_o, 6)

    drain()
    put_wait(gu.at[0, 0, pl.ds(0, HB)], g1_o, 0)
    put_wait(gu.at[0, 1, pl.ds(0, HB)], u1_o, 1)
    put_wait(dd.at[0, pl.ds(0, HB)], d1_o, 2)
    put_wait(gu.at[1, 0, pl.ds(0, HB)], g2_o, 3)
    put_wait(gu.at[1, 1, pl.ds(0, HB)], u2_o, 4)
    put_wait(dd.at[1, pl.ds(0, HB)], d2_o, 5)
    put_wait(ost, ps_o, 6)


def copy_out(*refs):
    n = len(refs) // 2
    sems = refs[-1]
    cps = [pltpu.make_async_copy(refs[k], refs[n + k], sems.at[k]) for k in range(n)]
    for cp in cps:
        cp.start()
    for cp in cps:
        cp.wait()


def run(xin, *weights):
    vm = pltpu.VMEM
    dma = pltpu.SemaphoreType.DMA
    w_out = jax.ShapeDtypeStruct((HB, D), BF)
    out_shape = (w_out,) * 6 + (jax.ShapeDtypeStruct((64, D), BF),)
    unit = (2, 2, 4, 64, 1024)
    half = (2, 2, 2, 32, 1024)
    one = (2, 2, 64, 1024)
    scratch = [
        vm((4, 4, 64, D), BF), vm((4, 4, 64, D), BF), vm((64, D), BF), vm((64, D), BF),
        vm((2, 2, 2 * HB, 128), F32), vm((2, HB, 256), F32), vm((2, 1, 128), F32),
        vm((2, 2, 2 * HB, 128), BF), vm((2, HB, 256), BF),
        vm((2, 2, HP, D), BF), vm((2, HP, D), BF), vm((4, 4, 64, HP), BF), vm((2, 4, 4, 64, D), BF),
        vm((4, 4, 64, HP), F32),
        vm(unit, BF), vm(unit, BF), vm(unit, BF), vm(unit, BF), vm((2, 4, 64, 1024), F32), vm(unit, BF),
        vm(half, BF), vm(one, BF), vm(one, BF), vm(half, BF), vm((64, D), BF),
        dma((POOL,)), dma((2, 16)), dma((16,)), dma((16,)), dma((2, 8, 2)), dma((2,)), dma((2, 18)),
        dma((5,)), dma((2, 4)),
    ]
    here = [pltpu.with_memory_space_constraint(v, pltpu.HBM) for v in (xin, *weights)]
    outs = pl.pallas_call(
        kernel,
        out_shape=tuple(pltpu.VMEM(o.shape, o.dtype) for o in out_shape),
        in_specs=[pl.BlockSpec(memory_space=pltpu.HBM)] * 9,
        out_specs=tuple(pl.BlockSpec(memory_space=pl.ANY) for _ in range(7)),
        scratch_shapes=scratch,
        compiler_params=pltpu.CompilerParams(
            collective_id=0, has_side_effects=True, vmem_limit_bytes=VMEM_MB * 1024 * 1024
        ),
    )(*here)
    return pl.pallas_call(
        copy_out,
        out_shape=out_shape,
        in_specs=[pl.BlockSpec(memory_space=pl.ANY)] * 7,
        out_specs=tuple(pl.BlockSpec(memory_space=pltpu.HBM) for _ in range(7)),
        scratch_shapes=[dma((7,))],
        compiler_params=pltpu.CompilerParams(vmem_limit_bytes=1024 * 1024),
    )(*outs)


def per_device(
    prompts, gain_first, gate_first, up_first, down_first, gain_second, gate_second, up_second, down_second
):
    xin = prompts.reshape(4, 4, 64, D)
    g1, u1, d1, g2, u2, d2, ps = run(
        xin,
        gain_first.reshape(1, 128), gate_first.T, up_first.T, down_first,
        gain_second.reshape(1, 128), gate_second.T, up_second.T, down_second,
    )
    return g1.T, u1.T, d1, g2.T, u2.T, d2, ps.reshape(1, 64, D)


def solution(mesh):
    w = P("fs", "tp")
    return jax.shard_map(
        per_device,
        mesh=mesh,
        in_specs=(P("tp", None, None), P("fs"), w, w, w, P("fs"), w, w, w),
        out_specs=(
            P(None, "fs"), P(None, "fs"), P("fs", None),
            P(None, "fs"), P(None, "fs"), P("fs", None),
            P("tp", "fs", None),
        ),
        check_vma=False,
    )
```
